32 devices in a mesh: grp: 2 (over y), sp: 4 (over z), tp: 4 (over x, core).
Axes of the slice: x: 2, y: 2, z: 4, core: 2. Of those that a mesh axis runs over, the one named last changes fastest.
Arguments:
- tokens: bfloat16 [1280, 2048], P(('grp', 'sp')), parts along dimension 0, may hold values from -6 to 6
- norm_gain: float32 [2048], replicated, may hold values from 0.6 to 5
- query_weight: bfloat16 [2048, 2048], P('sp', 'tp')
- key_weight: bfloat16 [2048, 512], P('sp', 'tp')
- value_weight: bfloat16 [2048, 512], P('sp', 'tp'), may hold values from -0.125 to 0.125
- map_lambda: float32 [16], P('tp'), may hold values from 0.3 to 0.8
- head_gain: float32 [16, 128], P('tp'), may hold values from 0.1 to 1.9
- attn_out_weight: bfloat16 [2048, 2048], P('tp', 'sp'), may hold values from -0.125 to 0.125
- pool_out_weight: bfloat16 [2048, 2048], P('tp', 'sp'), may hold values from -0.09375 to 0.09375
Outputs:
- mixed_rows: bfloat16 [1280, 2048], P(('grp', 'sp', 'tp')), parts along dimension 0
- log_totals: float32 [2, 16, 1280], P(None, 'tp', ('grp', 'sp')), parts along dimension 2
The draws below stay inside these ranges and needn't reach their ends.
There are 2 independent parts, one for each index of `grp`. The reference program is written for one: setup_inputs(seed, part) draws one part's arguments, and reference() takes and returns one part's arrays. A program takes and returns all parts, laid end to end along the dimension named above; an argument that names none is the same for every part. Nothing has to cross between parts.
All inputs are finite; a program needn't handle non-finite values.
Results may differ from the reference program's by a relative error of at most 0.013.
The reference program's roundings to bfloat16 on the way (of `normed`, `head_rows` and `pooled`) count: a program that leaves them out, or rounds other values in their place, can miss the bound.
Values may be sent and summed in bfloat16 or wider, within the bound.
A program may use at most 64 MiB of HBM per device.

```python
import math
import jax
import jax.numpy as jnp
from jax import lax

D = 2048
HEADS = 16
KV_HEADS = 4
HD = 64
VD = 128
SEQ = 640


def projection_pair(key):
    base_key = jax.random.fold_in(key, 71)
    query_key, other_key = jax.random.split(base_key)
    spread_std = 1.32 / math.sqrt(D)
    w_query = jax.random.normal(query_key, (D, HEADS * 2 * HD), jnp.float32) * spread_std
    fresh_part = jax.random.normal(other_key, (D, KV_HEADS * 2 * HD), jnp.float32) * spread_std
    w_key = fresh_part
    return (w_query, w_key)


def draw_query_weight(key, part):
    return projection_pair(key)[0].astype(jnp.bfloat16)


def draw_key_weight(key, part):
    return projection_pair(key)[1].astype(jnp.bfloat16)


def draw_norm_gain(key, part):
    gain_key = jax.random.fold_in(key, 13)
    return jax.random.uniform(gain_key, (D,), jnp.float32, 0.6, 1.4)


def shard_levels(own_key, shape, cuts, least, top_value):
    level, own = 1.0, jax.random.fold_in(own_key, 6)
    for dim, shards_of in cuts:
        steps = jnp.exp(jax.random.uniform(jax.random.fold_in(own, dim), (shards_of,), jnp.float32, least / len(cuts), top_value / len(cuts)))
        level = level * jnp.repeat(steps, shape[dim] // shards_of).reshape([-1 if axis == dim else 1 for axis in range(len(shape))])
    return level


def scatter_about(stream_key, dims, deviation, limit, cuts=(), kind=jnp.bfloat16):
    values = deviation * jax.random.normal(stream_key, dims, jnp.float32)
    if cuts:
        values = values * shard_levels(stream_key, dims, cuts, -0.22, 0.18)
    return jnp.clip(values, -limit, limit).astype(kind)


def setup_inputs(seed: int = 0, part: int = 0) -> dict:
    streams_of = jax.random.split(jax.random.key(seed), 10)
    part_splits = jax.random.split(jax.random.fold_in(streams_of[9], part), 10)
    tokens = scatter_about(part_splits[0], (SEQ, D), 1.0, 6.0, ((0, 4),))
    norm_gain = draw_norm_gain(jax.random.fold_in(streams_of[9], 71), part)
    query_weight = draw_query_weight(jax.random.fold_in(streams_of[9], 71), part)
    key_weight = draw_key_weight(jax.random.fold_in(streams_of[9], 71), part)
    value_weight = scatter_about(streams_of[4], (D, KV_HEADS * VD), D ** -0.5, 0.125, ((0, 4), (1, 4)))
    map_lambda = jnp.clip(0.3 + 0.5 * jax.random.uniform(streams_of[5], (HEADS,), jnp.float32) ** shard_levels(streams_of[5], (HEADS,), ((0, 4),), -0.2, 0.2), 0.3, 0.8)
    head_gain = jnp.clip(1.0 + 0.18 * jax.random.normal(streams_of[6], (HEADS, VD), jnp.float32), 0.1, 1.9)
    attn_out_weight = scatter_about(streams_of[7], (HEADS * VD, D), (HEADS * VD) ** -0.5, 0.125, ((0, 4), (1, 4)))
    pool_out_weight = scatter_about(streams_of[8], (D, D), (2 * D) ** -0.5, 0.09375, ((0, 4), (1, 4)))
    return {"tokens": tokens, "norm_gain": norm_gain, "query_weight": query_weight, "key_weight": key_weight, "value_weight": value_weight, "map_lambda": map_lambda, "head_gain": head_gain, "attn_out_weight": attn_out_weight, "pool_out_weight": pool_out_weight}


epsilon = 1e-06

def reference(tokens, norm_gain, query_weight, key_weight, value_weight, map_lambda, head_gain, attn_out_weight, pool_out_weight):
    group_heads = HEADS // KV_HEADS
    tokens_wide = tokens.astype(jnp.float32)
    normed = (tokens_wide * lax.rsqrt(lax.optimization_barrier(jnp.mean(tokens_wide * tokens_wide, axis=-1, keepdims=True)) + epsilon) * norm_gain).astype(jnp.bfloat16)
    queries = jnp.dot(normed, query_weight, preferred_element_type=jnp.float32).astype(jnp.bfloat16)
    keys = jnp.dot(normed, key_weight, preferred_element_type=jnp.float32).astype(jnp.bfloat16)
    values = jnp.dot(normed, value_weight, preferred_element_type=jnp.float32).astype(jnp.bfloat16)
    keys_f32 = keys.reshape(SEQ, KV_HEADS, 2, HD).astype(jnp.float32)
    values_f32 = values.reshape(SEQ, KV_HEADS, VD).astype(jnp.float32)
    block_len = math.gcd(SEQ, 256)
    query_blocks = queries.reshape(SEQ // block_len, block_len, KV_HEADS, group_heads, 2, HD)
    lambdas = map_lambda.reshape(KV_HEADS, group_heads, 1, 1)
    gains = head_gain.reshape(KV_HEADS, group_heads, 1, VD)

    def attend(query_blk):
        scores = jnp.einsum('qhgmd,khmd->hgmqk', query_blk.astype(jnp.float32), keys_f32) * HD ** (-0.5)
        highest = lax.optimization_barrier(jnp.max(scores, axis=-1))
        weights = jnp.exp(scores - highest[..., None])
        totals = lax.optimization_barrier(jnp.sum(weights, axis=-1))
        weights_b = lax.optimization_barrier(weights.astype(jnp.bfloat16)).astype(jnp.float32)
        reads = jnp.einsum('hgmqk,khe->hgmqe', weights_b, values_f32) / totals[..., None]
        contrast = reads[:, :, 0] - lambdas * reads[:, :, 1]
        scaled = contrast * lax.rsqrt(lax.optimization_barrier(jnp.mean(contrast * contrast, axis=-1, keepdims=True)) + epsilon) * gains
        head_rows = jnp.transpose(scaled, (2, 0, 1, 3)).reshape(block_len, HEADS * VD)
        return (head_rows.astype(jnp.bfloat16), highest + jnp.log(totals))
    head_rows, log_parts = lax.map(attend, query_blocks)
    head_rows = head_rows.reshape(SEQ, HEADS * VD)
    log_totals = jnp.transpose(log_parts, (3, 1, 2, 0, 4)).reshape(2, HEADS, SEQ)
    normed_f32 = normed.astype(jnp.float32)
    prefix = jnp.concatenate([jnp.zeros((1, D), jnp.float32), jnp.cumsum(normed_f32, axis=0)], axis=0)
    position = jnp.arange(SEQ)
    group_width = D // 4
    pieces = []
    for group in range(4):
        window = 2 ** (group + 1)
        lower_edge = jnp.clip(position - window // 2, 0, SEQ)
        upper_edge = jnp.clip(position + window - window // 2, 0, SEQ)
        counts_f = (upper_edge - lower_edge).astype(jnp.float32)[:, None]
        columns = prefix[:, group * group_width:(group + 1) * group_width]
        own_chan = normed_f32[:, group * group_width:(group + 1) * group_width]
        pieces.append((columns[upper_edge] - columns[lower_edge]) / counts_f - own_chan)
    pooled = jnp.concatenate(pieces, axis=1).astype(jnp.bfloat16)
    mixed = jnp.dot(head_rows, attn_out_weight, preferred_element_type=jnp.float32) + jnp.dot(pooled, pool_out_weight, preferred_element_type=jnp.float32)
    return (mixed.astype(jnp.bfloat16), log_totals)
```

```python
import functools
import math

import jax
import jax.numpy as jnp
from jax import lax
from jax.experimental import pallas as pl
from jax.experimental.pallas import tpu as pltpu
from jax.sharding import PartitionSpec as P

HD = 64
VD = 128
POOL_SPAN = 16


epsilon = 1e-06
very_low = -1e30


def extended(cells, sides, width):
    for axis, dim in sides:
        count = lax.axis_size(axis)
        ends = count - 1
        head = lax.slice_in_dim(cells, 0, width, axis=dim)
        tail = lax.slice_in_dim(cells, cells.shape[dim] - width, cells.shape[dim], axis=dim)
        cells = jnp.concatenate(
            [
                lax.ppermute(tail, axis, [(i, (i + 1) % count) for i in range(ends)]),
                cells,
                lax.ppermute(head, axis, [((i + 1) % count, i) for i in range(ends)]),
            ],
            axis=dim,
        )
    return cells


def add_products(totals, pieces, source):
    results = []
    for running, piece in zip(totals, pieces):
        results.append(jnp.dot(source, piece, preferred_element_type=jnp.float32))
    return tuple(results)


def on_device(
    tokens,
    norm_gain,
    query_weight,
    key_weight,
    value_weight,
    map_lambda,
    head_gain,
    attn_out_weight,
    pool_out_weight,
):
    tokens_wide = tokens.astype(jnp.float32)
    normed = (
        tokens_wide
        * lax.rsqrt(jnp.mean(tokens_wide * tokens_wide, axis=-1, keepdims=True) + epsilon)
        * norm_gain
    ).astype(jnp.bfloat16)
    row_count = normed.shape[0]
    sp_index = lax.axis_index("sp")
    tp_index = lax.axis_index("tp")
    group_width = pool_out_weight.shape[0]
    local_heads = map_lambda.shape[0]
    key_heads = value_weight.shape[1] // VD
    group_heads = local_heads // key_heads
    q_empty = jnp.zeros((row_count, query_weight.shape[1]), jnp.float32)
    k_empty = jnp.zeros((row_count, key_weight.shape[1]), jnp.float32)
    v_empty = jnp.zeros((row_count, value_weight.shape[1]), jnp.float32)
    q_acc, k_acc, v_acc = add_products(
        (q_empty, k_empty, v_empty),
        (
            lax.all_gather(query_weight, "sp", axis=0, tiled=True),
            lax.all_gather(key_weight, "sp", axis=0, tiled=True),
            lax.all_gather(value_weight, "sp", axis=0, tiled=True),
        ),
        normed,
    )
    queries = q_acc.astype(jnp.bfloat16).reshape(row_count, key_heads, group_heads, 2, HD)
    keys_flat = k_acc.astype(jnp.bfloat16)
    values_flat = v_acc.astype(jnp.bfloat16)

    def key_block(state_now, key_pair):
        maxima, totals, accums = state_now
        key_blk, val_blk = key_pair
        scores = jnp.einsum(
            "qhgmd,khmd->hgmqk", queries, key_blk, preferred_element_type=jnp.float32
        ) * HD ** (-0.5)
        highest = jnp.maximum(maxima, jnp.max(scores, axis=-1))
        factor = jnp.exp(maxima - highest)
        weights = jnp.exp(scores - highest[..., None])
        totals = totals * factor + jnp.sum(weights, axis=-1)
        accums = accums * factor[..., None] + jnp.einsum(
            "hgmqk,khe->hgmqe",
            weights.astype(jnp.bfloat16),
            val_blk,
            preferred_element_type=jnp.float32,
        )
        return ((highest, totals, accums), None)

    start_state = (
        jnp.full((key_heads, group_heads, 2, row_count), very_low, jnp.float32),
        jnp.zeros((key_heads, group_heads, 2, row_count), jnp.float32),
        jnp.zeros((key_heads, group_heads, 2, row_count, VD), jnp.float32),
    )
    key_piece = lax.all_gather(keys_flat, "sp", axis=0, tiled=True)
    val_piece = lax.all_gather(values_flat, "sp", axis=0, tiled=True)
    piece_len = key_piece.shape[0]
    block_len = math.gcd(piece_len, 512)
    key_blocks = key_piece.reshape(piece_len // block_len, block_len, key_heads, 2, HD)
    val_blocks = val_piece.reshape(piece_len // block_len, block_len, key_heads, VD)
    state_next, unused = lax.scan(key_block, start_state, (key_blocks, val_blocks))
    maxima, totals, accums = state_next
    log_parts = maxima + jnp.log(totals)
    log_totals = jnp.transpose(log_parts, (2, 0, 1, 3)).reshape(2, local_heads, row_count)
    reads = accums / totals[..., None]
    contrast = reads[:, :, 0] - map_lambda.reshape(key_heads, group_heads, 1, 1) * reads[:, :, 1]
    scaled = (
        contrast
        * lax.rsqrt(jnp.mean(contrast * contrast, axis=-1, keepdims=True) + epsilon)
        * head_gain.reshape(key_heads, group_heads, 1, VD)
    )
    attention_head_rows = (
        jnp.transpose(scaled, (2, 0, 1, 3))
        .reshape(row_count, local_heads * VD)
        .astype(jnp.bfloat16)
    )
    head_rows, log_totals = (attention_head_rows, log_totals)
    own_chan = lax.dynamic_slice_in_dim(normed, tp_index * group_width, group_width, 1)
    reach = POOL_SPAN // 2
    padded = extended(own_chan, (("sp", 0),), reach)
    window = jnp.left_shift(jnp.int32(2), tp_index)
    half_span = window // 2
    running = jnp.zeros((row_count, group_width), jnp.float32)
    for offset in range(POOL_SPAN):
        piece = lax.dynamic_slice_in_dim(padded, reach - half_span + offset, row_count, 0).astype(
            jnp.float32
        )
        running = running + jnp.where(offset < window, piece, 0.0)
    seq_len = row_count * lax.axis_size("sp")
    position = sp_index * row_count + jnp.arange(row_count, dtype=jnp.int32)
    lower_edge = jnp.clip(position - half_span, 0, seq_len)
    upper_edge = jnp.clip(position + window - half_span, 0, seq_len)
    counts_f = (upper_edge - lower_edge).astype(jnp.float32)[:, None]
    pooled = (running / counts_f - own_chan.astype(jnp.float32)).astype(jnp.bfloat16)
    attn_whole, pool_whole = (
        lax.all_gather(attn_out_weight, "sp", axis=1, tiled=True),
        lax.all_gather(pool_out_weight, "sp", axis=1, tiled=True),
    )
    mixed = lax.psum_scatter(
        (
            jnp.dot(head_rows, attn_whole, preferred_element_type=jnp.float32)
            + jnp.dot(pooled, pool_whole, preferred_element_type=jnp.float32)
        ).astype(jnp.bfloat16),
        "tp",
        scatter_dimension=0,
        tiled=True,
    )
    return (mixed, log_totals)


MESH = pl.DeviceIdType.MESH
LANES = 128


def fused_kernel(
    count,
    tok,
    gain,
    wq,
    wk,
    wv,
    lam,
    hgain,
    wao,
    wpo,
    mixed_out,
    lt_out,
    tok_own,
    norm_all,
    kv_own,
    q_own,
    w_kv,
    w_q,
    par_own,
    par_in,
    par_use,
    q_all,
    k_all,
    v_all,
    head_own,
    heads_all,
    pooled_all,
    part_out,
    part_in,
    cross_out,
    cross_in,
    block_out,
    block_in,
    lt_send,
    lt_in,
    wao_in,
    wpo_in,
    local_sem,
    z_send,
    z_recv,
    f_send,
    f_recv,
    kv_send,
    kv_recv,
    q_send,
    q_sib,
    q_twin,
    q_recv,
    par_sem,
    h_send,
    h_fwd,
    h_recv,
    p_send,
    p_recv,
    x_send,
    x_recv,
    o_send,
    o_recv,
    l_send,
    l_recv,
):
    g = lax.axis_index("grp")
    s = lax.axis_index("sp")
    t = lax.axis_index("tp")
    c = lax.rem(t, 2)
    x = t // 2
    rows, width = tok.shape
    quarter = width // 4
    shard = wq.shape[0]
    part = shard // 2
    half = s // 2
    in_half = c == half
    inner = (s > 0) & (s < count - 1)
    sib = t + 1 - 2 * c
    far = lax.rem(t + 2, 4)
    diag = lax.rem(sib + 2, 4)
    twin = 1 - g
    outer = jnp.where(half == 1, count - 1, 0)
    mate = 2 * half + 1 - lax.rem(s, 2)
    beyond = jnp.where(half == 0, 2, 1)
    near = jnp.where(c == 1, jnp.where(s == 2, 3, 2), jnp.where(s == 1, 0, 1))
    home = 2 * x + half
    mine = 2 * lax.rem(s, 2) + c
    theirs = 2 * lax.rem(s, 2) + 1 - c
    f32, bf16 = jnp.float32, jnp.bfloat16

    def span(index, size):
        return pl.ds(pl.multiple_of(index * size, size), size)

    def half_rows(owner, which):
        return pl.ds(pl.multiple_of(owner * shard + which * part, part), part)

    pieces = (
        (tok, tok_own),
        (wk, kv_own.at[:, 0:LANES]),
        (wv, kv_own.at[:, LANES : 2 * LANES]),
        (wq, q_own),
        (wao, wao_in),
        (wpo, wpo_in),
    )
    local = [
        pltpu.make_async_copy(src, dst, local_sem.at[i]) for i, (src, dst) in enumerate(pieces)
    ]
    own_pieces = (
        (wk, w_kv.at[span(s, shard), 0:LANES]),
        (wv, w_kv.at[span(s, shard), LANES : 2 * LANES]),
        (wq.at[:, span(mine, LANES)], w_q.at[span(s, shard), :]),
    )
    own_local = [
        pltpu.make_async_copy(src, dst, local_sem.at[len(pieces) + i])
        for i, (src, dst) in enumerate(own_pieces)
    ]
    greeted = []
    for off in range(1, count):
        peer = lax.rem(s + off, count)
        greeted += [{"sp": peer}, {"sp": peer, "tp": sib}]
    greeted += [{"tp": sib}, {"tp": far}, {"grp": twin}, {"grp": twin, "tp": sib}]
    barrier = pltpu.get_barrier_semaphore()
    for where in greeted:
        pl.semaphore_signal(barrier, inc=1, device_id=where, device_id_type=MESH)
    for piece in local:
        piece.start()

    @pl.when(in_half)
    def _():
        for piece in own_local:
            piece.start()

    for i in range(count):
        par_own[i : i + 1, :] = hgain[i : i + 1, :]
        par_own[count + i : count + i + 1, :] = jnp.full((1, LANES), lam[i], f32)

    def copy(src, dst, send, recv, where):
        return pltpu.make_async_remote_copy(
            src_ref=src,
            dst_ref=dst,
            send_sem=send,
            recv_sem=recv,
            device_id=where,
            device_id_type=MESH,
        )

    def z_copy(owner, up):
        place = norm_all.at[span(owner, rows), span(t, quarter)]
        step = 1 if up else -1
        where = {"sp": lax.rem(s + step + count, count)}
        return copy(place, place, z_send.at[owner, int(up)], z_recv.at[owner], where)

    def tok_forward(step, owner):
        col = span(far if step == 2 else t, quarter)
        place = norm_all.at[span(owner, rows), col]
        where = {"tp": far if step == 1 else sib}
        return copy(place, place, f_send.at[step, owner], f_recv.at[step, owner], where)

    def kv_first():
        src = kv_own.at[span(g, part), :]
        return copy(src, w_kv.at[half_rows(s, g), :], kv_send.at[0, s], kv_recv.at[s, g], {"sp": near})

    def kv_beside():
        where = {"tp": sib}
        return copy(kv_own, w_kv.at[span(s, shard), :], kv_send.at[1, s], kv_recv.at[s, 0], where)

    spread = ({"sp": outer}, {"tp": sib}, {"grp": twin}, {"grp": twin, "tp": sib})

    def kv_forward(kind, owner):
        place = w_kv.at[half_rows(owner, g), :]
        return copy(place, place, kv_send.at[kind, owner], kv_recv.at[owner, g], spread[kind])

    def kv_arrival(owner, which):
        place = w_kv.at[half_rows(owner, which), :]
        return copy(place, place, kv_send.at[0, owner], kv_recv.at[owner, which], {"tp": sib})

    def q_copy(r, core):
        i = 2 * r + core
        src = q_own.at[span(g, part), i * LANES : (i + 1) * LANES]
        where = {"sp": 2 * c + r, "tp": 2 * x + core}
        return copy(src, w_q.at[half_rows(s, g), :], q_send.at[r, core], q_recv.at[s, g], where)

    def q_beside():
        src = q_own.at[:, span(theirs, LANES)]
        return copy(src, w_q.at[span(s, shard), :], q_sib.at[0], q_recv.at[s, 0], {"tp": sib})

    def q_forward(owner):
        place = w_q.at[half_rows(owner, g), :]
        return copy(place, place, q_twin.at[owner], q_recv.at[owner, g], {"grp": twin})

    def q_arrival(owner, which):
        place = w_q.at[half_rows(owner, which), :]
        return copy(place, place, q_twin.at[owner], q_recv.at[owner, which], {"grp": twin})

    def par_copy():
        return copy(par_own, par_in, par_sem.at[0], par_sem.at[1], {"tp": sib})

    def sides(k, act):
        @pl.when(s >= k)
        def _():
            act(s - k, True, s < count - 1)

        @pl.when(s + k < count)
        def _():
            act(s + k, False, s > 0)

    def both_ways(act):
        @pl.when(s < count - 1)
        def _():
            act(True)

        @pl.when(s > 0)
        def _():
            act(False)

    def each_q(act):
        for r in range(2):

            @pl.when(2 * c + r != s)
            def _():
                for core in range(2):
                    act(r, core)

    local[0].wait()
    step = rows // 2

    def norm_rows(i, carry):
        at = pl.ds(pl.multiple_of(i * step, step), step)
        v = tok_own[at, :].astype(f32)
        scale = lax.rsqrt(jnp.mean(v * v, axis=-1, keepdims=True) + epsilon)
        to = pl.ds(pl.multiple_of(s * rows + i * step, step), step)
        norm_all[to, :] = (v * scale * gain[...]).astype(bf16)
        return carry

    lax.fori_loop(0, rows // step, norm_rows, 0)
    pl.semaphore_wait(barrier, len(greeted))
    both_ways(lambda up: z_copy(s, up).start())
    local[1].wait()
    local[2].wait()
    kv_first().start()
    local[3].wait()

    @pl.when(in_half)
    def _():
        kv_beside().start()
        q_beside().start()

    par_copy().start()

    @pl.when(jnp.logical_not(inner))
    def _():
        each_q(lambda r, core: q_copy(r, core).start())

    def z_tok(owner, up, more):
        z_copy(owner, True).wait_recv()

        @pl.when(more)
        def _():
            z_copy(owner, up).start()

        tok_forward(1, owner).start()
        tok_forward(0, owner).start()

    def x_tok(owner, up, more):
        tok_forward(1, owner).wait_recv()
        tok_forward(2, owner).start()

    def relays(owner):
        return inner & (owner // 2 != half)

    def z_kv(owner, up, more):
        @pl.when(in_half)
        def _():
            kv_arrival(owner, g).wait_recv()

            @pl.when(relays(owner))
            def _():
                kv_forward(0, owner).start()

            for kind in (2, 3, 1):
                kv_forward(kind, owner).start()

    def z_q(owner, up, more):
        q_arrival(owner, g).wait_recv()
        q_forward(owner).start()

    last = count - 1
    for k in range(1, count):
        sides(k, z_tok)
        if k > 1:
            sides(k - 1, x_tok)
        sides(k, z_kv)
        if k == 2:

            @pl.when(inner)
            def _():
                each_q(lambda r, core: q_copy(r, core).start())

    for k in range(1, count):
        sides(k, z_q)
    sides(last, x_tok)

    def tok_rest(owner, up, more):
        tok_forward(0, owner).wait_recv()
        tok_forward(2, owner).wait_recv()

    for k in range(1, count):
        sides(k, tok_rest)

    seq = rows * count
    group = wpo.shape[0]
    window = jnp.where(t == 0, 2, jnp.where(t == 1, 4, jnp.where(t == 2, 8, 16)))
    half_span = window // 2

    def pool(b, carry):
        at = b * rows + lax.broadcasted_iota(jnp.int32, (rows, seq), 0)
        col = lax.broadcasted_iota(jnp.int32, (rows, seq), 1)
        inside = (col >= at - half_span) & (col < at + window - half_span)
        band = jnp.where(inside, 1.0, 0.0).astype(bf16)
        total = jnp.dot(band, norm_all[:, span(t, group)], preferred_element_type=f32)
        pos = b * rows + lax.broadcasted_iota(jnp.int32, (rows, 1), 0)
        low = jnp.maximum(pos - half_span, 0)
        high = jnp.minimum(pos + window - half_span, seq)
        own = norm_all[span(b, rows), span(t, group)].astype(f32)
        pooled_all[span(b, rows), :] = (total / (high - low).astype(f32) - own).astype(bf16)
        return carry

    lax.fori_loop(0, count, pool, 0)

    def rest_kv(owner, up, more):
        @pl.when(jnp.logical_not(in_half))
        def _():
            kv_arrival(owner, g).wait_recv()

        kv_arrival(owner, twin).wait_recv()

    for k in range(1, count):
        sides(k, rest_kv)

    @pl.when(in_half)
    def _():
        for piece in own_local:
            piece.wait()

    @pl.when(jnp.logical_not(in_half))
    def _():
        kv_beside().wait_recv()
        q_beside().wait_recv()

    def project_kv(b, carry):
        acc = jnp.dot(norm_all[span(b, rows), :], w_kv[...], preferred_element_type=f32)
        k_all[span(b, rows), :] = acc[:, 0:LANES].astype(bf16)
        v_all[span(b, rows), :] = acc[:, LANES : 2 * LANES].astype(bf16)
        return carry

    lax.fori_loop(0, count, project_kv, 0)

    def rest_q(owner, up, more):
        q_arrival(owner, twin).wait_recv()

    for k in range(1, count):
        sides(k, rest_q)

    def project_q(b, carry):
        acc = jnp.dot(norm_all[span(b, rows), :], w_q[...], preferred_element_type=f32)
        q_all[span(b, rows), :] = acc.astype(bf16)
        return carry

    lax.fori_loop(0, count, project_q, 0)

    par_copy().wait_recv()
    par_use[...] = jnp.where(in_half, par_own[...], par_in[...])

    head_where = ({"sp": mate, "tp": home}, {"sp": beyond, "tp": home}, {"tp": sib})

    def head_copy(kind, b):
        src = head_own.at[span(b, rows), :]
        dst = heads_all.at[span(b, rows), span(mine, LANES)]
        return copy(src, dst, h_send.at[kind, b], h_recv.at[b, mine], head_where[kind])

    def head_forward(b, i):
        place = heads_all.at[span(b, rows), i * LANES : (i + 1) * LANES]
        return copy(place, place, h_fwd.at[b, i], h_recv.at[b, i], {"sp": outer})

    def lt_copy(b):
        where = {"sp": b, "tp": home}
        return copy(lt_send.at[b], lt_in.at[mine], l_send.at[b], l_recv.at[mine], where)

    def lt_arrival(i):
        return copy(lt_send.at[0], lt_in.at[i], l_send.at[0], l_recv.at[i], {"tp": sib})

    lane = lax.broadcasted_iota(jnp.int32, (rows, LANES), 1)
    lt_rows = lt_send.shape[2]
    base = HD ** (-0.5)

    def attend(b, carry):
        q = q_all[span(b, rows), :]
        zero = jnp.zeros_like(q)
        both_q = jnp.concatenate([jnp.where(lane < HD, q, zero), jnp.where(lane < HD, zero, q)], axis=0)
        raw = lax.dot_general(
            both_q, k_all[...], (((1,), (1,)), ((), ())), preferred_element_type=f32
        )
        highest = jnp.max(raw, axis=-1, keepdims=True)
        weights = jnp.exp2((raw - highest) * (base * math.log2(math.e)))
        totals = jnp.sum(weights, axis=-1, keepdims=True)
        reads = jnp.dot(weights.astype(bf16), v_all[...], preferred_element_type=f32) / totals
        logs = highest * base + jnp.log(totals)
        contrast = reads[:rows] - par_use[pl.ds(count + mine, 1), :] * reads[rows:]
        scaled = (
            contrast
            * lax.rsqrt(jnp.mean(contrast * contrast, axis=-1, keepdims=True) + epsilon)
            * par_use[pl.ds(mine, 1), :]
        ).astype(bf16)
        head_own[span(b, rows), :] = scaled

        @pl.when(in_half)
        def _():
            heads_all[span(b, rows), span(mine, LANES)] = scaled

        head_copy(1, b).start()
        head_copy(0, b).start()

        @pl.when(jnp.logical_not(in_half))
        def _():
            head_copy(2, b).start()

        both = jnp.where(lane == 0, logs[:rows], logs[rows:])
        padded = jnp.concatenate([both, jnp.zeros((lt_rows - rows, LANES), f32)], axis=0)
        lt_send[b] = jnp.transpose(padded)[0:8, :]

        @pl.when(jnp.logical_not(in_half & (b == s)))
        def _():
            lt_copy(b).start()

        return carry

    lax.fori_loop(0, count, attend, 0)

    local[4].wait()
    local[5].wait()
    sub = rows // 4
    is_relay = inner & jnp.logical_not(in_half)

    def part_copy(b):
        where = {"tp": sib}
        return copy(part_out.at[b, 1 - c], part_in.at[b], p_send.at[b], p_recv.at[b], where)

    def cross_copy(b):
        return copy(cross_out.at[b], cross_in.at[b], x_send.at[b], x_recv.at[b], {"tp": far})

    def out_copy(b):
        return copy(block_out.at[b], block_in.at[s], o_send.at[b], o_recv.at[s], {"sp": b})

    def first_sum(b):
        for i in range(count):

            @pl.when(jnp.logical_not(in_half & (mine == i)))
            def _():
                head_forward(b, i).wait_recv()

            @pl.when(is_relay)
            def _():
                head_forward(b, i).start()

        total = jnp.dot(heads_all[span(b, rows), :], wao_in[...], preferred_element_type=f32)
        total = total + jnp.dot(
            pooled_all[span(b, rows), :], wpo_in[...], preferred_element_type=f32
        )
        for j in range(4):
            part_out[b, j % 2, j // 2] = total[j * sub : (j + 1) * sub, :].astype(bf16)
        part_copy(b).start()

    def second_sum(b):
        part_copy(b).wait_recv()
        cross_out[b] = (
            part_out[b, c, 1 - x].astype(f32) + part_in[b, 1 - x].astype(f32)
        ).astype(bf16)
        cross_copy(b).start()

    def third_sum(b):
        cross_copy(b).wait_recv()
        block_out[b] = (
            part_out[b, c, x].astype(f32)
            + part_in[b, x].astype(f32)
            + cross_in[b].astype(f32)
        ).astype(bf16)

        @pl.when(b != s)
        def _():
            out_copy(b).start()

    def outward(b, carry):
        first_sum(b)
        second_sum(b)

        @pl.when(b > 0)
        def _():
            third_sum(b - 1)

        return carry

    lax.fori_loop(0, count, outward, 0)
    third_sum(count - 1)

    def put_logs(i, ref, at):
        for m in range(2):
            lt_out[m, i : i + 1, :] = ref[at, m : m + 1, 0:rows]

    for i in range(count):

        @pl.when(in_half & (mine == i))
        def _():
            put_logs(i, lt_send, s)

        @pl.when(jnp.logical_not(in_half & (mine == i)))
        def _():
            lt_arrival(i).wait_recv()
            put_logs(i, lt_in, i)

    for b in range(count):
        cols = slice(b * group, (b + 1) * group)

        @pl.when(s == b)
        def _():
            mixed_out[:, cols] = block_out[b]

        @pl.when(s != b)
        def _():
            where = {"sp": b}
            copy(block_out.at[s], block_in.at[b], o_send.at[s], o_recv.at[b], where).wait_recv()
            mixed_out[:, cols] = block_in[b]
            out_copy(b).wait_send()

        @pl.when(jnp.logical_not(in_half & (s == b)))
        def _():
            lt_copy(b).wait_send()

    both_ways(lambda up: z_copy(s, up).wait_send())
    kv_first().wait_send()
    par_copy().wait_send()
    each_q(lambda r, core: q_copy(r, core).wait_send())

    @pl.when(in_half)
    def _():
        kv_beside().wait_send()
        q_beside().wait_send()

    def sent(owner, up, more):
        @pl.when(more)
        def _():
            z_copy(owner, up).wait_send()

        for step in range(3):
            tok_forward(step, owner).wait_send()

        @pl.when(in_half)
        def _():
            @pl.when(relays(owner))
            def _():
                kv_forward(0, owner).wait_send()

            for kind in (1, 2, 3):
                kv_forward(kind, owner).wait_send()

        q_forward(owner).wait_send()

    for k in range(1, count):
        sides(k, sent)

    def drain(b, carry):
        head_copy(0, b).wait_send()
        head_copy(1, b).wait_send()

        @pl.when(jnp.logical_not(in_half))
        def _():
            head_copy(2, b).wait_send()

        @pl.when(is_relay)
        def _():
            for i in range(count):
                head_forward(b, i).wait_send()

        part_copy(b).wait_send()
        cross_copy(b).wait_send()
        return carry

    lax.fori_loop(0, count, drain, 0)


def fused(
    count,
    tokens,
    norm_gain,
    query_weight,
    key_weight,
    value_weight,
    map_lambda,
    head_gain,
    attn_out_weight,
    pool_out_weight,
):
    rows, width = tokens.shape
    cols = attn_out_weight.shape[1]
    shard = query_weight.shape[0]
    sub = rows // 4
    seq = rows * count
    lt_rows = -(-rows // LANES) * LANES
    bf16, f32 = jnp.bfloat16, jnp.float32
    vmem = pl.BlockSpec(memory_space=pltpu.VMEM)
    smem = pl.BlockSpec(memory_space=pltpu.SMEM)
    far = pl.BlockSpec(memory_space=pl.ANY)
    sems = pltpu.SemaphoreType.DMA
    return pl.pallas_call(
        functools.partial(fused_kernel, count),
        out_shape=(
            jax.ShapeDtypeStruct((sub, width), bf16),
            jax.ShapeDtypeStruct((2, count, rows), f32),
        ),
        in_specs=[far, vmem, far, far, far, smem, vmem, far, far],
        out_specs=(vmem, vmem),
        scratch_shapes=[
            pltpu.VMEM((rows, width), bf16),
            pltpu.VMEM((seq, width), bf16),
            pltpu.VMEM((shard, 2 * LANES), bf16),
            pltpu.VMEM((shard, count * LANES), bf16),
            pltpu.VMEM((width, 2 * LANES), bf16),
            pltpu.VMEM((width, LANES), bf16),
            pltpu.VMEM((2 * count, LANES), f32),
            pltpu.VMEM((2 * count, LANES), f32),
            pltpu.VMEM((2 * count, LANES), f32),
            pltpu.VMEM((seq, LANES), bf16),
            pltpu.VMEM((seq, LANES), bf16),
            pltpu.VMEM((seq, LANES), bf16),
            pltpu.VMEM((seq, LANES), bf16),
            pltpu.VMEM((seq, count * LANES), bf16),
            pltpu.VMEM((seq, pool_out_weight.shape[0]), bf16),
            pltpu.VMEM((count, 2, 2, sub, cols), bf16),
            pltpu.VMEM((count, 2, sub, cols), bf16),
            pltpu.VMEM((count, sub, cols), bf16),
            pltpu.VMEM((count, sub, cols), bf16),
            pltpu.VMEM((count, sub, cols), bf16),
            pltpu.VMEM((count, sub, cols), bf16),
            pltpu.VMEM((count, 8, lt_rows), f32),
            pltpu.VMEM((count, 8, lt_rows), f32),
            pltpu.VMEM(attn_out_weight.shape, bf16),
            pltpu.VMEM(pool_out_weight.shape, bf16),
            sems((9,)),
            sems((count, 2)),
            sems((count,)),
            sems((3, count)),
            sems((3, count)),
            sems((4, count)),
            sems((count, 2)),
            sems((2, 2)),
            sems((1,)),
            sems((count,)),
            sems((count, 2)),
            sems((2,)),
            sems((3, count)),
            sems((count, count)),
            sems((count, count)),
            sems((count,)),
            sems((count,)),
            sems((count,)),
            sems((count,)),
            sems((count,)),
            sems((count,)),
            sems((count,)),
            sems((count,)),
        ],
        compiler_params=pltpu.CompilerParams(collective_id=0, has_side_effects=True),
    )(
        tokens,
        norm_gain.reshape(1, width),
        query_weight,
        key_weight,
        value_weight,
        map_lambda,
        head_gain,
        attn_out_weight,
        pool_out_weight,
    )


def fits(shape, tokens, query_weight, value_weight, map_lambda, pool_out_weight):
    count = shape["sp"]
    return (
        shape["grp"] == 2
        and shape["tp"] == 4
        and count == 4
        and map_lambda.shape[0] == count
        and value_weight.shape[1] == VD == LANES == 2 * HD
        and tokens.shape[0] % 32 == 0
        and tokens.shape[1] % (4 * LANES) == 0
        and query_weight.shape[0] % 32 == 0
        and query_weight.shape[1] == count * LANES
        and pool_out_weight.shape[0] * 4 == tokens.shape[1]
        and pool_out_weight.shape[1] % LANES == 0
        and pool_out_weight.shape[1] * count == tokens.shape[1]
        and pool_out_weight.shape[0] == pool_out_weight.shape[1]
        and tokens.shape[0] * count * tokens.shape[1] <= 1 << 22
    )


def solution(mesh):
    placed = (
        P(("grp", "sp"), None),
        P(),
        P("sp", "tp"),
        P("sp", "tp"),
        P("sp", "tp"),
        P("tp"),
        P("tp", None),
        P("tp", "sp"),
        P("tp", "sp"),
    )
    shape = dict(mesh.shape)

    def chosen(*args):
        if fits(shape, args[0], args[2], args[4], args[5], args[8]):
            return fused(shape["sp"], *args)
        return on_device(*args)

    return jax.shard_map(
        chosen,
        mesh=mesh,
        in_specs=placed,
        out_specs=(P(("grp", "sp", "tp"), None), P(None, "tp", ("grp", "sp"))),
        check_vma=False,
    )
```

```python
import functools
import math

import jax
import jax.numpy as jnp
from jax import lax
from jax.experimental import pallas as pl
from jax.experimental.pallas import tpu as pltpu
from jax.sharding import PartitionSpec as P

HD = 64
VD = 128
POOL_SPAN = 16


epsilon = 1e-06
very_low = -1e30


def extended(cells, sides, width):
    for axis, dim in sides:
        count = lax.axis_size(axis)
        ends = count - 1
        head = lax.slice_in_dim(cells, 0, width, axis=dim)
        tail = lax.slice_in_dim(cells, cells.shape[dim] - width, cells.shape[dim], axis=dim)
        cells = jnp.concatenate(
            [
                lax.ppermute(tail, axis, [(i, (i + 1) % count) for i in range(ends)]),
                cells,
                lax.ppermute(head, axis, [((i + 1) % count, i) for i in range(ends)]),
            ],
            axis=dim,
        )
    return cells


def add_products(totals, pieces, source):
    results = []
    for running, piece in zip(totals, pieces):
        results.append(jnp.dot(source, piece, preferred_element_type=jnp.float32))
    return tuple(results)


def on_device(
    tokens,
    norm_gain,
    query_weight,
    key_weight,
    value_weight,
    map_lambda,
    head_gain,
    attn_out_weight,
    pool_out_weight,
):
    tokens_wide = tokens.astype(jnp.float32)
    normed = (
        tokens_wide
        * lax.rsqrt(jnp.mean(tokens_wide * tokens_wide, axis=-1, keepdims=True) + epsilon)
        * norm_gain
    ).astype(jnp.bfloat16)
    row_count = normed.shape[0]
    sp_index = lax.axis_index("sp")
    tp_index = lax.axis_index("tp")
    group_width = pool_out_weight.shape[0]
    local_heads = map_lambda.shape[0]
    key_heads = value_weight.shape[1] // VD
    group_heads = local_heads // key_heads
    q_empty = jnp.zeros((row_count, query_weight.shape[1]), jnp.float32)
    k_empty = jnp.zeros((row_count, key_weight.shape[1]), jnp.float32)
    v_empty = jnp.zeros((row_count, value_weight.shape[1]), jnp.float32)
    q_acc, k_acc, v_acc = add_products(
        (q_empty, k_empty, v_empty),
        (
            lax.all_gather(query_weight, "sp", axis=0, tiled=True),
            lax.all_gather(key_weight, "sp", axis=0, tiled=True),
            lax.all_gather(value_weight, "sp", axis=0, tiled=True),
        ),
        normed,
    )
    queries = q_acc.astype(jnp.bfloat16).reshape(row_count, key_heads, group_heads, 2, HD)
    keys_flat = k_acc.astype(jnp.bfloat16)
    values_flat = v_acc.astype(jnp.bfloat16)

    def key_block(state_now, key_pair):
        maxima, totals, accums = state_now
        key_blk, val_blk = key_pair
        scores = jnp.einsum(
            "qhgmd,khmd->hgmqk", queries, key_blk, preferred_element_type=jnp.float32
        ) * HD ** (-0.5)
        highest = jnp.maximum(maxima, jnp.max(scores, axis=-1))
        factor = jnp.exp(maxima - highest)
        weights = jnp.exp(scores - highest[..., None])
        totals = totals * factor + jnp.sum(weights, axis=-1)
        accums = accums * factor[..., None] + jnp.einsum(
            "hgmqk,khe->hgmqe",
            weights.astype(jnp.bfloat16),
            val_blk,
            preferred_element_type=jnp.float32,
        )
        return ((highest, totals, accums), None)

    start_state = (
        jnp.full((key_heads, group_heads, 2, row_count), very_low, jnp.float32),
        jnp.zeros((key_heads, group_heads, 2, row_count), jnp.float32),
        jnp.zeros((key_heads, group_heads, 2, row_count, VD), jnp.float32),
    )
    key_piece = lax.all_gather(keys_flat, "sp", axis=0, tiled=True)
    val_piece = lax.all_gather(values_flat, "sp", axis=0, tiled=True)
    piece_len = key_piece.shape[0]
    block_len = math.gcd(piece_len, 512)
    key_blocks = key_piece.reshape(piece_len // block_len, block_len, key_heads, 2, HD)
    val_blocks = val_piece.reshape(piece_len // block_len, block_len, key_heads, VD)
    state_next, unused = lax.scan(key_block, start_state, (key_blocks, val_blocks))
    maxima, totals, accums = state_next
    log_parts = maxima + jnp.log(totals)
    log_totals = jnp.transpose(log_parts, (2, 0, 1, 3)).reshape(2, local_heads, row_count)
    reads = accums / totals[..., None]
    contrast = reads[:, :, 0] - map_lambda.reshape(key_heads, group_heads, 1, 1) * reads[:, :, 1]
    scaled = (
        contrast
        * lax.rsqrt(jnp.mean(contrast * contrast, axis=-1, keepdims=True) + epsilon)
        * head_gain.reshape(key_heads, group_heads, 1, VD)
    )
    attention_head_rows = (
        jnp.transpose(scaled, (2, 0, 1, 3))
        .reshape(row_count, local_heads * VD)
        .astype(jnp.bfloat16)
    )
    head_rows, log_totals = (attention_head_rows, log_totals)
    own_chan = lax.dynamic_slice_in_dim(normed, tp_index * group_width, group_width, 1)
    reach = POOL_SPAN // 2
    padded = extended(own_chan, (("sp", 0),), reach)
    window = jnp.left_shift(jnp.int32(2), tp_index)
    half_span = window // 2
    running = jnp.zeros((row_count, group_width), jnp.float32)
    for offset in range(POOL_SPAN):
        piece = lax.dynamic_slice_in_dim(padded, reach - half_span + offset, row_count, 0).astype(
            jnp.float32
        )
        running = running + jnp.where(offset < window, piece, 0.0)
    seq_len = row_count * lax.axis_size("sp")
    position = sp_index * row_count + jnp.arange(row_count, dtype=jnp.int32)
    lower_edge = jnp.clip(position - half_span, 0, seq_len)
    upper_edge = jnp.clip(position + window - half_span, 0, seq_len)
    counts_f = (upper_edge - lower_edge).astype(jnp.float32)[:, None]
    pooled = (running / counts_f - own_chan.astype(jnp.float32)).astype(jnp.bfloat16)
    attn_whole, pool_whole = (
        lax.all_gather(attn_out_weight, "sp", axis=1, tiled=True),
        lax.all_gather(pool_out_weight, "sp", axis=1, tiled=True),
    )
    mixed = lax.psum_scatter(
        (
            jnp.dot(head_rows, attn_whole, preferred_element_type=jnp.float32)
            + jnp.dot(pooled, pool_whole, preferred_element_type=jnp.float32)
        ).astype(jnp.bfloat16),
        "tp",
        scatter_dimension=0,
        tiled=True,
    )
    return (mixed, log_totals)


MESH = pl.DeviceIdType.MESH
LANES = 128
scope = jax.named_scope


def fused_kernel(
    count,
    tok,
    gain,
    wq,
    wk,
    wv,
    lam,
    hgain,
    wao,
    wpo,
    mixed_out,
    lt_out,
    tok_own,
    gain_own,
    lam_own,
    hgain_own,
    norm_all,
    kv_own,
    w_kv,
    w_q,
    wa_all,
    wp_all,
    par_own,
    par_in,
    par_use,
    q_all,
    k_all,
    v_all,
    head_own,
    heads_all,
    pooled_all,
    part_out,
    part_in,
    cross_out,
    cross_in,
    block_out,
    block_in,
    lt_send,
    lt_in,
    local_sem,
    z_send,
    z_recv,
    f_send,
    f_recv,
    kv_send,
    kv_fwd,
    kv_recv,
    q_send,
    q_twin,
    q_recv,
    w_send,
    w_fwd,
    w_recv,
    par_sem,
    h_send,
    h_recv,
    p_send,
    p_recv,
    x_send,
    x_recv,
    o_send,
    o_recv,
    l_send,
    l_recv,
):
    g = lax.axis_index("grp")
    s = lax.axis_index("sp")
    t = lax.axis_index("tp")
    c = lax.rem(t, 2)
    x = t // 2
    rows, width = tok.shape
    quarter = width // 4
    shard = wq.shape[0]
    part = shard // 2
    pair = 2 * LANES
    group = wpo.shape[0]
    cols = wpo.shape[1]
    half = s // 2
    inner = (s > 0) & (s < count - 1)
    at_home = inner & (c == half)
    away = inner & (c != half)
    sib = t + 1 - 2 * c
    far = lax.rem(t + 2, 4)
    twin = 1 - g
    near = 1 + half
    other = count - 1 - s
    edge = jnp.where(half == 0, 0, count - 1)
    far_edge = count - 1 - edge
    target = 1 + c
    home = 2 * x + half
    f32, bf16 = jnp.float32, jnp.bfloat16

    def span(index, size):
        return pl.ds(pl.multiple_of(index * size, size), size)

    def half_rows(owner, which):
        return pl.ds(pl.multiple_of(owner * shard + which * part, part), part)

    barrier = pltpu.get_barrier_semaphore()

    def greet(where):
        pl.semaphore_signal(barrier, inc=1, device_id=where, device_id_type=MESH)

    for off in range(1, count):
        peer = lax.rem(s + off, count)
        peer_inner = (peer > 0) & (peer < count - 1)

        @pl.when(inner | peer_inner)
        def _():
            greet({"sp": peer})
            greet({"sp": peer, "tp": sib})

    @pl.when(inner)
    def _():
        greet({"tp": sib})
        greet({"tp": far})
        greet({"grp": twin})

    pieces = (
        (tok, tok_own),
        (gain, gain_own),
        (wk, kv_own.at[:, 0:LANES]),
        (wv, kv_own.at[:, LANES:pair]),
        (lam, lam_own),
        (hgain, hgain_own),
        (wao, wa_all.at[:, span(lax.rem(s, 2), cols)]),
        (wpo, wp_all.at[:, span(lax.rem(s, 2), cols)]),
        (wk, w_kv.at[span(s, shard), 0:LANES]),
        (wv, w_kv.at[span(s, shard), LANES:pair]),
        (wq.at[:, span(c, pair)], w_q.at[span(s, shard), :]),
    )
    local = [
        pltpu.make_async_copy(src, dst, local_sem.at[i]) for i, (src, dst) in enumerate(pieces)
    ]
    for piece in local[:4]:
        piece.start()

    @pl.when(inner)
    def _():
        for piece in local[4:8]:
            piece.start()

    @pl.when(at_home)
    def _():
        for piece in local[8:]:
            piece.start()

    def copy(src, dst, send, recv, where):
        return pltpu.make_async_remote_copy(
            src_ref=src,
            dst_ref=dst,
            send_sem=send,
            recv_sem=recv,
            device_id=where,
            device_id_type=MESH,
        )

    def z_copy(owner, dest):
        place = norm_all.at[span(owner, rows), span(t, quarter)]
        return copy(place, place, z_send.at[owner], z_recv.at[owner], {"sp": dest})

    def tok_forward(step, owner):
        col = span(far if step == 2 else t, quarter)
        place = norm_all.at[span(owner, rows), col]
        where = {"tp": far if step == 1 else sib}
        return copy(place, place, f_send.at[step, owner], f_recv.at[step, owner], where)

    def kv_first():
        src = kv_own.at[span(g, part), :]
        dst = w_kv.at[half_rows(s, g), :]
        return copy(src, dst, kv_send.at[0], kv_recv.at[s, g], {"sp": target})

    def kv_beside():
        dst = w_kv.at[span(s, shard), :]
        return copy(kv_own, dst, kv_send.at[1], kv_recv.at[s, 0], {"tp": sib})

    def kv_forward(kind, owner):
        which = twin if kind == 2 else g
        place = w_kv.at[half_rows(owner, which), :]
        where = {"grp": twin} if kind == 0 else {"tp": sib}
        return copy(place, place, kv_fwd.at[kind, owner], kv_recv.at[owner, which], where)

    def kv_arrival(owner, which):
        place = w_kv.at[half_rows(owner, which), :]
        return copy(place, place, kv_fwd.at[0, owner], kv_recv.at[owner, which], {"tp": sib})

    def q_copy(core):
        src = wq.at[span(g, part), core * pair : (core + 1) * pair]
        dst = w_q.at[half_rows(s, g), :]
        where = {"sp": target, "tp": 2 * x + core}
        return copy(src, dst, q_send.at[core], q_recv.at[s, g], where)

    def q_beside():
        src = wq.at[:, span(1 - c, pair)]
        return copy(src, w_q.at[span(s, shard), :], q_send.at[2], q_recv.at[s, 0], {"tp": sib})

    def q_forward(owner):
        place = w_q.at[half_rows(owner, g), :]
        return copy(place, place, q_twin.at[owner], q_recv.at[owner, g], {"grp": twin})

    def q_arrival(owner, which):
        place = w_q.at[half_rows(owner, which), :]
        return copy(place, place, q_twin.at[owner], q_recv.at[owner, which], {"grp": twin})

    stores = (wa_all, wp_all)

    def w_copy(kind):
        src = (wao, wpo)[kind].at[span(g, part), :]
        dst = stores[kind].at[span(g, part), span(lax.rem(s, 2), cols)]
        return copy(src, dst, w_send.at[kind], w_recv.at[kind, g], {"sp": near})

    def w_forward(kind):
        place = stores[kind].at[span(g, part), span(lax.rem(edge, 2), cols)]
        return copy(place, place, w_fwd.at[kind], w_recv.at[kind, g], {"grp": twin})

    def w_arrival(kind, which):
        place = stores[kind].at[span(which, part), span(lax.rem(edge, 2), cols)]
        return copy(place, place, w_fwd.at[kind], w_recv.at[kind, which], {"grp": twin})

    def par_copy():
        return copy(par_own, par_in, par_sem.at[0], par_sem.at[1], {"tp": sib})

    head_where = ({"sp": other, "tp": home}, {"tp": sib})

    def head_copy(kind, b, h):
        src = head_own.at[span(b, rows), span(h, LANES)]
        dst = heads_all.at[span(b, rows), span(2 * c + h, LANES)]
        return copy(src, dst, h_send.at[kind, b, h], h_recv.at[b, 2 * c + h], head_where[kind])

    def head_arrival(b, i):
        place = heads_all.at[span(b, rows), i * LANES : (i + 1) * LANES]
        return copy(place, place, h_send.at[0, b, 0], h_recv.at[b, i], {"tp": sib})

    def lt_copy(b):
        where = {"sp": b, "tp": home}
        return copy(lt_send.at[b], lt_in.at[c], l_send.at[b], l_recv.at[c], where)

    def lt_arrival(core):
        return copy(lt_send.at[0], lt_in.at[core], l_send.at[0], l_recv.at[core], {"tp": sib})

    def part_copy(b, e):
        src = part_out.at[b, e, 1 - c]
        return copy(src, part_in.at[b, e], p_send.at[b, e], p_recv.at[b, e], {"tp": sib})

    def cross_copy(b, e):
        src = cross_out.at[b, e]
        return copy(src, cross_in.at[b, e], x_send.at[b, e], x_recv.at[b, e], {"tp": far})

    def out_copy(b, e):
        to = 2 * half + e
        return copy(block_out.at[b, e], block_in.at[to], o_send.at[b, e], o_recv.at[to], {"sp": b})

    def out_arrival(i):
        return copy(block_out.at[0, 0], block_in.at[i], o_send.at[0, 0], o_recv.at[i], {"sp": near})

    local[0].wait()
    local[1].wait()
    step = rows // 2

    def norm_rows(i, carry):
        at = pl.ds(pl.multiple_of(i * step, step), step)
        v = tok_own[at, :].astype(f32)
        scale = lax.rsqrt(jnp.mean(v * v, axis=-1, keepdims=True) + epsilon)
        to = pl.ds(pl.multiple_of(s * rows + i * step, step), step)
        norm_all[to, :] = (v * scale * gain_own[...]).astype(bf16)
        return carry

    with scope("norm"):
        lax.fori_loop(0, rows // step, norm_rows, 0)
    with scope("barrier"):
        pl.semaphore_wait(barrier, jnp.where(inner, 9, 4))
    sends_on = s != target

    @pl.when(inner)
    def _():
        z_copy(s, other).start()

    @pl.when(jnp.logical_not(inner))
    def _():
        z_copy(s, near).start()

    local[2].wait()
    local[3].wait()

    @pl.when(sends_on)
    def _():
        kv_first().start()

    def outer_work():
        for core in range(2):
            q_copy(core).start()
        for kind in range(2):
            w_copy(kind).start()

    pl.when(jnp.logical_not(inner))(outer_work)

    def inner_work():
        @pl.when(at_home)
        def _():
            kv_beside().start()
            q_beside().start()

        local[4].wait()
        local[5].wait()
        par_own[0:count, :] = hgain_own[...]
        for i in range(count):
            par_own[count + i : count + i + 1, :] = jnp.full((1, LANES), lam_own[i], f32)

        @pl.when(at_home)
        def _():
            par_copy().start()

        def tok_in(owner, onward):
            z_copy(owner, other).wait_recv()
            if onward:
                z_copy(owner, other).start()
            tok_forward(1, owner).start()
            tok_forward(0, owner).start()

        def tok_x(owner):
            tok_forward(1, owner).wait_recv()
            tok_forward(2, owner).start()

        def kv_in(owner):
            @pl.when(at_home)
            def _():
                kv_arrival(owner, g).wait_recv()
                kv_forward(0, owner).start()
                kv_forward(1, owner).start()

        def kv_y(owner):
            @pl.when(at_home)
            def _():
                kv_arrival(owner, twin).wait_recv()
                kv_forward(2, owner).start()

        def q_in(owner):
            q_arrival(owner, g).wait_recv()
            q_forward(owner).start()

        owners = (edge, other, far_edge)
        with scope("tok0"):
            tok_in(edge, True)

        @pl.when(away)
        def _():
            for core in range(2):
                q_copy(core).start()

        with scope("tok1"):
            tok_in(other, False)
        with scope("kv0"):
            kv_in(edge)
        with scope("kv1"):
            kv_in(other)
        with scope("q0"):
            q_in(edge)
        with scope("x0"):
            tok_x(edge)
        with scope("x1"):
            tok_x(other)
        with scope("tok2"):
            tok_in(far_edge, False)
        with scope("kv2"):
            kv_in(far_edge)
        with scope("q1"):
            q_in(other)
        with scope("q2"):
            q_in(far_edge)
        with scope("kvy"):
            for owner in owners:
                kv_y(owner)
        with scope("x2"):
            tok_x(far_edge)
        with scope("rest"):
            for owner in owners:
                tok_forward(0, owner).wait_recv()
                tok_forward(2, owner).wait_recv()

        seq = rows * count
        window = jnp.where(t == 0, 2, jnp.where(t == 1, 4, jnp.where(t == 2, 8, 16)))
        half_span = window // 2

        def pool(b, carry):
            at = b * rows + lax.broadcasted_iota(jnp.int32, (rows, seq), 0)
            col = lax.broadcasted_iota(jnp.int32, (rows, seq), 1)
            inside = (col >= at - half_span) & (col < at + window - half_span)
            band = jnp.where(inside, 1.0, 0.0).astype(bf16)
            total = jnp.dot(band, norm_all[:, span(t, group)], preferred_element_type=f32)
            pos = b * rows + lax.broadcasted_iota(jnp.int32, (rows, 1), 0)
            low = jnp.maximum(pos - half_span, 0)
            high = jnp.minimum(pos + window - half_span, seq)
            own = norm_all[span(b, rows), span(t, group)].astype(f32)
            pooled_all[span(b, rows), :] = (total / (high - low).astype(f32) - own).astype(bf16)
            return carry

        with scope("pool"):
            lax.fori_loop(0, count, pool, 0)

        with scope("kvrest"):

            @pl.when(at_home)
            def _():
                local[8].wait()
                local[9].wait()
                local[10].wait()

            @pl.when(away)
            def _():
                for owner in owners:
                    kv_arrival(owner, g).wait_recv()
                    kv_arrival(owner, twin).wait_recv()
                kv_beside().wait_recv()
                q_beside().wait_recv()
                par_copy().wait_recv()

        def project_kv(b, carry):
            acc = jnp.dot(norm_all[span(b, rows), :], w_kv[...], preferred_element_type=f32)
            k_all[span(b, rows), :] = acc[:, 0:LANES].astype(bf16)
            v_all[span(b, rows), :] = acc[:, LANES:pair].astype(bf16)
            return carry

        with scope("projkv"):
            lax.fori_loop(0, count, project_kv, 0)

        with scope("qrest"):
            for owner in owners:
                q_arrival(owner, twin).wait_recv()

        def project_q(b, carry):
            acc = jnp.dot(norm_all[span(b, rows), :], w_q[...], preferred_element_type=f32)
            q_all[span(b, rows), :] = acc.astype(bf16)
            return carry

        with scope("projq"):
            lax.fori_loop(0, count, project_q, 0)

        with scope("wao"):
            w_arrival(0, g).wait_recv()
            w_forward(0).start()

        par_use[...] = jnp.where(at_home, par_own[...], par_in[...])
        lane = lax.broadcasted_iota(jnp.int32, (rows, LANES), 1)
        lt_rows = lt_send.shape[3]
        base = HD ** (-0.5)

        def attend(n, carry):
            b = n // 2
            h = lax.rem(n, 2)
            head = 2 * c + h
            q = q_all[span(b, rows), span(h, LANES)]
            zero = jnp.zeros_like(q)
            both_q = jnp.concatenate(
                [jnp.where(lane < HD, q, zero), jnp.where(lane < HD, zero, q)], axis=0
            )
            raw = lax.dot_general(
                both_q, k_all[...], (((1,), (1,)), ((), ())), preferred_element_type=f32
            )
            highest = jnp.max(raw, axis=-1, keepdims=True)
            weights = jnp.exp2((raw - highest) * (base * math.log2(math.e)))
            totals = jnp.sum(weights, axis=-1, keepdims=True)
            reads = jnp.dot(weights.astype(bf16), v_all[...], preferred_element_type=f32) / totals
            logs = highest * base + jnp.log(totals)
            contrast = reads[:rows] - par_use[pl.ds(count + head, 1), :] * reads[rows:]
            scaled = (
                contrast
                * lax.rsqrt(jnp.mean(contrast * contrast, axis=-1, keepdims=True) + epsilon)
                * par_use[pl.ds(head, 1), :]
            ).astype(bf16)
            head_own[span(b, rows), span(h, LANES)] = scaled

            @pl.when(at_home)
            def _():
                heads_all[span(b, rows), span(head, LANES)] = scaled

            head_copy(0, b, h).start()

            @pl.when(away)
            def _():
                head_copy(1, b, h).start()

            both = jnp.where(lane == 0, logs[:rows], logs[rows:])
            padded = jnp.concatenate([both, jnp.zeros((lt_rows - rows, LANES), f32)], axis=0)
            lt_send[b, h] = jnp.transpose(padded)[0:8, :]

            @pl.when((h == 1) & jnp.logical_not(at_home & (b == s)))
            def _():
                lt_copy(b).start()

            @pl.when(n == 3)
            def _():
                w_arrival(1, g).wait_recv()
                w_forward(1).start()

            return carry

        with scope("attend"):
            lax.fori_loop(0, 2 * count, attend, 0)

        sub = rows // 4
        with scope("wrest"):
            local[6].wait()
            local[7].wait()
            w_arrival(0, twin).wait_recv()
            w_arrival(1, twin).wait_recv()

        def first_sum(b, e):
            @pl.when(e == 0)
            def _():
                for i in range(count):

                    @pl.when(jnp.logical_not(at_home & (i // 2 == c)))
                    def _():
                        head_arrival(b, i).wait_recv()

            at = span(e, cols)
            total = jnp.dot(heads_all[span(b, rows), :], wa_all[:, at], preferred_element_type=f32)
            total = total + jnp.dot(
                pooled_all[span(b, rows), :], wp_all[:, at], preferred_element_type=f32
            )
            for j in range(4):
                part_out[b, e, j % 2, j // 2] = total[j * sub : (j + 1) * sub, :].astype(bf16)
            part_copy(b, e).start()

        def second_sum(b, e):
            part_copy(b, e).wait_recv()
            cross_out[b, e] = (
                part_out[b, e, c, 1 - x].astype(f32) + part_in[b, e, 1 - x].astype(f32)
            ).astype(bf16)
            cross_copy(b, e).start()

        def third_sum(b, e):
            cross_copy(b, e).wait_recv()
            block_out[b, e] = (
                part_out[b, e, c, x].astype(f32)
                + part_in[b, e, x].astype(f32)
                + cross_in[b, e].astype(f32)
            ).astype(bf16)

            @pl.when(b != s)
            def _():
                out_copy(b, e).start()

        def outward(n, carry):
            with scope("S1"):
                first_sum(n // 2, lax.rem(n, 2))
            with scope("S2"):
                second_sum(n // 2, lax.rem(n, 2))

            @pl.when(n > 0)
            def _():
                with scope("S3"):
                    third_sum((n - 1) // 2, lax.rem(n - 1, 2))

            return carry

        lax.fori_loop(0, 2 * count, outward, 0)
        with scope("S3last"):
            third_sum(count - 1, 1)

    pl.when(inner)(inner_work)

    def put_logs(core, ref, at):
        for h in range(2):
            for m in range(2):
                i = 2 * core + h
                lt_out[m, i : i + 1, :] = ref[at, h, m : m + 1, 0:rows]

    for core in range(2):

        @pl.when(at_home & (c == core))
        def _():
            put_logs(core, lt_send, s)

        @pl.when(jnp.logical_not(at_home & (c == core)))
        def _():
            lt_arrival(core).wait_recv()
            put_logs(core, lt_in, core)

    for i in range(count):
        with scope(f"final{i}"):
            at = slice(i * cols, (i + 1) * cols)

            @pl.when(s == 1 + i // 2)
            def _():
                mixed_out[:, at] = block_out[s, i % 2]

            @pl.when(s != 1 + i // 2)
            def _():
                out_arrival(i).wait_recv()
                mixed_out[:, at] = block_in[i]

    @pl.when(sends_on)
    def _():
        kv_first().wait_send()
        for core in range(2):
            q_copy(core).wait_send()

    @pl.when(jnp.logical_not(inner))
    def _():
        z_copy(s, near).wait_send()
        for kind in range(2):
            w_copy(kind).wait_send()

    @pl.when(at_home)
    def _():
        kv_beside().wait_send()
        q_beside().wait_send()
        par_copy().wait_send()
        for owner in (edge, other, far_edge):
            for kind in range(3):
                kv_forward(kind, owner).wait_send()

    @pl.when(inner)
    def _():
        z_copy(s, other).wait_send()
        z_copy(edge, other).wait_send()
        for owner in (edge, other, far_edge):
            for step in range(3):
                tok_forward(step, owner).wait_send()
            q_forward(owner).wait_send()
        for kind in range(2):
            w_forward(kind).wait_send()

        def drain(b, carry):
            for h in range(2):
                head_copy(0, b, h).wait_send()

                @pl.when(away)
                def _():
                    head_copy(1, b, h).wait_send()

                part_copy(b, h).wait_send()
                cross_copy(b, h).wait_send()

                @pl.when(b != s)
                def _():
                    out_copy(b, h).wait_send()

            @pl.when(jnp.logical_not(at_home & (b == s)))
            def _():
                lt_copy(b).wait_send()

            return carry

        lax.fori_loop(0, count, drain, 0)


def fused(
    count,
    tokens,
    norm_gain,
    query_weight,
    key_weight,
    value_weight,
    map_lambda,
    head_gain,
    attn_out_weight,
    pool_out_weight,
):
    rows, width = tokens.shape
    group, cols = pool_out_weight.shape
    shard = query_weight.shape[0]
    sub = rows // 4
    seq = rows * count
    pair = 2 * LANES
    lt_rows = -(-rows // LANES) * LANES
    bf16, f32 = jnp.bfloat16, jnp.float32
    vmem = pl.BlockSpec(memory_space=pltpu.VMEM)
    far = pl.BlockSpec(memory_space=pl.ANY)
    sems = pltpu.SemaphoreType.DMA
    return pl.pallas_call(
        functools.partial(fused_kernel, count),
        out_shape=(
            jax.ShapeDtypeStruct((sub, width), bf16),
            jax.ShapeDtypeStruct((2, count, rows), f32),
        ),
        in_specs=[far] * 9,
        out_specs=(vmem, vmem),
        scratch_shapes=[
            pltpu.VMEM((rows, width), bf16),
            pltpu.VMEM((1, width), f32),
            pltpu.SMEM((count,), f32),
            pltpu.VMEM((count, LANES), f32),
            pltpu.VMEM((seq, width), bf16),
            pltpu.VMEM((shard, pair), bf16),
            pltpu.VMEM((width, pair), bf16),
            pltpu.VMEM((width, pair), bf16),
            pltpu.VMEM((group, 2 * cols), bf16),
            pltpu.VMEM((group, 2 * cols), bf16),
            pltpu.VMEM((2 * count, LANES), f32),
            pltpu.VMEM((2 * count, LANES), f32),
            pltpu.VMEM((2 * count, LANES), f32),
            pltpu.VMEM((seq, pair), bf16),
            pltpu.VMEM((seq, LANES), bf16),
            pltpu.VMEM((seq, LANES), bf16),
            pltpu.VMEM((seq, pair), bf16),
            pltpu.VMEM((seq, count * LANES), bf16),
            pltpu.VMEM((seq, group), bf16),
            pltpu.VMEM((count, 2, 2, 2, sub, cols), bf16),
            pltpu.VMEM((count, 2, 2, sub, cols), bf16),
            pltpu.VMEM((count, 2, sub, cols), bf16),
            pltpu.VMEM((count, 2, sub, cols), bf16),
            pltpu.VMEM((count, 2, sub, cols), bf16),
            pltpu.VMEM((count, sub, cols), bf16),
            pltpu.VMEM((count, 2, 8, lt_rows), f32),
            pltpu.VMEM((2, 2, 8, lt_rows), f32),
            sems((11,)),
            sems((count,)),
            sems((count,)),
            sems((3, count)),
            sems((3, count)),
            sems((2,)),
            sems((3, count)),
            sems((count, 2)),
            sems((3,)),
            sems((count,)),
            sems((count, 2)),
            sems((2,)),
            sems((2,)),
            sems((2, 2)),
            sems((2,)),
            sems((2, count, 2)),
            sems((count, count)),
            sems((count, 2)),
            sems((count, 2)),
            sems((count, 2)),
            sems((count, 2)),
            sems((count, 2)),
            sems((count,)),
            sems((count,)),
            sems((2,)),
        ],
        compiler_params=pltpu.CompilerParams(collective_id=0, has_side_effects=True),
    )(
        tokens,
        norm_gain.reshape(1, width),
        query_weight,
        key_weight,
        value_weight,
        map_lambda,
        head_gain,
        attn_out_weight,
        pool_out_weight,
    )


def fits(shape, tokens, query_weight, value_weight, map_lambda, pool_out_weight):
    count = shape["sp"]
    return (
        shape["grp"] == 2
        and shape["tp"] == 4
        and count == 4
        and map_lambda.shape[0] == count
        and value_weight.shape[1] == VD == LANES == 2 * HD
        and tokens.shape[0] % 32 == 0
        and tokens.shape[1] % (4 * LANES) == 0
        and query_weight.shape[0] % 32 == 0
        and query_weight.shape[1] == count * LANES
        and pool_out_weight.shape[0] * 4 == tokens.shape[1]
        and pool_out_weight.shape[1] % LANES == 0
        and pool_out_weight.shape[1] * count == tokens.shape[1]
        and pool_out_weight.shape[0] == pool_out_weight.shape[1]
        and pool_out_weight.shape[0] == query_weight.shape[0]
        and tokens.shape[0] * count * tokens.shape[1] <= 1 << 22
    )


def solution(mesh):
    placed = (
        P(("grp", "sp"), None),
        P(),
        P("sp", "tp"),
        P("sp", "tp"),
        P("sp", "tp"),
        P("tp"),
        P("tp", None),
        P("tp", "sp"),
        P("tp", "sp"),
    )
    shape = dict(mesh.shape)

    def chosen(*args):
        if fits(shape, args[0], args[2], args[4], args[5], args[8]):
            return fused(shape["sp"], *args)
        return on_device(*args)

    return jax.shard_map(
        chosen,
        mesh=mesh,
        in_specs=placed,
        out_specs=(P(("grp", "sp", "tp"), None), P(None, "tp", ("grp", "sp"))),
        check_vma=False,
    )
```

```python
import functools
import math

import jax
import jax.numpy as jnp
from jax import lax
from jax.experimental import pallas as pl
from jax.experimental.pallas import tpu as pltpu
from jax.sharding import PartitionSpec as P

HD = 64
VD = 128
POOL_SPAN = 16


epsilon = 1e-06
very_low = -1e30


def extended(cells, sides, width):
    for axis, dim in sides:
        count = lax.axis_size(axis)
        ends = count - 1
        head = lax.slice_in_dim(cells, 0, width, axis=dim)
        tail = lax.slice_in_dim(cells, cells.shape[dim] - width, cells.shape[dim], axis=dim)
        cells = jnp.concatenate(
            [
                lax.ppermute(tail, axis, [(i, (i + 1) % count) for i in range(ends)]),
                cells,
                lax.ppermute(head, axis, [((i + 1) % count, i) for i in range(ends)]),
            ],
            axis=dim,
        )
    return cells


def add_products(totals, pieces, source):
    results = []
    for running, piece in zip(totals, pieces):
        results.append(jnp.dot(source, piece, preferred_element_type=jnp.float32))
    return tuple(results)


def on_device(
    tokens,
    norm_gain,
    query_weight,
    key_weight,
    value_weight,
    map_lambda,
    head_gain,
    attn_out_weight,
    pool_out_weight,
):
    tokens_wide = tokens.astype(jnp.float32)
    normed = (
        tokens_wide
        * lax.rsqrt(jnp.mean(tokens_wide * tokens_wide, axis=-1, keepdims=True) + epsilon)
        * norm_gain
    ).astype(jnp.bfloat16)
    row_count = normed.shape[0]
    sp_index = lax.axis_index("sp")
    tp_index = lax.axis_index("tp")
    group_width = pool_out_weight.shape[0]
    local_heads = map_lambda.shape[0]
    key_heads = value_weight.shape[1] // VD
    group_heads = local_heads // key_heads
    q_empty = jnp.zeros((row_count, query_weight.shape[1]), jnp.float32)
    k_empty = jnp.zeros((row_count, key_weight.shape[1]), jnp.float32)
    v_empty = jnp.zeros((row_count, value_weight.shape[1]), jnp.float32)
    q_acc, k_acc, v_acc = add_products(
        (q_empty, k_empty, v_empty),
        (
            lax.all_gather(query_weight, "sp", axis=0, tiled=True),
            lax.all_gather(key_weight, "sp", axis=0, tiled=True),
            lax.all_gather(value_weight, "sp", axis=0, tiled=True),
        ),
        normed,
    )
    queries = q_acc.astype(jnp.bfloat16).reshape(row_count, key_heads, group_heads, 2, HD)
    keys_flat = k_acc.astype(jnp.bfloat16)
    values_flat = v_acc.astype(jnp.bfloat16)

    def key_block(state_now, key_pair):
        maxima, totals, accums = state_now
        key_blk, val_blk = key_pair
        scores = jnp.einsum(
            "qhgmd,khmd->hgmqk", queries, key_blk, preferred_element_type=jnp.float32
        ) * HD ** (-0.5)
        highest = jnp.maximum(maxima, jnp.max(scores, axis=-1))
        factor = jnp.exp(maxima - highest)
        weights = jnp.exp(scores - highest[..., None])
        totals = totals * factor + jnp.sum(weights, axis=-1)
        accums = accums * factor[..., None] + jnp.einsum(
            "hgmqk,khe->hgmqe",
            weights.astype(jnp.bfloat16),
            val_blk,
            preferred_element_type=jnp.float32,
        )
        return ((highest, totals, accums), None)

    start_state = (
        jnp.full((key_heads, group_heads, 2, row_count), very_low, jnp.float32),
        jnp.zeros((key_heads, group_heads, 2, row_count), jnp.float32),
        jnp.zeros((key_heads, group_heads, 2, row_count, VD), jnp.float32),
    )
    key_piece = lax.all_gather(keys_flat, "sp", axis=0, tiled=True)
    val_piece = lax.all_gather(values_flat, "sp", axis=0, tiled=True)
    piece_len = key_piece.shape[0]
    block_len = math.gcd(piece_len, 512)
    key_blocks = key_piece.reshape(piece_len // block_len, block_len, key_heads, 2, HD)
    val_blocks = val_piece.reshape(piece_len // block_len, block_len, key_heads, VD)
    state_next, unused = lax.scan(key_block, start_state, (key_blocks, val_blocks))
    maxima, totals, accums = state_next
    log_parts = maxima + jnp.log(totals)
    log_totals = jnp.transpose(log_parts, (2, 0, 1, 3)).reshape(2, local_heads, row_count)
    reads = accums / totals[..., None]
    contrast = reads[:, :, 0] - map_lambda.reshape(key_heads, group_heads, 1, 1) * reads[:, :, 1]
    scaled = (
        contrast
        * lax.rsqrt(jnp.mean(contrast * contrast, axis=-1, keepdims=True) + epsilon)
        * head_gain.reshape(key_heads, group_heads, 1, VD)
    )
    attention_head_rows = (
        jnp.transpose(scaled, (2, 0, 1, 3))
        .reshape(row_count, local_heads * VD)
        .astype(jnp.bfloat16)
    )
    head_rows, log_totals = (attention_head_rows, log_totals)
    own_chan = lax.dynamic_slice_in_dim(normed, tp_index * group_width, group_width, 1)
    reach = POOL_SPAN // 2
    padded = extended(own_chan, (("sp", 0),), reach)
    window = jnp.left_shift(jnp.int32(2), tp_index)
    half_span = window // 2
    running = jnp.zeros((row_count, group_width), jnp.float32)
    for offset in range(POOL_SPAN):
        piece = lax.dynamic_slice_in_dim(padded, reach - half_span + offset, row_count, 0).astype(
            jnp.float32
        )
        running = running + jnp.where(offset < window, piece, 0.0)
    seq_len = row_count * lax.axis_size("sp")
    position = sp_index * row_count + jnp.arange(row_count, dtype=jnp.int32)
    lower_edge = jnp.clip(position - half_span, 0, seq_len)
    upper_edge = jnp.clip(position + window - half_span, 0, seq_len)
    counts_f = (upper_edge - lower_edge).astype(jnp.float32)[:, None]
    pooled = (running / counts_f - own_chan.astype(jnp.float32)).astype(jnp.bfloat16)
    attn_whole, pool_whole = (
        lax.all_gather(attn_out_weight, "sp", axis=1, tiled=True),
        lax.all_gather(pool_out_weight, "sp", axis=1, tiled=True),
    )
    mixed = lax.psum_scatter(
        (
            jnp.dot(head_rows, attn_whole, preferred_element_type=jnp.float32)
            + jnp.dot(pooled, pool_whole, preferred_element_type=jnp.float32)
        ).astype(jnp.bfloat16),
        "tp",
        scatter_dimension=0,
        tiled=True,
    )
    return (mixed, log_totals)


MESH = pl.DeviceIdType.MESH
LANES = 128
scope = jax.named_scope


def fused_kernel(
    count,
    tok,
    gain,
    wq,
    wk,
    wv,
    lam,
    hgain,
    wao,
    wpo,
    mixed_out,
    lt_out,
    tok_own,
    gain_own,
    lam_own,
    hgain_own,
    norm_all,
    kv_own,
    w_kv,
    w_q,
    wa_all,
    wp_own,
    par_own,
    par_in,
    par_use,
    q_all,
    k_all,
    v_all,
    head_own,
    heads_all,
    pooled_all,
    part_out,
    part_in,
    cross_out,
    cross_in,
    block_out,
    block_in,
    pool_in,
    lt_send,
    lt_in,
    local_sem,
    z_send,
    z_out,
    z_recv,
    f_send,
    f_recv,
    kv_send,
    kv_fwd,
    kv_recv,
    q_send,
    q_twin,
    q_recv,
    w_send,
    w_recv,
    par_sem,
    h_send,
    h_recv,
    p_send,
    p_recv,
    x_send,
    x_recv,
    o_send,
    o_recv,
    l_send,
    l_recv,
):
    g = lax.axis_index("grp")
    s = lax.axis_index("sp")
    t = lax.axis_index("tp")
    c = lax.rem(t, 2)
    x = t // 2
    rows, width = tok.shape
    quarter = width // 4
    shard = wq.shape[0]
    part = shard // 2
    pair = 2 * LANES
    group = wpo.shape[0]
    cols = wpo.shape[1]
    half = s // 2
    inner = (s > 0) & (s < count - 1)
    at_home = inner & (c == half)
    away = inner & (c != half)
    sib = t + 1 - 2 * c
    far = lax.rem(t + 2, 4)
    twin = 1 - g
    near = 1 + half
    other = count - 1 - s
    edge = jnp.where(half == 0, 0, count - 1)
    far_edge = count - 1 - edge
    target = 1 + c
    home = 2 * x + half
    f32, bf16 = jnp.float32, jnp.bfloat16

    def span(index, size):
        return pl.ds(pl.multiple_of(index * size, size), size)

    def half_rows(owner, which):
        return pl.ds(pl.multiple_of(owner * shard + which * part, part), part)

    barrier = pltpu.get_barrier_semaphore()

    def greet(where):
        pl.semaphore_signal(barrier, inc=1, device_id=where, device_id_type=MESH)

    for off in range(1, count):
        peer = lax.rem(s + off, count)
        peer_inner = (peer > 0) & (peer < count - 1)

        @pl.when(inner | peer_inner)
        def _():
            greet({"sp": peer})
            greet({"sp": peer, "tp": sib})

    greet({"tp": sib})
    greet({"tp": far})

    @pl.when(inner)
    def _():
        greet({"grp": twin})

    pieces = (
        (tok, tok_own),
        (gain, gain_own),
        (wk, kv_own.at[:, 0:LANES]),
        (wv, kv_own.at[:, LANES:pair]),
        (lam, lam_own),
        (hgain, hgain_own),
        (wao, wa_all.at[0]),
        (wpo, wp_own),
        (wk, w_kv.at[span(s, shard), 0:LANES]),
        (wv, w_kv.at[span(s, shard), LANES:pair]),
        (wq.at[:, span(c, pair)], w_q.at[span(s, shard), :]),
    )
    local = [
        pltpu.make_async_copy(src, dst, local_sem.at[i]) for i, (src, dst) in enumerate(pieces)
    ]
    for piece in local[:4]:
        piece.start()

    local[7].start()

    @pl.when(inner)
    def _():
        for piece in local[4:7]:
            piece.start()

    @pl.when(at_home)
    def _():
        for piece in local[8:]:
            piece.start()

    def copy(src, dst, send, recv, where):
        return pltpu.make_async_remote_copy(
            src_ref=src,
            dst_ref=dst,
            send_sem=send,
            recv_sem=recv,
            device_id=where,
            device_id_type=MESH,
        )

    chunk = rows // 2

    def z_copy(u, dest):
        place = norm_all.at[span(u, chunk), span(t, quarter)]
        return copy(place, place, z_send.at[u], z_recv.at[u], {"sp": dest})

    def z_outward(u):
        place = norm_all.at[span(u, chunk), span(t, quarter)]
        return copy(place, place, z_out.at[u], z_recv.at[u], {"sp": edge})

    def tok_forward(step, u):
        col = span(far if step == 2 else t, quarter)
        place = norm_all.at[span(u, chunk), col]
        where = {"tp": far if step == 1 else sib}
        return copy(place, place, f_send.at[step, u], f_recv.at[step, u], where)

    def kv_first():
        src = kv_own.at[span(g, part), :]
        dst = w_kv.at[half_rows(s, g), :]
        return copy(src, dst, kv_send.at[0], kv_recv.at[s, g], {"sp": target})

    def kv_first_whole():
        dst = w_kv.at[span(s, shard), :]
        return copy(kv_own, dst, kv_send.at[0], kv_recv.at[s, 0], {"sp": near})

    def kv_beside():
        dst = w_kv.at[span(s, shard), :]
        return copy(kv_own, dst, kv_send.at[1], kv_recv.at[s, 0], {"tp": sib})

    def kv_edge():
        place = w_kv.at[span(edge, shard), :]
        return copy(place, place, kv_fwd.at[1, edge], kv_recv.at[edge, 0], {"tp": sib})

    def kv_forward(kind, owner):
        which = twin if kind == 2 else g
        place = w_kv.at[half_rows(owner, which), :]
        where = {"grp": twin} if kind == 0 else {"tp": sib}
        return copy(place, place, kv_fwd.at[kind, owner], kv_recv.at[owner, which], where)

    def kv_arrival(owner, which):
        place = w_kv.at[half_rows(owner, which), :]
        return copy(place, place, kv_fwd.at[0, owner], kv_recv.at[owner, which], {"tp": sib})

    def q_copy(core):
        src = wq.at[span(g, part), core * pair : (core + 1) * pair]
        dst = w_q.at[half_rows(s, g), :]
        where = {"sp": target, "tp": 2 * x + core}
        return copy(src, dst, q_send.at[core], q_recv.at[s, g], where)

    def q_whole(core):
        src = wq.at[:, core * pair : (core + 1) * pair]
        dst = w_q.at[span(s, shard), :]
        where = {"sp": near, "tp": 2 * x + core}
        return copy(src, dst, q_send.at[core], q_recv.at[s, 0], where)

    def q_edge():
        place = w_q.at[span(edge, shard), :]
        return copy(place, place, q_twin.at[edge], q_recv.at[edge, 0], {"tp": sib})

    def q_beside():
        src = wq.at[:, span(1 - c, pair)]
        return copy(src, w_q.at[span(s, shard), :], q_send.at[2], q_recv.at[s, 0], {"tp": sib})

    def q_forward(owner):
        place = w_q.at[half_rows(owner, g), :]
        return copy(place, place, q_twin.at[owner], q_recv.at[owner, g], {"grp": twin})

    def q_arrival(owner, which):
        place = w_q.at[half_rows(owner, which), :]
        return copy(place, place, q_twin.at[owner], q_recv.at[owner, which], {"grp": twin})

    def w_copy():
        return copy(wao, wa_all.at[1], w_send.at[0], w_recv.at[0], {"sp": near})

    def par_copy():
        return copy(par_own, par_in, par_sem.at[0], par_sem.at[1], {"tp": sib})

    head_where = ({"sp": other, "tp": home}, {"tp": sib})

    def head_copy(kind, b):
        dst = heads_all.at[span(b, rows), span(c, pair)]
        src = head_own.at[span(b, rows), :]
        return copy(src, dst, h_send.at[kind, b], h_recv.at[b, c], head_where[kind])

    def head_arrival(b, core):
        place = heads_all.at[span(b, rows), core * pair : (core + 1) * pair]
        return copy(place, place, h_send.at[0, b], h_recv.at[b, core], {"tp": sib})

    def lt_copy(b):
        where = {"sp": b, "tp": home}
        return copy(lt_send.at[b], lt_in.at[c], l_send.at[b], l_recv.at[c], where)

    def lt_arrival(core):
        return copy(lt_send.at[0], lt_in.at[core], l_send.at[0], l_recv.at[core], {"tp": sib})

    def part_copy(b, e):
        src = part_out.at[b, e, 1 - c]
        return copy(src, part_in.at[b, e], p_send.at[b, e], p_recv.at[b, e], {"tp": sib})

    def cross_copy(b, e):
        src = cross_out.at[b, e]
        return copy(src, cross_in.at[b, e], x_send.at[b, e], x_recv.at[b, e], {"tp": far})

    def out_copy(b, e):
        to = s if e == 0 else edge
        return copy(block_out.at[b, e], block_in.at[to], o_send.at[b, e], o_recv.at[to], {"sp": b})

    def out_arrival(i):
        return copy(block_out.at[0, 0], block_in.at[i], o_send.at[0, 0], o_recv.at[i], {"sp": near})

    def pool_copy(b):
        dst = pool_in.at[half]
        where = {"sp": b}
        return copy(block_out.at[b, 0], dst, o_send.at[b, 0], o_recv.at[count + half], where)

    def pool_arrival(i):
        dst = pool_in.at[i]
        return copy(block_out.at[0, 0], dst, o_send.at[0, 0], o_recv.at[count + i], {"sp": near})

    local[0].wait()
    local[1].wait()
    step = rows // 2

    def norm_rows(i, carry):
        at = pl.ds(pl.multiple_of(i * step, step), step)
        v = tok_own[at, :].astype(f32)
        scale = lax.rsqrt(jnp.mean(v * v, axis=-1, keepdims=True) + epsilon)
        to = pl.ds(pl.multiple_of(s * rows + i * step, step), step)
        norm_all[to, :] = (v * scale * gain_own[...]).astype(bf16)
        return carry

    with scope("norm"):
        lax.fori_loop(0, rows // step, norm_rows, 0)
    with scope("barrier"):
        pl.semaphore_wait(barrier, jnp.where(inner, 9, 6))
    sends_on = s != target

    @pl.when(inner)
    def _():
        z_copy(2 * s, other).start()
        z_copy(2 * s + 1, other).start()
        z_outward(2 * s).start()
        z_outward(2 * s + 1).start()

    @pl.when(jnp.logical_not(inner))
    def _():
        z_copy(2 * s, near).start()
        z_copy(2 * s + 1, near).start()

    local[2].wait()
    local[3].wait()

    sends_near = jnp.logical_not(inner) & (c == half)
    sends_past = sends_on & jnp.logical_not(sends_near)

    @pl.when(sends_near)
    def _():
        kv_first_whole().start()
        for core in range(2):
            q_whole(core).start()

    @pl.when(sends_past)
    def _():
        kv_first().start()
        for core in range(2):
            q_copy(core).start()

    seq = rows * count
    window = jnp.where(t == 0, 2, jnp.where(t == 1, 4, jnp.where(t == 2, 8, 16)))
    half_span = window // 2
    sub = rows // 4

    def pool(b, carry):
        at = b * rows + lax.broadcasted_iota(jnp.int32, (rows, seq), 0)
        col = lax.broadcasted_iota(jnp.int32, (rows, seq), 1)
        inside = (col >= at - half_span) & (col < at + window - half_span)
        band = jnp.where(inside, 1.0, 0.0).astype(bf16)
        total = jnp.dot(band, norm_all[:, span(t, group)], preferred_element_type=f32)
        pos = b * rows + lax.broadcasted_iota(jnp.int32, (rows, 1), 0)
        low = jnp.maximum(pos - half_span, 0)
        high = jnp.minimum(pos + window - half_span, seq)
        own = norm_all[span(b, rows), span(t, group)].astype(f32)
        pooled_all[span(b, rows), :] = (total / (high - low).astype(f32) - own).astype(bf16)
        return carry

    def hand_parts(b, e, total):
        for j in range(4):
            part_out[b, e, j % 2, j // 2] = total[j * sub : (j + 1) * sub, :].astype(bf16)
        part_copy(b, e).start()

    def pool_product(b):
        return jnp.dot(pooled_all[span(b, rows), :], wp_own[...], preferred_element_type=f32)

    def second_sum(b, e):
        part_copy(b, e).wait_recv()
        cross_out[b, e] = (
            part_out[b, e, c, 1 - x].astype(f32) + part_in[b, e, 1 - x].astype(f32)
        ).astype(bf16)
        cross_copy(b, e).start()

    def third_sum(b, e, send):
        cross_copy(b, e).wait_recv()
        block_out[b, e] = (
            part_out[b, e, c, x].astype(f32)
            + part_in[b, e, x].astype(f32)
            + cross_in[b, e].astype(f32)
        ).astype(bf16)

        @pl.when(b != s)
        def _():
            send().start()

    def outer_work():
        w_copy().start()
        with scope("otok"):
            for owner in (near, count - 1 - near, far_edge):
                z_copy(2 * owner, near).wait_recv()
                z_copy(2 * owner + 1, near).wait_recv()
        with scope("opool"):
            lax.fori_loop(0, count, pool, 0)
        local[7].wait()

        def outer_steps(m, carry):
            @pl.when((m >= 1) & (m < count + 1))
            def _():
                second_sum(m - 1, 0)

            @pl.when(m < count)
            def _():
                hand_parts(m, 0, pool_product(m))

            @pl.when(m >= 2)
            def _():
                third_sum(m - 2, 0, lambda: pool_copy(m - 2))

            return carry

        with scope("osum"):
            lax.fori_loop(0, count + 2, outer_steps, 0)

    pl.when(jnp.logical_not(inner))(outer_work)

    def inner_work():
        @pl.when(at_home)
        def _():
            kv_beside().start()
            q_beside().start()

        local[4].wait()
        local[5].wait()
        par_own[0:count, :] = hgain_own[...]
        for i in range(count):
            par_own[count + i : count + i + 1, :] = jnp.full((1, LANES), lam_own[i], f32)

        @pl.when(at_home)
        def _():
            par_copy().start()

        def tok_in(u, onward):
            z_copy(u, other).wait_recv()
            if onward:
                z_copy(u, other).start()
            else:
                z_outward(u).start()
            tok_forward(1, u).start()
            tok_forward(0, u).start()

        def tok_x(u):
            tok_forward(1, u).wait_recv()
            tok_forward(2, u).start()

        def kv_in(owner):
            @pl.when(at_home)
            def _():
                kv_arrival(owner, g).wait_recv()
                kv_forward(0, owner).start()
                kv_forward(1, owner).start()

        def kv_y(owner):
            @pl.when(at_home)
            def _():
                kv_arrival(owner, twin).wait_recv()
                kv_forward(2, owner).start()

        def q_in(owner):
            q_arrival(owner, g).wait_recv()
            q_forward(owner).start()

        owners = (edge, other, far_edge)
        split = (other, far_edge)
        with scope("tok0"):
            tok_in(2 * edge, True)
            tok_in(2 * other, False)
        with scope("tok1"):
            tok_in(2 * edge + 1, True)
            tok_in(2 * other + 1, False)
        with scope("kv1"):
            kv_in(other)
        with scope("kv0"):

            @pl.when(at_home)
            def _():
                kv_edge().wait_recv()
                kv_edge().start()

        with scope("q1"):
            q_in(other)
        with scope("kvy1"):
            kv_y(other)
        with scope("tok2"):
            tok_in(2 * far_edge, False)
            tok_in(2 * far_edge + 1, False)
        with scope("x01"):
            for u in (2 * edge, 2 * other, 2 * edge + 1, 2 * other + 1):
                tok_x(u)
        with scope("kv2"):
            kv_in(far_edge)
        with scope("q2"):
            q_in(far_edge)
        with scope("pool"):
            lax.fori_loop(0, count, pool, 0)
        with scope("x2"):
            tok_x(2 * far_edge)
            tok_x(2 * far_edge + 1)
        with scope("kvy2"):
            kv_y(far_edge)
        with scope("rest"):
            for owner in owners:
                for u in (2 * owner, 2 * owner + 1):
                    tok_forward(0, u).wait_recv()
                    tok_forward(2, u).wait_recv()

        with scope("kvrest"):

            @pl.when(at_home)
            def _():
                local[8].wait()
                local[9].wait()
                local[10].wait()

            @pl.when(away)
            def _():
                kv_edge().wait_recv()
                for owner in split:
                    kv_arrival(owner, g).wait_recv()
                    kv_arrival(owner, twin).wait_recv()
                kv_beside().wait_recv()
                q_beside().wait_recv()
                par_copy().wait_recv()

        def project_kv(b, carry):
            acc = jnp.dot(norm_all[span(b, rows), :], w_kv[...], preferred_element_type=f32)
            k_all[span(b, rows), :] = acc[:, 0:LANES].astype(bf16)
            v_all[span(b, rows), :] = acc[:, LANES:pair].astype(bf16)
            return carry

        with scope("projkv"):
            lax.fori_loop(0, count, project_kv, 0)

        with scope("qrest"):
            q_edge().wait_recv()
            for owner in split:
                q_arrival(owner, twin).wait_recv()

        def project_q(b, carry):
            acc = jnp.dot(norm_all[span(b, rows), :], w_q[...], preferred_element_type=f32)
            q_all[span(b, rows), :] = acc.astype(bf16)
            return carry

        with scope("projq"):
            lax.fori_loop(0, count, project_q, 0)

        par_use[...] = jnp.where(at_home, par_own[...], par_in[...])
        lane = lax.broadcasted_iota(jnp.int32, (rows, LANES), 1)
        lt_rows = lt_send.shape[2]
        base = HD ** (-0.5)

        def one_head(b, h):
            head = 2 * c + h
            q = q_all[span(b, rows), h * LANES : (h + 1) * LANES]
            zero = jnp.zeros_like(q)
            both_q = jnp.concatenate(
                [jnp.where(lane < HD, q, zero), jnp.where(lane < HD, zero, q)], axis=0
            )
            raw = lax.dot_general(
                both_q, k_all[...], (((1,), (1,)), ((), ())), preferred_element_type=f32
            )
            highest = jnp.max(raw, axis=-1, keepdims=True)
            weights = jnp.exp2((raw - highest) * (base * math.log2(math.e)))
            totals = jnp.sum(weights, axis=-1, keepdims=True)
            reads = jnp.dot(weights.astype(bf16), v_all[...], preferred_element_type=f32) / totals
            logs = highest * base + jnp.log(totals)
            contrast = reads[:rows] - par_use[pl.ds(count + head, 1), :] * reads[rows:]
            scaled = (
                contrast
                * lax.rsqrt(jnp.mean(contrast * contrast, axis=-1, keepdims=True) + epsilon)
                * par_use[pl.ds(head, 1), :]
            ).astype(bf16)
            return scaled, logs[:rows], logs[rows:]

        def attend(b):
            done = [one_head(b, h) for h in range(2)]
            for h in range(2):
                head_own[span(b, rows), h * LANES : (h + 1) * LANES] = done[h][0]
            head_copy(0, b).start()

            @pl.when(away)
            def _():
                head_copy(1, b).start()

            @pl.when(at_home)
            def _():
                heads_all[span(b, rows), span(c, pair)] = head_own[span(b, rows), :]

            both = jnp.where(
                lane < 2,
                jnp.where(lane == 0, done[0][1], done[0][2]),
                jnp.where(lane == 2, done[1][1], done[1][2]),
            )
            padded = jnp.concatenate([both, jnp.zeros((lt_rows - rows, LANES), f32)], axis=0)
            lt_send[b] = jnp.transpose(padded)[0:8, :]

            @pl.when(jnp.logical_not(at_home & (b == s)))
            def _():
                lt_copy(b).start()

        def first_sum(b):
            for core in range(2):

                @pl.when(jnp.logical_not(at_home & (c == core)))
                def _():
                    head_arrival(b, core).wait_recv()

            for e in range(2):
                if e == 1:

                    @pl.when(b == 0)
                    def _():
                        w_copy().wait_recv()

                total = jnp.dot(
                    heads_all[span(b, rows), :], wa_all[e], preferred_element_type=f32
                )
                hand_parts(b, e, total + pool_product(b) if e == 0 else total)

        def steps(m, carry):
            @pl.when(m < count)
            def _():
                with scope("att"):
                    attend(m)

            @pl.when(m == 2)
            def _():
                local[6].wait()
                local[7].wait()

            @pl.when((m >= 3) & (m < count + 3))
            def _():
                with scope("S2"):
                    for e in range(2):
                        second_sum(m - 3, e)

            @pl.when((m >= 2) & (m < count + 2))
            def _():
                with scope("S1"):
                    first_sum(m - 2)

            @pl.when(m >= 4)
            def _():
                with scope("S3"):
                    for e in range(2):
                        third_sum(m - 4, e, lambda: out_copy(m - 4, e))

            return carry

        lax.fori_loop(0, 2 * count, steps, 0)

    pl.when(inner)(inner_work)

    def put_logs(core, ref, at):
        for h in range(2):
            for m in range(2):
                i = 2 * core + h
                lt_out[m, i : i + 1, :] = ref[at, 2 * h + m : 2 * h + m + 1, 0:rows]

    for core in range(2):

        @pl.when(at_home & (c == core))
        def _():
            put_logs(core, lt_send, s)

        @pl.when(jnp.logical_not(at_home & (c == core)))
        def _():
            lt_arrival(core).wait_recv()
            put_logs(core, lt_in, core)

    for i in range(count):
        with scope(f"final{i}"):
            at = slice(i * cols, (i + 1) * cols)
            maker = min(max(i, 1), count - 2)
            e = 0 if i == maker else 1

            @pl.when(s == maker)
            def _():
                mixed_out[:, at] = block_out[s, e]

            @pl.when(s != maker)
            def _():
                out_arrival(i).wait_recv()
                mixed_out[:, at] = block_in[i]

            if e == 1:
                which = i // (count - 1)

                @pl.when(s == i)
                def _():
                    both = mixed_out[:, at].astype(f32) + block_out[s, 0].astype(f32)
                    mixed_out[:, at] = both.astype(bf16)

                @pl.when(s != i)
                def _():
                    pool_arrival(which).wait_recv()
                    both = mixed_out[:, at].astype(f32) + pool_in[which].astype(f32)
                    mixed_out[:, at] = both.astype(bf16)

    @pl.when(sends_near)
    def _():
        kv_first_whole().wait_send()
        for core in range(2):
            q_whole(core).wait_send()

    @pl.when(sends_past)
    def _():
        kv_first().wait_send()
        for core in range(2):
            q_copy(core).wait_send()

    @pl.when(jnp.logical_not(inner))
    def _():
        z_copy(2 * s, near).wait_send()
        z_copy(2 * s + 1, near).wait_send()
        w_copy().wait_send()

        def drain_outer(b, carry):
            part_copy(b, 0).wait_send()
            cross_copy(b, 0).wait_send()

            @pl.when(b != s)
            def _():
                pool_copy(b).wait_send()

            return carry

        lax.fori_loop(0, count, drain_outer, 0)

    @pl.when(at_home)
    def _():
        kv_beside().wait_send()
        q_beside().wait_send()
        par_copy().wait_send()
        kv_edge().wait_send()
        for owner in (other, far_edge):
            for kind in range(3):
                kv_forward(kind, owner).wait_send()

    @pl.when(inner)
    def _():
        for owner in (s, edge):
            z_copy(2 * owner, other).wait_send()
            z_copy(2 * owner + 1, other).wait_send()
        for owner in (s, other, far_edge):
            z_outward(2 * owner).wait_send()
            z_outward(2 * owner + 1).wait_send()
        for owner in (edge, other, far_edge):
            for step in range(3):
                tok_forward(step, 2 * owner).wait_send()
                tok_forward(step, 2 * owner + 1).wait_send()
        for owner in (other, far_edge):
            q_forward(owner).wait_send()

        def drain(b, carry):
            head_copy(0, b).wait_send()

            @pl.when(away)
            def _():
                head_copy(1, b).wait_send()

            for h in range(2):
                part_copy(b, h).wait_send()
                cross_copy(b, h).wait_send()

                @pl.when(b != s)
                def _():
                    out_copy(b, h).wait_send()

            @pl.when(jnp.logical_not(at_home & (b == s)))
            def _():
                lt_copy(b).wait_send()

            return carry

        lax.fori_loop(0, count, drain, 0)


def fused(
    count,
    tokens,
    norm_gain,
    query_weight,
    key_weight,
    value_weight,
    map_lambda,
    head_gain,
    attn_out_weight,
    pool_out_weight,
):
    rows, width = tokens.shape
    group, cols = pool_out_weight.shape
    shard = query_weight.shape[0]
    sub = rows // 4
    seq = rows * count
    pair = 2 * LANES
    lt_rows = -(-rows // LANES) * LANES
    bf16, f32 = jnp.bfloat16, jnp.float32
    vmem = pl.BlockSpec(memory_space=pltpu.VMEM)
    far = pl.BlockSpec(memory_space=pl.ANY)
    sems = pltpu.SemaphoreType.DMA
    return pl.pallas_call(
        functools.partial(fused_kernel, count),
        out_shape=(
            pltpu.VMEM((sub, width), bf16),
            pltpu.VMEM((2, count, rows), f32),
        ),
        in_specs=[far] * 9,
        out_specs=(vmem, vmem),
        scratch_shapes=[
            pltpu.VMEM((rows, width), bf16),
            pltpu.VMEM((1, width), f32),
            pltpu.SMEM((count,), f32),
            pltpu.VMEM((count, LANES), f32),
            pltpu.VMEM((seq, width), bf16),
            pltpu.VMEM((shard, pair), bf16),
            pltpu.VMEM((width, pair), bf16),
            pltpu.VMEM((width, pair), bf16),
            pltpu.VMEM((2, group, cols), bf16),
            pltpu.VMEM((group, cols), bf16),
            pltpu.VMEM((2 * count, LANES), f32),
            pltpu.VMEM((2 * count, LANES), f32),
            pltpu.VMEM((2 * count, LANES), f32),
            pltpu.VMEM((seq, pair), bf16),
            pltpu.VMEM((seq, LANES), bf16),
            pltpu.VMEM((seq, LANES), bf16),
            pltpu.VMEM((seq, pair), bf16),
            pltpu.VMEM((seq, count * LANES), bf16),
            pltpu.VMEM((seq, group), bf16),
            pltpu.VMEM((count, 2, 2, 2, sub, cols), bf16),
            pltpu.VMEM((count, 2, 2, sub, cols), bf16),
            pltpu.VMEM((count, 2, sub, cols), bf16),
            pltpu.VMEM((count, 2, sub, cols), bf16),
            pltpu.VMEM((count, 2, sub, cols), bf16),
            pltpu.VMEM((count, sub, cols), bf16),
            pltpu.VMEM((2, sub, cols), bf16),
            pltpu.VMEM((count, 8, lt_rows), f32),
            pltpu.VMEM((2, 8, lt_rows), f32),
            sems((11,)),
            sems((2 * count,)),
            sems((2 * count,)),
            sems((2 * count,)),
            sems((3, 2 * count)),
            sems((3, 2 * count)),
            sems((2,)),
            sems((3, count)),
            sems((count, 2)),
            sems((3,)),
            sems((count,)),
            sems((count, 2)),
            sems((1,)),
            sems((1,)),
            sems((2,)),
            sems((2, count)),
            sems((count, 2)),
            sems((count, 2)),
            sems((count, 2)),
            sems((count, 2)),
            sems((count, 2)),
            sems((count, 2)),
            sems((count + 2,)),
            sems((count,)),
            sems((2,)),
        ],
        compiler_params=pltpu.CompilerParams(collective_id=0, has_side_effects=True),
    )(
        tokens,
        norm_gain.reshape(1, width),
        query_weight,
        key_weight,
        value_weight,
        map_lambda,
        head_gain,
        attn_out_weight,
        pool_out_weight,
    )


def fits(shape, tokens, query_weight, value_weight, map_lambda, pool_out_weight):
    count = shape["sp"]
    return (
        shape["grp"] == 2
        and shape["tp"] == 4
        and count == 4
        and map_lambda.shape[0] == count
        and value_weight.shape[1] == VD == LANES == 2 * HD
        and tokens.shape[0] % 32 == 0
        and tokens.shape[1] % (4 * LANES) == 0
        and query_weight.shape[0] % 32 == 0
        and query_weight.shape[1] == count * LANES
        and pool_out_weight.shape[0] * 4 == tokens.shape[1]
        and pool_out_weight.shape[1] % LANES == 0
        and pool_out_weight.shape[1] * count == tokens.shape[1]
        and pool_out_weight.shape[0] == pool_out_weight.shape[1]
        and pool_out_weight.shape[0] == query_weight.shape[0]
        and tokens.shape[0] * count * tokens.shape[1] <= 1 << 22
    )


def solution(mesh):
    placed = (
        P(("grp", "sp"), None),
        P(),
        P("sp", "tp"),
        P("sp", "tp"),
        P("sp", "tp"),
        P("tp"),
        P("tp", None),
        P("tp", "sp"),
        P("tp", "sp"),
    )
    shape = dict(mesh.shape)

    def chosen(*args):
        if fits(shape, args[0], args[2], args[4], args[5], args[8]):
            return fused(shape["sp"], *args)
        return on_device(*args)

    return jax.shard_map(
        chosen,
        mesh=mesh,
        in_specs=placed,
        out_specs=(P(("grp", "sp", "tp"), None), P(None, "tp", ("grp", "sp"))),
        check_vma=False,
    )
```

```python
import functools
import math

import jax
import jax.numpy as jnp
from jax import lax
from jax.experimental import pallas as pl
from jax.experimental.pallas import tpu as pltpu
from jax.sharding import PartitionSpec as P

HD = 64
VD = 128
POOL_SPAN = 16


epsilon = 1e-06
very_low = -1e30


def extended(cells, sides, width):
    for axis, dim in sides:
        count = lax.axis_size(axis)
        ends = count - 1
        head = lax.slice_in_dim(cells, 0, width, axis=dim)
        tail = lax.slice_in_dim(cells, cells.shape[dim] - width, cells.shape[dim], axis=dim)
        cells = jnp.concatenate(
            [
                lax.ppermute(tail, axis, [(i, (i + 1) % count) for i in range(ends)]),
                cells,
                lax.ppermute(head, axis, [((i + 1) % count, i) for i in range(ends)]),
            ],
            axis=dim,
        )
    return cells


def add_products(totals, pieces, source):
    results = []
    for running, piece in zip(totals, pieces):
        results.append(jnp.dot(source, piece, preferred_element_type=jnp.float32))
    return tuple(results)


def on_device(
    tokens,
    norm_gain,
    query_weight,
    key_weight,
    value_weight,
    map_lambda,
    head_gain,
    attn_out_weight,
    pool_out_weight,
):
    tokens_wide = tokens.astype(jnp.float32)
    normed = (
        tokens_wide
        * lax.rsqrt(jnp.mean(tokens_wide * tokens_wide, axis=-1, keepdims=True) + epsilon)
        * norm_gain
    ).astype(jnp.bfloat16)
    row_count = normed.shape[0]
    sp_index = lax.axis_index("sp")
    tp_index = lax.axis_index("tp")
    group_width = pool_out_weight.shape[0]
    local_heads = map_lambda.shape[0]
    key_heads = value_weight.shape[1] // VD
    group_heads = local_heads // key_heads
    q_empty = jnp.zeros((row_count, query_weight.shape[1]), jnp.float32)
    k_empty = jnp.zeros((row_count, key_weight.shape[1]), jnp.float32)
    v_empty = jnp.zeros((row_count, value_weight.shape[1]), jnp.float32)
    q_acc, k_acc, v_acc = add_products(
        (q_empty, k_empty, v_empty),
        (
            lax.all_gather(query_weight, "sp", axis=0, tiled=True),
            lax.all_gather(key_weight, "sp", axis=0, tiled=True),
            lax.all_gather(value_weight, "sp", axis=0, tiled=True),
        ),
        normed,
    )
    queries = q_acc.astype(jnp.bfloat16).reshape(row_count, key_heads, group_heads, 2, HD)
    keys_flat = k_acc.astype(jnp.bfloat16)
    values_flat = v_acc.astype(jnp.bfloat16)

    def key_block(state_now, key_pair):
        maxima, totals, accums = state_now
        key_blk, val_blk = key_pair
        scores = jnp.einsum(
            "qhgmd,khmd->hgmqk", queries, key_blk, preferred_element_type=jnp.float32
        ) * HD ** (-0.5)
        highest = jnp.maximum(maxima, jnp.max(scores, axis=-1))
        factor = jnp.exp(maxima - highest)
        weights = jnp.exp(scores - highest[..., None])
        totals = totals * factor + jnp.sum(weights, axis=-1)
        accums = accums * factor[..., None] + jnp.einsum(
            "hgmqk,khe->hgmqe",
            weights.astype(jnp.bfloat16),
            val_blk,
            preferred_element_type=jnp.float32,
        )
        return ((highest, totals, accums), None)

    start_state = (
        jnp.full((key_heads, group_heads, 2, row_count), very_low, jnp.float32),
        jnp.zeros((key_heads, group_heads, 2, row_count), jnp.float32),
        jnp.zeros((key_heads, group_heads, 2, row_count, VD), jnp.float32),
    )
    key_piece = lax.all_gather(keys_flat, "sp", axis=0, tiled=True)
    val_piece = lax.all_gather(values_flat, "sp", axis=0, tiled=True)
    piece_len = key_piece.shape[0]
    block_len = math.gcd(piece_len, 512)
    key_blocks = key_piece.reshape(piece_len // block_len, block_len, key_heads, 2, HD)
    val_blocks = val_piece.reshape(piece_len // block_len, block_len, key_heads, VD)
    state_next, unused = lax.scan(key_block, start_state, (key_blocks, val_blocks))
    maxima, totals, accums = state_next
    log_parts = maxima + jnp.log(totals)
    log_totals = jnp.transpose(log_parts, (2, 0, 1, 3)).reshape(2, local_heads, row_count)
    reads = accums / totals[..., None]
    contrast = reads[:, :, 0] - map_lambda.reshape(key_heads, group_heads, 1, 1) * reads[:, :, 1]
    scaled = (
        contrast
        * lax.rsqrt(jnp.mean(contrast * contrast, axis=-1, keepdims=True) + epsilon)
        * head_gain.reshape(key_heads, group_heads, 1, VD)
    )
    attention_head_rows = (
        jnp.transpose(scaled, (2, 0, 1, 3))
        .reshape(row_count, local_heads * VD)
        .astype(jnp.bfloat16)
    )
    head_rows, log_totals = (attention_head_rows, log_totals)
    own_chan = lax.dynamic_slice_in_dim(normed, tp_index * group_width, group_width, 1)
    reach = POOL_SPAN // 2
    padded = extended(own_chan, (("sp", 0),), reach)
    window = jnp.left_shift(jnp.int32(2), tp_index)
    half_span = window // 2
    running = jnp.zeros((row_count, group_width), jnp.float32)
    for offset in range(POOL_SPAN):
        piece = lax.dynamic_slice_in_dim(padded, reach - half_span + offset, row_count, 0).astype(
            jnp.float32
        )
        running = running + jnp.where(offset < window, piece, 0.0)
    seq_len = row_count * lax.axis_size("sp")
    position = sp_index * row_count + jnp.arange(row_count, dtype=jnp.int32)
    lower_edge = jnp.clip(position - half_span, 0, seq_len)
    upper_edge = jnp.clip(position + window - half_span, 0, seq_len)
    counts_f = (upper_edge - lower_edge).astype(jnp.float32)[:, None]
    pooled = (running / counts_f - own_chan.astype(jnp.float32)).astype(jnp.bfloat16)
    attn_whole, pool_whole = (
        lax.all_gather(attn_out_weight, "sp", axis=1, tiled=True),
        lax.all_gather(pool_out_weight, "sp", axis=1, tiled=True),
    )
    mixed = lax.psum_scatter(
        (
            jnp.dot(head_rows, attn_whole, preferred_element_type=jnp.float32)
            + jnp.dot(pooled, pool_whole, preferred_element_type=jnp.float32)
        ).astype(jnp.bfloat16),
        "tp",
        scatter_dimension=0,
        tiled=True,
    )
    return (mixed, log_totals)


MESH = pl.DeviceIdType.MESH
LANES = 128
scope = jax.named_scope


def fused_kernel(
    count,
    tok,
    gain,
    wq,
    wk,
    wv,
    lam,
    hgain,
    wao,
    wpo,
    mixed_out,
    lt_out,
    tok_own,
    gain_own,
    lam_own,
    hgain_own,
    norm_all,
    kv_own,
    q_own,
    kv_relay,
    q_relay,
    w_kv,
    w_q,
    wa_all,
    wp_own,
    par_own,
    par_in,
    par_use,
    acc_kv,
    acc_q,
    q_all,
    k_all,
    v_all,
    head_own,
    heads_all,
    pooled_all,
    part_out,
    part_in,
    cross_out,
    cross_in,
    block_out,
    block_in,
    pool_in,
    lt_send,
    lt_in,
    local_sem,
    z_send,
    z_recv,
    f_send,
    f_recv,
    kv_send,
    kv_fwd,
    kv_recv,
    q_send,
    q_twin,
    q_recv,
    r_recv,
    w_send,
    w_fwd,
    w_recv,
    par_sem,
    h_send,
    h_recv,
    p_send,
    p_recv,
    x_send,
    x_recv,
    o_send,
    o_recv,
    l_send,
    l_recv,
):
    g = lax.axis_index("grp")
    s = lax.axis_index("sp")
    t = lax.axis_index("tp")
    c = lax.rem(t, 2)
    x = t // 2
    rows, width = tok.shape
    quarter = width // 4
    shard = wq.shape[0]
    part = shard // 2
    pair = 2 * LANES
    group = wpo.shape[0]
    cols = wpo.shape[1]
    half = s // 2
    inner = (s > 0) & (s < count - 1)
    at_home = inner & (c == half)
    away = inner & (c != half)
    sib = t + 1 - 2 * c
    far = lax.rem(t + 2, 4)
    twin = 1 - g
    near = 1 + half
    other = count - 1 - s
    edge = jnp.where(half == 0, 0, count - 1)
    far_edge = count - 1 - edge
    target = 1 + c
    home = 2 * x + half
    f32, bf16 = jnp.float32, jnp.bfloat16

    def span(index, size):
        return pl.ds(pl.multiple_of(index * size, size), size)

    def half_rows(owner, which):
        return pl.ds(pl.multiple_of(owner * shard + which * part, part), part)

    barrier = pltpu.get_barrier_semaphore()

    def greet(where):
        pl.semaphore_signal(barrier, inc=1, device_id=where, device_id_type=MESH)

    for off in range(1, count):
        peer = lax.rem(s + off, count)
        peer_inner = (peer > 0) & (peer < count - 1)

        @pl.when(inner | peer_inner)
        def _():
            greet({"sp": peer})
            greet({"sp": peer, "tp": sib})

    greet({"tp": sib})
    greet({"tp": far})

    @pl.when(inner)
    def _():
        greet({"grp": twin})

    pieces = (
        (tok, tok_own),
        (gain, gain_own),
        (wk, kv_own.at[:, 0:LANES]),
        (wv, kv_own.at[:, LANES:pair]),
        (lam, lam_own),
        (hgain, hgain_own),
        (wao, wa_all.at[0]),
        (wpo, wp_own),
        (wk, w_kv.at[span(s, shard), 0:LANES]),
        (wv, w_kv.at[span(s, shard), LANES:pair]),
        (wq.at[:, span(c, pair)], w_q.at[span(s, shard), :]),
        (wq, q_own),
    )
    local = [
        pltpu.make_async_copy(src, dst, local_sem.at[i]) for i, (src, dst) in enumerate(pieces)
    ]
    for piece in local[:4]:
        piece.start()
    local[11].start()

    local[7].start()

    @pl.when(inner)
    def _():
        for piece in local[4:7]:
            piece.start()

    @pl.when(at_home)
    def _():
        for piece in local[8:11]:
            piece.start()

    def copy(src, dst, send, recv, where):
        return pltpu.make_async_remote_copy(
            src_ref=src,
            dst_ref=dst,
            send_sem=send,
            recv_sem=recv,
            device_id=where,
            device_id_type=MESH,
        )

    chunk = rows // 2

    def z_copy(u, dest):
        place = norm_all.at[span(u, chunk), span(t, quarter)]
        return copy(place, place, z_send.at[0], z_recv.at[u], {"sp": dest})

    def z_outward(u):
        place = norm_all.at[span(u, chunk), span(t, quarter)]
        return copy(place, place, z_send.at[1], z_recv.at[u], {"sp": edge})

    def tok_forward(step, u):
        col = span(far if step == 2 else t, quarter)
        place = norm_all.at[span(u, chunk), col]
        where = {"tp": far if step == 1 else sib}
        got = f_recv.at[u] if step == 1 else f_recv.at[2 * count + step // 2]
        return copy(place, place, f_send.at[step], got, where)

    def tok_late(step, u):
        col = span(far if step == 2 else t, quarter)
        place = norm_all.at[span(u, chunk), col]
        got = f_recv.at[2 * count + 2 + step + lax.rem(u, 2)]
        return copy(place, place, f_send.at[step], got, {"tp": sib})

    def all_sent(ref, sem):
        copy(ref, ref, sem, sem, {"tp": sib}).wait_send()

    def kv_first():
        src = kv_own.at[span(g, part), :]
        dst = w_kv.at[half_rows(s, g), :]
        return copy(src, dst, kv_send.at[0], kv_recv.at[s, g], {"sp": target})

    def kv_first_whole():
        dst = w_kv.at[span(s, shard), :]
        return copy(kv_own, dst, kv_send.at[0], kv_recv.at[s, 0], {"sp": near})

    def kv_beside():
        dst = w_kv.at[span(s, shard), :]
        return copy(kv_own, dst, kv_send.at[1], kv_recv.at[s, 0], {"tp": sib})

    def kv_edge():
        place = w_kv.at[span(edge, shard), :]
        return copy(place, place, kv_fwd.at[0], kv_recv.at[edge, 0], {"tp": sib})

    def kv_forward(kind, owner):
        which = twin if kind == 2 else g
        place = w_kv.at[half_rows(owner, which), :]
        where = {"grp": twin} if kind == 0 else {"tp": sib}
        return copy(place, place, kv_fwd.at[0], kv_recv.at[owner, which], where)

    def kv_arrival(owner, which):
        place = w_kv.at[half_rows(owner, which), :]
        return copy(place, place, kv_fwd.at[0], kv_recv.at[owner, which], {"tp": sib})

    def q_copy(core):
        src = q_own.at[span(g, part), core * pair : (core + 1) * pair]
        dst = w_q.at[half_rows(s, g), :]
        where = {"sp": target, "tp": 2 * x + core}
        return copy(src, dst, q_send.at[0], q_recv.at[s, g], where)

    def q_whole(core):
        src = q_own.at[:, core * pair : (core + 1) * pair]
        dst = w_q.at[span(s, shard), :]
        where = {"sp": near, "tp": 2 * x + core}
        return copy(src, dst, q_send.at[0], q_recv.at[s, 0], where)

    def q_edge():
        place = w_q.at[span(edge, shard), :]
        return copy(place, place, q_twin.at[0], q_recv.at[edge, 0], {"tp": sib})

    def relay_copy(i):
        if i == 0:
            src, dst = kv_own.at[span(g, part), :], kv_relay
        else:
            src = q_own.at[span(g, part), (i - 1) * pair : i * pair]
            dst = q_relay.at[i - 1]
        send = kv_send.at[0] if i == 0 else q_send.at[0]
        return copy(src, dst, send, r_recv.at[i], {"sp": near})

    def relay_forward(i):
        if i == 0:
            dst = w_kv.at[half_rows(edge, g), :]
            return copy(kv_relay, dst, kv_send.at[2], kv_recv.at[edge, g], {"sp": other})
        dst = w_q.at[half_rows(edge, g), :]
        where = {"sp": other, "tp": 2 * x + i - 1}
        return copy(q_relay.at[i - 1], dst, q_send.at[2], q_recv.at[edge, g], where)

    def q_beside():
        src = q_own.at[:, span(1 - c, pair)]
        return copy(src, w_q.at[span(s, shard), :], q_send.at[1], q_recv.at[s, 0], {"tp": sib})

    def q_forward(owner):
        place = w_q.at[half_rows(owner, g), :]
        return copy(place, place, q_twin.at[0], q_recv.at[owner, g], {"grp": twin})

    def q_arrival(owner, which):
        place = w_q.at[half_rows(owner, which), :]
        return copy(place, place, q_twin.at[0], q_recv.at[owner, which], {"grp": twin})

    w_rows = (span(g, part // 2), pl.ds(part, part), span(twin, part // 2))

    def w_copy(kind):
        src, dst = wao.at[w_rows[kind], :], wa_all.at[1, w_rows[kind], :]
        return copy(src, dst, w_send.at[kind], w_recv.at[kind], {"sp": near})

    def w_forward():
        place = wa_all.at[1, w_rows[0], :]
        return copy(place, place, w_fwd.at[0], w_recv.at[2], {"grp": twin})

    def w_arrival(kind):
        place = wa_all.at[1, w_rows[kind], :]
        return copy(place, place, w_fwd.at[0], w_recv.at[kind], {"grp": twin})

    def par_copy():
        return copy(par_own, par_in, par_sem.at[0], par_sem.at[1], {"tp": sib})

    head_where = ({"sp": other, "tp": home}, {"tp": sib})

    def head_copy(kind, b):
        dst = heads_all.at[span(b, rows), span(c, pair)]
        src = head_own.at[span(b, rows), :]
        return copy(src, dst, h_send.at[kind], h_recv.at[b, c], head_where[kind])

    def head_arrival(b, core):
        place = heads_all.at[span(b, rows), core * pair : (core + 1) * pair]
        return copy(place, place, h_send.at[0], h_recv.at[b, core], {"tp": sib})

    def lt_copy(b):
        where = {"sp": b, "tp": home}
        return copy(lt_send.at[b], lt_in.at[c], l_send.at[0], l_recv.at[c], where)

    def lt_arrival(core):
        return copy(lt_send.at[0], lt_in.at[core], l_send.at[0], l_recv.at[core], {"tp": sib})

    def part_copy(b, e):
        src = part_out.at[b, e, 1 - c]
        return copy(src, part_in.at[b, e], p_send.at[0], p_recv.at[b, e], {"tp": sib})

    def cross_copy(b, e):
        src = cross_out.at[b, e]
        return copy(src, cross_in.at[b, e], x_send.at[0], x_recv.at[b, e], {"tp": far})

    def out_copy(b, e):
        to = s if e == 0 else edge
        return copy(block_out.at[b, e], block_in.at[to], o_send.at[0], o_recv.at[to], {"sp": b})

    def out_arrival(i):
        return copy(block_out.at[0, 0], block_in.at[i], o_send.at[0], o_recv.at[i], {"sp": near})

    def pool_copy(b):
        dst = pool_in.at[half]
        where = {"sp": b}
        return copy(block_out.at[b, 0], dst, o_send.at[0], o_recv.at[count + half], where)

    def pool_arrival(i):
        dst = pool_in.at[i]
        return copy(block_out.at[0, 0], dst, o_send.at[0], o_recv.at[count + i], {"sp": near})

    local[0].wait()
    local[1].wait()
    step = rows // 2

    def norm_rows(i, carry):
        at = pl.ds(pl.multiple_of(i * step, step), step)
        v = tok_own[at, :].astype(f32)
        scale = lax.rsqrt(jnp.mean(v * v, axis=-1, keepdims=True) + epsilon)
        to = pl.ds(pl.multiple_of(s * rows + i * step, step), step)
        norm_all[to, :] = (v * scale * gain_own[...]).astype(bf16)
        return carry

    with scope("norm"):
        lax.fori_loop(0, rows // step, norm_rows, 0)
    with scope("barrier"):
        pl.semaphore_wait(barrier, jnp.where(inner, 9, 6))
    sends_on = s != target

    @pl.when(inner)
    def _():
        z_copy(2 * s, other).start()
        z_copy(2 * s + 1, other).start()
        z_outward(2 * s).start()
        z_outward(2 * s + 1).start()

    @pl.when(jnp.logical_not(inner))
    def _():
        z_copy(2 * s, near).start()
        z_copy(2 * s + 1, near).start()

    local[2].wait()
    local[3].wait()
    local[11].wait()

    sends_near = jnp.logical_not(inner) & (c == half)

    sends_relay = jnp.logical_not(inner) & (c != half)

    @pl.when(sends_relay)
    def _():
        for i in range(3):
            relay_copy(i).start()

    @pl.when(away)
    def _():
        kv_first().start()
        for core in range(2):
            q_copy(core).start()

    seq = rows * count
    window = jnp.where(t == 0, 2, jnp.where(t == 1, 4, jnp.where(t == 2, 8, 16)))
    half_span = window // 2
    sub = rows // 4

    def pool(b, carry):
        at = b * rows + lax.broadcasted_iota(jnp.int32, (rows, seq), 0)
        col = lax.broadcasted_iota(jnp.int32, (rows, seq), 1)
        inside = (col >= at - half_span) & (col < at + window - half_span)
        band = jnp.where(inside, 1.0, 0.0).astype(bf16)
        total = jnp.dot(band, norm_all[:, span(t, group)], preferred_element_type=f32)
        pos = b * rows + lax.broadcasted_iota(jnp.int32, (rows, 1), 0)
        low = jnp.maximum(pos - half_span, 0)
        high = jnp.minimum(pos + window - half_span, seq)
        own = norm_all[span(b, rows), span(t, group)].astype(f32)
        pooled_all[span(b, rows), :] = (total / (high - low).astype(f32) - own).astype(bf16)
        return carry

    def hand_parts(b, e, total):
        for j in range(4):
            part_out[b, e, j % 2, j // 2] = total[j * sub : (j + 1) * sub, :].astype(bf16)
        part_copy(b, e).start()

    def pool_product(b):
        return jnp.dot(pooled_all[span(b, rows), :], wp_own[...], preferred_element_type=f32)

    def second_sum(b, e):
        part_copy(b, e).wait_recv()
        cross_out[b, e] = (
            part_out[b, e, c, 1 - x].astype(f32) + part_in[b, e, 1 - x].astype(f32)
        ).astype(bf16)
        cross_copy(b, e).start()

    def third_sum(b, e, send):
        cross_copy(b, e).wait_recv()
        block_out[b, e] = (
            part_out[b, e, c, x].astype(f32)
            + part_in[b, e, x].astype(f32)
            + cross_in[b, e].astype(f32)
        ).astype(bf16)

        @pl.when(b != s)
        def _():
            send().start()

    def outer_work():
        with scope("otok"):
            for u in (2 * near, 2 * near + 1, 2 * (count - 1 - near)):
                z_copy(u, near).wait_recv()

            @pl.when(sends_near)
            def _():
                kv_first_whole().start()
                for core in range(2):
                    q_whole(core).start()

            z_copy(2 * (count - 1 - near) + 1, near).wait_recv()
            z_copy(2 * far_edge, near).wait_recv()
            z_copy(2 * far_edge + 1, near).wait_recv()
        with scope("opool"):
            lax.fori_loop(0, count, pool, 0)
        w_copy(0).start()
        w_copy(1).start()
        local[7].wait()

        def outer_steps(m, carry):
            @pl.when((m >= 1) & (m < count + 1))
            def _():
                second_sum(m - 1, 0)

            @pl.when(m < count)
            def _():
                hand_parts(m, 0, pool_product(m))

            @pl.when(m >= 2)
            def _():
                third_sum(m - 2, 0, lambda: pool_copy(m - 2))

            return carry

        with scope("osum"):
            lax.fori_loop(0, count + 2, outer_steps, 0)

    pl.when(jnp.logical_not(inner))(outer_work)

    def inner_work():
        @pl.when(at_home)
        def _():
            kv_beside().start()
            q_beside().start()

        local[4].wait()
        local[5].wait()
        par_own[0:count, :] = hgain_own[...]
        for i in range(count):
            par_own[count + i : count + i + 1, :] = jnp.full((1, LANES), lam_own[i], f32)

        @pl.when(at_home)
        def _():
            par_copy().start()

        def tok_in(u, onward, beside=tok_forward):
            z_copy(u, other).wait_recv()
            if onward:
                z_copy(u, other).start()
            else:
                z_outward(u).start()
            tok_forward(1, u).start()
            beside(0, u).start()

        def tok_x(u, beside=tok_forward):
            tok_forward(1, u).wait_recv()
            beside(2, u).start()

        def kv_in(owner):
            @pl.when(at_home)
            def _():
                kv_arrival(owner, g).wait_recv()
                kv_forward(0, owner).start()
                kv_forward(1, owner).start()

        def r_arrive(i):
            relay_copy(i).wait_recv()
            relay_forward(i).start()

        def kv_y(owner):
            @pl.when(at_home)
            def _():
                kv_arrival(owner, twin).wait_recv()
                kv_forward(2, owner).start()

        def q_in(owner):
            q_arrival(owner, g).wait_recv()
            q_forward(owner).start()

        owners = (edge, other, far_edge)
        split = (other, far_edge)
        with scope("tok0"):
            tok_in(2 * edge, True)
            tok_in(2 * other, False)
        with scope("tok1"):
            tok_in(2 * edge + 1, True)
            tok_in(2 * other + 1, False)
        with scope("relay0"):

            @pl.when(away)
            def _():
                r_arrive(0)

        with scope("kv1"):
            kv_in(other)
        with scope("x0"):
            tok_x(2 * edge)
            tok_x(2 * other)
        with scope("q1"):
            q_in(other)
        with scope("relay1"):

            @pl.when(away)
            def _():
                r_arrive(1)
                r_arrive(2)

        with scope("tok2"):
            tok_in(2 * far_edge, False, tok_late)
        with scope("kvy1"):
            kv_y(other)
        with scope("x1"):
            tok_x(2 * edge + 1)
            tok_x(2 * other + 1)
        with scope("tok3"):
            tok_in(2 * far_edge + 1, False, tok_late)
        with scope("kv0"):

            @pl.when(at_home)
            def _():
                kv_edge().wait_recv()
                kv_edge().start()

        with scope("kv2"):
            kv_in(far_edge)
        with scope("pool"):
            lax.fori_loop(0, count, pool, 0)
        with scope("q2"):
            q_in(far_edge)
        with scope("x2"):
            tok_x(2 * far_edge, tok_late)
            tok_x(2 * far_edge + 1, tok_late)
        with scope("kvy2"):
            kv_y(far_edge)

        early = pl.ds(pl.multiple_of(half * rows, rows), 3 * rows)
        late = span(far_edge, rows)
        k_early = pl.ds(pl.multiple_of(half * shard, shard), 3 * shard)
        k_late = span(far_edge, shard)

        def early_product(store, w):
            store[...] = jnp.dot(
                norm_all[early, k_early], w[k_early, :], preferred_element_type=f32
            )

        def late_product(store, w, put):
            acc = store[...] + jnp.dot(
                norm_all[early, k_late], w[k_late, :], preferred_element_type=f32
            )
            put(early, acc.astype(bf16))
            acc = jnp.dot(norm_all[late, :], w[...], preferred_element_type=f32)
            put(late, acc.astype(bf16))

        def early_tokens(step):
            place = norm_all.at[0 : 2 * rows, 0:quarter]
            got = f_recv.at[2 * count + step // 2]
            return copy(place, place, f_send.at[step], got, {"tp": sib})

        with scope("earlykv"):
            for step in (0, 2):
                early_tokens(step).wait_recv()

            @pl.when(at_home)
            def _():
                local[8].wait()
                local[9].wait()
                local[10].wait()

            @pl.when(away)
            def _():
                kv_edge().wait_recv()
                kv_arrival(other, g).wait_recv()
                kv_arrival(other, twin).wait_recv()
                kv_beside().wait_recv()
                q_beside().wait_recv()
                par_copy().wait_recv()

            early_product(acc_kv, w_kv)
        with scope("rest"):
            for step in (0, 2):
                for u in (2 * far_edge, 2 * far_edge + 1):
                    tok_late(step, u).wait_recv()
        with scope("kvrest"):

            @pl.when(away)
            def _():
                kv_arrival(far_edge, g).wait_recv()
                kv_arrival(far_edge, twin).wait_recv()

        def put_kv(at, value):
            k_all[at, :] = value[:, 0:LANES]
            v_all[at, :] = value[:, LANES:pair]

        def put_q(at, value):
            q_all[at, :] = value

        with scope("projkv"):
            late_product(acc_kv, w_kv, put_kv)
        with scope("earlyq"):
            q_edge().wait_recv()
            q_arrival(other, twin).wait_recv()
            early_product(acc_q, w_q)
        with scope("qrest"):
            q_arrival(far_edge, twin).wait_recv()
        with scope("projq"):
            late_product(acc_q, w_q, put_q)

        par_use[...] = jnp.where(at_home, par_own[...], par_in[...])
        lane = lax.broadcasted_iota(jnp.int32, (rows, LANES), 1)
        lt_rows = lt_send.shape[2]
        base = HD ** (-0.5)

        def one_head(b, h):
            head = 2 * c + h
            q = q_all[span(b, rows), h * LANES : (h + 1) * LANES]
            zero = jnp.zeros_like(q)
            both_q = jnp.concatenate(
                [jnp.where(lane < HD, q, zero), jnp.where(lane < HD, zero, q)], axis=0
            )
            raw = lax.dot_general(
                both_q, k_all[...], (((1,), (1,)), ((), ())), preferred_element_type=f32
            )
            highest = jnp.max(raw, axis=-1, keepdims=True)
            weights = jnp.exp2((raw - highest) * (base * math.log2(math.e)))
            totals = jnp.sum(weights, axis=-1, keepdims=True)
            reads = jnp.dot(weights.astype(bf16), v_all[...], preferred_element_type=f32) / totals
            logs = highest * base + jnp.log(totals)
            contrast = reads[:rows] - par_use[pl.ds(count + head, 1), :] * reads[rows:]
            scaled = (
                contrast
                * lax.rsqrt(jnp.mean(contrast * contrast, axis=-1, keepdims=True) + epsilon)
                * par_use[pl.ds(head, 1), :]
            ).astype(bf16)
            return scaled, logs[:rows], logs[rows:]

        def attend(b):
            done = [one_head(b, h) for h in range(2)]
            for h in range(2):
                head_own[span(b, rows), h * LANES : (h + 1) * LANES] = done[h][0]
            head_copy(0, b).start()

            @pl.when(away)
            def _():
                head_copy(1, b).start()

            @pl.when(at_home)
            def _():
                heads_all[span(b, rows), span(c, pair)] = head_own[span(b, rows), :]

            both = jnp.where(
                lane < 2,
                jnp.where(lane == 0, done[0][1], done[0][2]),
                jnp.where(lane == 2, done[1][1], done[1][2]),
            )
            padded = jnp.concatenate([both, jnp.zeros((lt_rows - rows, LANES), f32)], axis=0)
            lt_send[b] = jnp.transpose(padded)[0:8, :]

            @pl.when(jnp.logical_not(at_home & (b == s)))
            def _():
                lt_copy(b).start()

        def first_sum(b):
            for core in range(2):

                @pl.when(jnp.logical_not(at_home & (c == core)))
                def _():
                    head_arrival(b, core).wait_recv()

            for e in range(2):
                if e == 1:

                    @pl.when(b == 0)
                    def _():
                        with scope("wrest"):
                            w_arrival(1).wait_recv()
                            w_arrival(2).wait_recv()

                total = jnp.dot(heads_all[span(b, rows), :], wa_all[e], preferred_element_type=f32)
                hand_parts(b, e, total + pool_product(b) if e == 0 else total)

        def attend_all(b, carry):
            with scope("att"):
                attend(b)

            @pl.when(b == 0)
            def _():
                with scope("wao"):
                    w_arrival(0).wait_recv()
                    w_forward().start()

            return carry

        lax.fori_loop(0, count, attend_all, 0)
        local[6].wait()
        local[7].wait()

        def steps(m, carry):
            @pl.when(m < count)
            def _():
                with scope("S1"):
                    first_sum(m)
                with scope("S2"):
                    for e in range(2):
                        second_sum(m, e)

            @pl.when(m >= 2)
            def _():
                with scope("S3"):
                    for e in range(2):
                        third_sum(m - 2, e, lambda: out_copy(m - 2, e))

            return carry

        lax.fori_loop(0, count + 2, steps, 0)

    pl.when(inner)(inner_work)

    def put_logs(core, ref, at):
        for h in range(2):
            for m in range(2):
                i = 2 * core + h
                lt_out[m, i : i + 1, :] = ref[at, 2 * h + m : 2 * h + m + 1, 0:rows]

    for core in range(2):

        @pl.when(at_home & (c == core))
        def _():
            put_logs(core, lt_send, s)

        @pl.when(jnp.logical_not(at_home & (c == core)))
        def _():
            lt_arrival(core).wait_recv()
            put_logs(core, lt_in, core)

    for i in range(count):
        with scope(f"final{i}"):
            at = slice(i * cols, (i + 1) * cols)
            maker = min(max(i, 1), count - 2)
            e = 0 if i == maker else 1

            @pl.when(s == maker)
            def _():
                mixed_out[:, at] = block_out[s, e]

            @pl.when(s != maker)
            def _():
                out_arrival(i).wait_recv()
                mixed_out[:, at] = block_in[i]

            if e == 1:
                which = i // (count - 1)

                @pl.when(s == i)
                def _():
                    both = mixed_out[:, at].astype(f32) + block_out[s, 0].astype(f32)
                    mixed_out[:, at] = both.astype(bf16)

                @pl.when(s != i)
                def _():
                    pool_arrival(which).wait_recv()
                    both = mixed_out[:, at].astype(f32) + pool_in[which].astype(f32)
                    mixed_out[:, at] = both.astype(bf16)

    @pl.when(sends_near)
    def _():
        kv_first_whole().wait_send()
        all_sent(w_q.at[0 : 2 * shard, :], q_send.at[0])

    @pl.when(sends_relay | away)
    def _():
        relay_copy(0).wait_send()
        all_sent(w_q.at[0:shard, :], q_send.at[0])

    @pl.when(away)
    def _():
        relay_forward(0).wait_send()
        all_sent(w_q.at[0:shard, :], q_send.at[2])

    @pl.when(jnp.logical_not(inner))
    def _():
        all_sent(norm_all.at[0:rows, 0:quarter], z_send.at[0])
        w_copy(0).wait_send()
        w_copy(1).wait_send()
        all_sent(part_in.at[:, 0], p_send.at[0])
        all_sent(cross_in.at[:, 0], x_send.at[0])
        all_sent(block_out.at[0 : count - 1, 0], o_send.at[0])

    @pl.when(at_home)
    def _():
        kv_beside().wait_send()
        q_beside().wait_send()
        par_copy().wait_send()
        all_sent(w_kv, kv_fwd.at[0])

    @pl.when(away)
    def _():
        all_sent(head_own, h_send.at[1])

    @pl.when(inner)
    def _():
        all_sent(norm_all.at[0 : 2 * rows, 0:quarter], z_send.at[0])
        for sem in (z_send.at[1], f_send.at[0], f_send.at[1], f_send.at[2]):
            all_sent(norm_all.at[0 : 3 * rows, 0:quarter], sem)
        all_sent(w_q.at[0:shard, :], q_twin.at[0])
        w_forward().wait_send()
        all_sent(head_own, h_send.at[0])
        all_sent(part_in, p_send.at[0])
        all_sent(cross_in, x_send.at[0])
        all_sent(block_out.at[0 : count - 1], o_send.at[0])

    @pl.when(inner & jnp.logical_not(at_home))
    def _():
        all_sent(lt_send, l_send.at[0])

    @pl.when(at_home)
    def _():
        all_sent(lt_send.at[0 : count - 1], l_send.at[0])


def fused(
    count,
    tokens,
    norm_gain,
    query_weight,
    key_weight,
    value_weight,
    map_lambda,
    head_gain,
    attn_out_weight,
    pool_out_weight,
):
    rows, width = tokens.shape
    group, cols = pool_out_weight.shape
    shard = query_weight.shape[0]
    sub = rows // 4
    seq = rows * count
    pair = 2 * LANES
    lt_rows = -(-rows // LANES) * LANES
    bf16, f32 = jnp.bfloat16, jnp.float32
    vmem = pl.BlockSpec(memory_space=pltpu.VMEM)
    far = pl.BlockSpec(memory_space=pl.ANY)
    sems = pltpu.SemaphoreType.DMA
    return pl.pallas_call(
        functools.partial(fused_kernel, count),
        out_shape=(
            pltpu.VMEM((sub, width), bf16),
            pltpu.VMEM((2, count, rows), f32),
        ),
        in_specs=[far] * 9,
        out_specs=(vmem, vmem),
        scratch_shapes=[
            pltpu.VMEM((rows, width), bf16),
            pltpu.VMEM((1, width), f32),
            pltpu.SMEM((count,), f32),
            pltpu.VMEM((count, LANES), f32),
            pltpu.VMEM((seq, width), bf16),
            pltpu.VMEM((shard, pair), bf16),
            pltpu.VMEM((shard, count * LANES), bf16),
            pltpu.VMEM((shard // 2, pair), bf16),
            pltpu.VMEM((2, shard // 2, pair), bf16),
            pltpu.VMEM((width, pair), bf16),
            pltpu.VMEM((width, pair), bf16),
            pltpu.VMEM((2, group, cols), bf16),
            pltpu.VMEM((group, cols), bf16),
            pltpu.VMEM((2 * count, LANES), f32),
            pltpu.VMEM((2 * count, LANES), f32),
            pltpu.VMEM((2 * count, LANES), f32),
            pltpu.VMEM((3 * rows, pair), f32),
            pltpu.VMEM((3 * rows, pair), f32),
            pltpu.VMEM((seq, pair), bf16),
            pltpu.VMEM((seq, LANES), bf16),
            pltpu.VMEM((seq, LANES), bf16),
            pltpu.VMEM((seq, pair), bf16),
            pltpu.VMEM((seq, count * LANES), bf16),
            pltpu.VMEM((seq, group), bf16),
            pltpu.VMEM((count, 2, 2, 2, sub, cols), bf16),
            pltpu.VMEM((count, 2, 2, sub, cols), bf16),
            pltpu.VMEM((count, 2, sub, cols), bf16),
            pltpu.VMEM((count, 2, sub, cols), bf16),
            pltpu.VMEM((count, 2, sub, cols), bf16),
            pltpu.VMEM((count, sub, cols), bf16),
            pltpu.VMEM((2, sub, cols), bf16),
            pltpu.VMEM((count, 8, lt_rows), f32),
            pltpu.VMEM((2, 8, lt_rows), f32),
            sems((12,)),
            sems((2,)),
            sems((2 * count,)),
            sems((3,)),
            sems((2 * count + 6,)),
            sems((3,)),
            sems((1,)),
            sems((count, 2)),
            sems((3,)),
            sems((1,)),
            sems((count, 2)),
            sems((3,)),
            sems((2,)),
            sems((1,)),
            sems((3,)),
            sems((2,)),
            sems((2,)),
            sems((count, 2)),
            sems((1,)),
            sems((count, 2)),
            sems((1,)),
            sems((count, 2)),
            sems((1,)),
            sems((count + 2,)),
            sems((1,)),
            sems((2,)),
        ],
        compiler_params=pltpu.CompilerParams(collective_id=0, has_side_effects=True),
    )(
        tokens,
        norm_gain.reshape(1, width),
        query_weight,
        key_weight,
        value_weight,
        map_lambda,
        head_gain,
        attn_out_weight,
        pool_out_weight,
    )


def fits(shape, tokens, query_weight, value_weight, map_lambda, pool_out_weight):
    count = shape["sp"]
    return (
        shape["grp"] == 2
        and shape["tp"] == 4
        and count == 4
        and map_lambda.shape[0] == count
        and value_weight.shape[1] == VD == LANES == 2 * HD
        and tokens.shape[0] % 32 == 0
        and tokens.shape[1] % (4 * LANES) == 0
        and query_weight.shape[0] % 32 == 0
        and query_weight.shape[1] == count * LANES
        and pool_out_weight.shape[0] * 4 == tokens.shape[1]
        and pool_out_weight.shape[1] % LANES == 0
        and pool_out_weight.shape[1] * count == tokens.shape[1]
        and pool_out_weight.shape[0] == pool_out_weight.shape[1]
        and pool_out_weight.shape[0] == query_weight.shape[0]
        and tokens.shape[0] * count * tokens.shape[1] <= 1 << 22
    )


def solution(mesh):
    placed = (
        P(("grp", "sp"), None),
        P(),
        P("sp", "tp"),
        P("sp", "tp"),
        P("sp", "tp"),
        P("tp"),
        P("tp", None),
        P("tp", "sp"),
        P("tp", "sp"),
    )
    shape = dict(mesh.shape)

    def chosen(*args):
        if fits(shape, args[0], args[2], args[4], args[5], args[8]):
            return fused(shape["sp"], *args)
        return on_device(*args)

    return jax.shard_map(
        chosen,
        mesh=mesh,
        in_specs=placed,
        out_specs=(P(("grp", "sp", "tp"), None), P(None, "tp", ("grp", "sp"))),
        check_vma=False,
    )
```

```python
import functools
import math

import jax
import jax.numpy as jnp
from jax import lax
from jax.experimental import pallas as pl
from jax.experimental.pallas import tpu as pltpu
from jax.sharding import PartitionSpec as P

HD = 64
VD = 128
POOL_SPAN = 16


epsilon = 1e-06
very_low = -1e30


def extended(cells, sides, width):
    for axis, dim in sides:
        count = lax.axis_size(axis)
        ends = count - 1
        head = lax.slice_in_dim(cells, 0, width, axis=dim)
        tail = lax.slice_in_dim(cells, cells.shape[dim] - width, cells.shape[dim], axis=dim)
        cells = jnp.concatenate(
            [
                lax.ppermute(tail, axis, [(i, (i + 1) % count) for i in range(ends)]),
                cells,
                lax.ppermute(head, axis, [((i + 1) % count, i) for i in range(ends)]),
            ],
            axis=dim,
        )
    return cells


def add_products(totals, pieces, source):
    results = []
    for running, piece in zip(totals, pieces):
        results.append(jnp.dot(source, piece, preferred_element_type=jnp.float32))
    return tuple(results)


def on_device(
    tokens,
    norm_gain,
    query_weight,
    key_weight,
    value_weight,
    map_lambda,
    head_gain,
    attn_out_weight,
    pool_out_weight,
):
    tokens_wide = tokens.astype(jnp.float32)
    normed = (
        tokens_wide
        * lax.rsqrt(jnp.mean(tokens_wide * tokens_wide, axis=-1, keepdims=True) + epsilon)
        * norm_gain
    ).astype(jnp.bfloat16)
    row_count = normed.shape[0]
    sp_index = lax.axis_index("sp")
    tp_index = lax.axis_index("tp")
    group_width = pool_out_weight.shape[0]
    local_heads = map_lambda.shape[0]
    key_heads = value_weight.shape[1] // VD
    group_heads = local_heads // key_heads
    q_empty = jnp.zeros((row_count, query_weight.shape[1]), jnp.float32)
    k_empty = jnp.zeros((row_count, key_weight.shape[1]), jnp.float32)
    v_empty = jnp.zeros((row_count, value_weight.shape[1]), jnp.float32)
    q_acc, k_acc, v_acc = add_products(
        (q_empty, k_empty, v_empty),
        (
            lax.all_gather(query_weight, "sp", axis=0, tiled=True),
            lax.all_gather(key_weight, "sp", axis=0, tiled=True),
            lax.all_gather(value_weight, "sp", axis=0, tiled=True),
        ),
        normed,
    )
    queries = q_acc.astype(jnp.bfloat16).reshape(row_count, key_heads, group_heads, 2, HD)
    keys_flat = k_acc.astype(jnp.bfloat16)
    values_flat = v_acc.astype(jnp.bfloat16)

    def key_block(state_now, key_pair):
        maxima, totals, accums = state_now
        key_blk, val_blk = key_pair
        scores = jnp.einsum(
            "qhgmd,khmd->hgmqk", queries, key_blk, preferred_element_type=jnp.float32
        ) * HD ** (-0.5)
        highest = jnp.maximum(maxima, jnp.max(scores, axis=-1))
        factor = jnp.exp(maxima - highest)
        weights = jnp.exp(scores - highest[..., None])
        totals = totals * factor + jnp.sum(weights, axis=-1)
        accums = accums * factor[..., None] + jnp.einsum(
            "hgmqk,khe->hgmqe",
            weights.astype(jnp.bfloat16),
            val_blk,
            preferred_element_type=jnp.float32,
        )
        return ((highest, totals, accums), None)

    start_state = (
        jnp.full((key_heads, group_heads, 2, row_count), very_low, jnp.float32),
        jnp.zeros((key_heads, group_heads, 2, row_count), jnp.float32),
        jnp.zeros((key_heads, group_heads, 2, row_count, VD), jnp.float32),
    )
    key_piece = lax.all_gather(keys_flat, "sp", axis=0, tiled=True)
    val_piece = lax.all_gather(values_flat, "sp", axis=0, tiled=True)
    piece_len = key_piece.shape[0]
    block_len = math.gcd(piece_len, 512)
    key_blocks = key_piece.reshape(piece_len // block_len, block_len, key_heads, 2, HD)
    val_blocks = val_piece.reshape(piece_len // block_len, block_len, key_heads, VD)
    state_next, unused = lax.scan(key_block, start_state, (key_blocks, val_blocks))
    maxima, totals, accums = state_next
    log_parts = maxima + jnp.log(totals)
    log_totals = jnp.transpose(log_parts, (2, 0, 1, 3)).reshape(2, local_heads, row_count)
    reads = accums / totals[..., None]
    contrast = reads[:, :, 0] - map_lambda.reshape(key_heads, group_heads, 1, 1) * reads[:, :, 1]
    scaled = (
        contrast
        * lax.rsqrt(jnp.mean(contrast * contrast, axis=-1, keepdims=True) + epsilon)
        * head_gain.reshape(key_heads, group_heads, 1, VD)
    )
    attention_head_rows = (
        jnp.transpose(scaled, (2, 0, 1, 3))
        .reshape(row_count, local_heads * VD)
        .astype(jnp.bfloat16)
    )
    head_rows, log_totals = (attention_head_rows, log_totals)
    own_chan = lax.dynamic_slice_in_dim(normed, tp_index * group_width, group_width, 1)
    reach = POOL_SPAN // 2
    padded = extended(own_chan, (("sp", 0),), reach)
    window = jnp.left_shift(jnp.int32(2), tp_index)
    half_span = window // 2
    running = jnp.zeros((row_count, group_width), jnp.float32)
    for offset in range(POOL_SPAN):
        piece = lax.dynamic_slice_in_dim(padded, reach - half_span + offset, row_count, 0).astype(
            jnp.float32
        )
        running = running + jnp.where(offset < window, piece, 0.0)
    seq_len = row_count * lax.axis_size("sp")
    position = sp_index * row_count + jnp.arange(row_count, dtype=jnp.int32)
    lower_edge = jnp.clip(position - half_span, 0, seq_len)
    upper_edge = jnp.clip(position + window - half_span, 0, seq_len)
    counts_f = (upper_edge - lower_edge).astype(jnp.float32)[:, None]
    pooled = (running / counts_f - own_chan.astype(jnp.float32)).astype(jnp.bfloat16)
    attn_whole, pool_whole = (
        lax.all_gather(attn_out_weight, "sp", axis=1, tiled=True),
        lax.all_gather(pool_out_weight, "sp", axis=1, tiled=True),
    )
    mixed = lax.psum_scatter(
        (
            jnp.dot(head_rows, attn_whole, preferred_element_type=jnp.float32)
            + jnp.dot(pooled, pool_whole, preferred_element_type=jnp.float32)
        ).astype(jnp.bfloat16),
        "tp",
        scatter_dimension=0,
        tiled=True,
    )
    return (mixed, log_totals)


MESH = pl.DeviceIdType.MESH
LANES = 128
scope = jax.named_scope


def fused_kernel(
    count,
    tok,
    gain,
    wq,
    wk,
    wv,
    lam,
    hgain,
    wao,
    wpo,
    mixed_out,
    lt_out,
    tok_own,
    gain_own,
    lam_own,
    hgain_own,
    norm_all,
    kv_own,
    q_own,
    kv_relay,
    q_relay,
    q_relay_whole,
    w_kv,
    w_q,
    wa_all,
    wp_own,
    par_own,
    par_in,
    par_use,
    acc_kv,
    acc_q,
    q_all,
    k_all,
    v_all,
    head_own,
    heads_all,
    pooled_all,
    part_out,
    part_in,
    cross_out,
    cross_in,
    block_out,
    block_in,
    pool_in,
    lt_send,
    lt_in,
    local_sem,
    z_send,
    z_recv,
    f_send,
    f_recv,
    kv_send,
    kv_fwd,
    kv_recv,
    q_send,
    q_twin,
    q_recv,
    r_recv,
    w_send,
    w_fwd,
    w_recv,
    par_sem,
    h_send,
    h_recv,
    p_send,
    p_recv,
    x_send,
    x_recv,
    o_send,
    o_recv,
    l_send,
    l_recv,
):
    g = lax.axis_index("grp")
    s = lax.axis_index("sp")
    t = lax.axis_index("tp")
    c = lax.rem(t, 2)
    x = t // 2
    rows, width = tok.shape
    quarter = width // 4
    shard = wq.shape[0]
    part = shard // 2
    pair = 2 * LANES
    group = wpo.shape[0]
    cols = wpo.shape[1]
    half = s // 2
    inner = (s > 0) & (s < count - 1)
    at_home = inner & (c == half)
    away = inner & (c != half)
    sib = t + 1 - 2 * c
    far = lax.rem(t + 2, 4)
    twin = 1 - g
    near = 1 + half
    other = count - 1 - s
    edge = jnp.where(half == 0, 0, count - 1)
    far_edge = count - 1 - edge
    target = 1 + c
    home = 2 * x + half
    f32, bf16 = jnp.float32, jnp.bfloat16

    def span(index, size):
        return pl.ds(pl.multiple_of(index * size, size), size)

    def half_rows(owner, which):
        return pl.ds(pl.multiple_of(owner * shard + which * part, part), part)

    barrier = pltpu.get_barrier_semaphore()

    def greet(where):
        pl.semaphore_signal(barrier, inc=1, device_id=where, device_id_type=MESH)

    for off in range(1, count):
        peer = lax.rem(s + off, count)
        peer_inner = (peer > 0) & (peer < count - 1)

        @pl.when(inner | peer_inner)
        def _():
            greet({"sp": peer})
            greet({"sp": peer, "tp": sib})

    greet({"tp": sib})
    greet({"tp": far})

    @pl.when(inner)
    def _():
        greet({"grp": twin})

    pieces = (
        (tok, tok_own),
        (gain, gain_own),
        (wk, kv_own.at[:, 0:LANES]),
        (wv, kv_own.at[:, LANES:pair]),
        (lam, lam_own),
        (hgain, hgain_own),
        (wao, wa_all.at[0]),
        (wpo, wp_own),
        (wk, w_kv.at[span(s, shard), 0:LANES]),
        (wv, w_kv.at[span(s, shard), LANES:pair]),
        (wq.at[:, span(c, pair)], w_q.at[span(s, shard), :]),
        (wq, q_own),
    )
    local = [
        pltpu.make_async_copy(src, dst, local_sem.at[i]) for i, (src, dst) in enumerate(pieces)
    ]
    for piece in local[:4]:
        piece.start()
    local[11].start()

    local[7].start()

    @pl.when(inner)
    def _():
        for piece in local[4:7]:
            piece.start()

    @pl.when(at_home)
    def _():
        for piece in local[8:11]:
            piece.start()

    def copy(src, dst, send, recv, where):
        return pltpu.make_async_remote_copy(
            src_ref=src,
            dst_ref=dst,
            send_sem=send,
            recv_sem=recv,
            device_id=where,
            device_id_type=MESH,
        )

    chunk = rows // 2

    def z_copy(u, dest):
        place = norm_all.at[span(u, chunk), span(t, quarter)]
        return copy(place, place, z_send.at[0], z_recv.at[u], {"sp": dest})

    def z_outward(u):
        place = norm_all.at[span(u, chunk), span(t, quarter)]
        return copy(place, place, z_send.at[1], z_recv.at[u], {"sp": edge})

    def tok_forward(step, u):
        col = span(far if step == 2 else t, quarter)
        place = norm_all.at[span(u, chunk), col]
        where = {"tp": far if step == 1 else sib}
        got = f_recv.at[u] if step == 1 else f_recv.at[2 * count + step // 2]
        return copy(place, place, f_send.at[step], got, where)

    def tok_late(step, u):
        col = span(far if step == 2 else t, quarter)
        place = norm_all.at[span(u, chunk), col]
        got = f_recv.at[2 * count + 2 + step + lax.rem(u, 2)]
        return copy(place, place, f_send.at[step], got, {"tp": sib})

    def all_sent(ref, sem):
        copy(ref, ref, sem, sem, {"tp": sib}).wait_send()

    def kv_first():
        src = kv_own.at[span(g, part), :]
        dst = w_kv.at[half_rows(s, g), :]
        return copy(src, dst, kv_send.at[0], kv_recv.at[s, g], {"sp": target})

    def kv_first_whole():
        dst = w_kv.at[span(s, shard), :]
        return copy(kv_own, dst, kv_send.at[0], kv_recv.at[s, 0], {"sp": near})

    def kv_beside():
        dst = w_kv.at[span(s, shard), :]
        return copy(kv_own, dst, kv_send.at[1], kv_recv.at[s, 0], {"tp": sib})

    def kv_edge():
        place = w_kv.at[span(edge, shard), :]
        return copy(place, place, kv_fwd.at[0], kv_recv.at[edge, 0], {"tp": sib})

    def kv_forward(kind, owner):
        which = twin if kind == 2 else g
        place = w_kv.at[half_rows(owner, which), :]
        where = {"grp": twin} if kind == 0 else {"tp": sib}
        return copy(place, place, kv_fwd.at[0], kv_recv.at[owner, which], where)

    def kv_arrival(owner, which):
        place = w_kv.at[half_rows(owner, which), :]
        return copy(place, place, kv_fwd.at[0], kv_recv.at[owner, which], {"tp": sib})

    def q_copy(core):
        src = q_own.at[span(g, part), core * pair : (core + 1) * pair]
        dst = w_q.at[half_rows(s, g), :]
        where = {"sp": target, "tp": 2 * x + core}
        return copy(src, dst, q_send.at[0], q_recv.at[s, g], where)

    def q_whole(core):
        src = q_own.at[:, core * pair : (core + 1) * pair]
        dst = w_q.at[span(s, shard), :]
        where = {"sp": near, "tp": 2 * x + core}
        return copy(src, dst, q_send.at[0], q_recv.at[s, 0], where)

    def q_edge():
        place = w_q.at[span(edge, shard), :]
        return copy(place, place, q_twin.at[0], q_recv.at[edge, 0], {"tp": sib})

    def relay_copy(i):
        if i == 0:
            src, dst = kv_own.at[span(g, part), :], kv_relay
        elif i == 1:
            src, dst = q_own.at[span(g, part), 0:pair], q_relay
        else:
            src, dst = q_own.at[:, pair : 2 * pair], q_relay_whole
        send = kv_send.at[0] if i == 0 else q_send.at[0]
        return copy(src, dst, send, r_recv.at[i], {"sp": near})

    def relay_forward(i):
        if i == 0:
            dst = w_kv.at[half_rows(edge, g), :]
            return copy(kv_relay, dst, kv_send.at[2], kv_recv.at[edge, g], {"sp": other})
        where = {"sp": other, "tp": 2 * x + i - 1}
        if i == 1:
            dst = w_q.at[half_rows(edge, g), :]
            return copy(q_relay, dst, q_send.at[2], q_recv.at[edge, g], where)
        dst = w_q.at[span(edge, shard), :]
        return copy(q_relay_whole, dst, q_send.at[2], q_recv.at[edge, 0], where)

    def q_far_whole():
        place = w_q.at[span(far_edge, shard), :]
        return copy(place, place, q_twin.at[0], q_recv.at[far_edge, 0], {"tp": sib})

    def q_beside():
        src = q_own.at[:, span(1 - c, pair)]
        return copy(src, w_q.at[span(s, shard), :], q_send.at[1], q_recv.at[s, 0], {"tp": sib})

    def q_forward(owner):
        place = w_q.at[half_rows(owner, g), :]
        return copy(place, place, q_twin.at[0], q_recv.at[owner, g], {"grp": twin})

    def q_arrival(owner, which):
        place = w_q.at[half_rows(owner, which), :]
        return copy(place, place, q_twin.at[0], q_recv.at[owner, which], {"grp": twin})

    w_rows = (span(g, part // 2), pl.ds(part, part), span(twin, part // 2))

    def w_copy(kind):
        src, dst = wao.at[w_rows[kind], :], wa_all.at[1, w_rows[kind], :]
        return copy(src, dst, w_send.at[kind], w_recv.at[kind], {"sp": near})

    def w_forward():
        place = wa_all.at[1, w_rows[0], :]
        return copy(place, place, w_fwd.at[0], w_recv.at[2], {"grp": twin})

    def w_arrival(kind):
        place = wa_all.at[1, w_rows[kind], :]
        return copy(place, place, w_fwd.at[0], w_recv.at[kind], {"grp": twin})

    def par_copy():
        return copy(par_own, par_in, par_sem.at[0], par_sem.at[1], {"tp": sib})

    head_where = ({"sp": other, "tp": home}, {"tp": sib})

    def head_copy(kind, b):
        dst = heads_all.at[c, span(b, rows), :]
        src = head_own.at[span(b, rows), :]
        return copy(src, dst, h_send.at[kind], h_recv.at[b, c], head_where[kind])

    def head_arrival(b, core):
        place = heads_all.at[core, span(b, rows), :]
        return copy(place, place, h_send.at[0], h_recv.at[b, core], {"tp": sib})

    def lt_copy(b):
        where = {"sp": b, "tp": home}
        return copy(lt_send.at[b], lt_in.at[c], l_send.at[0], l_recv.at[c], where)

    def lt_arrival(core):
        return copy(lt_send.at[0], lt_in.at[core], l_send.at[0], l_recv.at[core], {"tp": sib})

    def part_copy(b, e):
        src = part_out.at[b, e, 1 - c]
        return copy(src, part_in.at[b, e], p_send.at[0], p_recv.at[b, e], {"tp": sib})

    def cross_copy(b, e):
        src = cross_out.at[b, e]
        return copy(src, cross_in.at[b, e], x_send.at[0], x_recv.at[b, e], {"tp": far})

    def out_copy(b, e):
        to = s if e == 0 else edge
        return copy(block_out.at[b, e], block_in.at[to], o_send.at[0], o_recv.at[to], {"sp": b})

    def out_arrival(i):
        return copy(block_out.at[0, 0], block_in.at[i], o_send.at[0], o_recv.at[i], {"sp": near})

    def pool_copy(b):
        dst = pool_in.at[half]
        where = {"sp": b}
        return copy(block_out.at[b, 0], dst, o_send.at[0], o_recv.at[count + half], where)

    def pool_arrival(i):
        dst = pool_in.at[i]
        return copy(block_out.at[0, 0], dst, o_send.at[0], o_recv.at[count + i], {"sp": near})

    local[0].wait()
    local[1].wait()
    step = rows // 2

    def norm_rows(i, carry):
        at = pl.ds(pl.multiple_of(i * step, step), step)
        v = tok_own[at, :].astype(f32)
        scale = lax.rsqrt(jnp.mean(v * v, axis=-1, keepdims=True) + epsilon)
        to = pl.ds(pl.multiple_of(s * rows + i * step, step), step)
        norm_all[to, :] = (v * scale * gain_own[...]).astype(bf16)
        return carry

    with scope("norm"):
        lax.fori_loop(0, rows // step, norm_rows, 0)
    with scope("barrier"):
        pl.semaphore_wait(barrier, jnp.where(inner, 9, 6))
    sends_on = s != target

    @pl.when(inner)
    def _():
        z_copy(2 * s, other).start()
        z_copy(2 * s + 1, other).start()
        z_outward(2 * s).start()
        z_outward(2 * s + 1).start()

    @pl.when(jnp.logical_not(inner))
    def _():
        z_copy(2 * s, near).start()
        z_copy(2 * s + 1, near).start()

    local[2].wait()
    local[3].wait()
    local[11].wait()

    sends_near = jnp.logical_not(inner) & (c == half)

    sends_relay = jnp.logical_not(inner) & (c != half)

    @pl.when(sends_relay)
    def _():
        for i in range(3):
            relay_copy(i).start()

    @pl.when(away)
    def _():
        kv_first().start()
        for core in range(2):
            q_copy(core).start()

    seq = rows * count
    window = jnp.where(t == 0, 2, jnp.where(t == 1, 4, jnp.where(t == 2, 8, 16)))
    half_span = window // 2
    sub = rows // 4

    def pool(b, carry):
        at = b * rows + lax.broadcasted_iota(jnp.int32, (rows, seq), 0)
        col = lax.broadcasted_iota(jnp.int32, (rows, seq), 1)
        inside = (col >= at - half_span) & (col < at + window - half_span)
        band = jnp.where(inside, 1.0, 0.0).astype(bf16)
        total = jnp.dot(band, norm_all[:, span(t, group)], preferred_element_type=f32)
        pos = b * rows + lax.broadcasted_iota(jnp.int32, (rows, 1), 0)
        low = jnp.maximum(pos - half_span, 0)
        high = jnp.minimum(pos + window - half_span, seq)
        own = norm_all[span(b, rows), span(t, group)].astype(f32)
        pooled_all[span(b, rows), :] = (total / (high - low).astype(f32) - own).astype(bf16)
        return carry

    def hand_parts(b, e, total):
        for j in range(4):
            part_out[b, e, j % 2, j // 2] = total[j * sub : (j + 1) * sub, :].astype(bf16)
        part_copy(b, e).start()

    def pool_product(b):
        return jnp.dot(pooled_all[span(b, rows), :], wp_own[...], preferred_element_type=f32)

    def second_sum(b, e):
        part_copy(b, e).wait_recv()
        cross_out[b, e] = (
            part_out[b, e, c, 1 - x].astype(f32) + part_in[b, e, 1 - x].astype(f32)
        ).astype(bf16)
        cross_copy(b, e).start()

    def third_sum(b, e, send):
        cross_copy(b, e).wait_recv()
        block_out[b, e] = (
            part_out[b, e, c, x].astype(f32)
            + part_in[b, e, x].astype(f32)
            + cross_in[b, e].astype(f32)
        ).astype(bf16)

        @pl.when(b != s)
        def _():
            send().start()

    def outer_work():
        with scope("otok"):
            for u in (2 * near, 2 * near + 1, 2 * (count - 1 - near)):
                z_copy(u, near).wait_recv()

            @pl.when(sends_near)
            def _():
                kv_first_whole().start()
                for core in range(2):
                    q_whole(core).start()
                w_copy(0).start()
                w_copy(1).start()

            z_copy(2 * (count - 1 - near) + 1, near).wait_recv()
            z_copy(2 * far_edge, near).wait_recv()
            z_copy(2 * far_edge + 1, near).wait_recv()
        with scope("opool"):
            lax.fori_loop(0, count, pool, 0)

        @pl.when(sends_relay)
        def _():
            w_copy(0).start()
            w_copy(1).start()

        local[7].wait()

        def outer_steps(m, carry):
            @pl.when((m >= 1) & (m < count + 1))
            def _():
                second_sum(m - 1, 0)

            @pl.when(m < count)
            def _():
                hand_parts(m, 0, pool_product(m))

            @pl.when(m >= 2)
            def _():
                third_sum(m - 2, 0, lambda: pool_copy(m - 2))

            return carry

        with scope("osum"):
            lax.fori_loop(0, count + 2, outer_steps, 0)

    pl.when(jnp.logical_not(inner))(outer_work)

    def inner_work():
        @pl.when(at_home)
        def _():
            kv_beside().start()
            q_beside().start()

        local[4].wait()
        local[5].wait()
        par_own[0:count, :] = hgain_own[...]
        for i in range(count):
            par_own[count + i : count + i + 1, :] = jnp.full((1, LANES), lam_own[i], f32)

        @pl.when(at_home)
        def _():
            par_copy().start()

        def tok_in(u, onward, beside=tok_forward):
            z_copy(u, other).wait_recv()
            if onward:
                z_copy(u, other).start()
            else:
                z_outward(u).start()
            tok_forward(1, u).start()
            beside(0, u).start()

        def tok_x(u, beside=tok_forward):
            tok_forward(1, u).wait_recv()
            beside(2, u).start()

        def kv_in(owner):
            @pl.when(at_home)
            def _():
                kv_arrival(owner, g).wait_recv()
                kv_forward(0, owner).start()
                kv_forward(1, owner).start()

        def r_arrive(i):
            relay_copy(i).wait_recv()
            relay_forward(i).start()

        def kv_y(owner):
            @pl.when(at_home)
            def _():
                kv_arrival(owner, twin).wait_recv()
                kv_forward(2, owner).start()

        def q_in(owner):
            q_arrival(owner, g).wait_recv()
            q_forward(owner).start()

        owners = (edge, other, far_edge)
        split = (other, far_edge)
        with scope("tok0"):
            tok_in(2 * edge, True)
            tok_in(2 * other, False)
        with scope("tok1"):
            tok_in(2 * edge + 1, True)
            tok_in(2 * other + 1, False)
        with scope("relay0"):

            @pl.when(away)
            def _():
                r_arrive(0)

        with scope("kv1"):
            kv_in(other)
        with scope("x0"):
            tok_x(2 * edge)
            tok_x(2 * other)
        with scope("q1"):
            q_in(other)
        with scope("relay1"):

            @pl.when(away)
            def _():
                r_arrive(1)

        with scope("tok2"):
            tok_in(2 * far_edge, False, tok_late)
        with scope("kvy1"):
            kv_y(other)
        with scope("x1"):
            tok_x(2 * edge + 1)
            tok_x(2 * other + 1)
        with scope("tok3"):
            tok_in(2 * far_edge + 1, False, tok_late)
        with scope("relay2"):

            @pl.when(away)
            def _():
                r_arrive(2)

        with scope("kv0"):

            @pl.when(at_home)
            def _():
                kv_edge().wait_recv()
                kv_edge().start()

        with scope("kv2"):
            kv_in(far_edge)
        with scope("pool"):
            lax.fori_loop(0, count, pool, 0)
        with scope("q2"):

            @pl.when(c == 0)
            def _():
                q_in(far_edge)

        with scope("x2"):
            tok_x(2 * far_edge, tok_late)
            tok_x(2 * far_edge + 1, tok_late)

        early = pl.ds(pl.multiple_of(half * rows, rows), 3 * rows)
        late = span(far_edge, rows)
        k_early = pl.ds(pl.multiple_of(half * shard, shard), 3 * shard)
        k_late = span(far_edge, shard)

        def early_product(store, w):
            store[...] = jnp.dot(
                norm_all[early, k_early], w[k_early, :], preferred_element_type=f32
            )

        def late_product(store, w, put):
            acc = store[...] + jnp.dot(
                norm_all[early, k_late], w[k_late, :], preferred_element_type=f32
            )
            put(early, acc.astype(bf16))
            acc = jnp.dot(norm_all[late, :], w[...], preferred_element_type=f32)
            put(late, acc.astype(bf16))

        def early_tokens(step):
            place = norm_all.at[0 : 2 * rows, 0:quarter]
            got = f_recv.at[2 * count + step // 2]
            return copy(place, place, f_send.at[step], got, {"tp": sib})

        with scope("earlykv"):
            for step in (0, 2):
                early_tokens(step).wait_recv()

            @pl.when(at_home)
            def _():
                local[8].wait()
                local[9].wait()
                local[10].wait()

            @pl.when(away)
            def _():
                kv_edge().wait_recv()
                kv_arrival(other, g).wait_recv()
                kv_arrival(other, twin).wait_recv()
                kv_beside().wait_recv()
                q_beside().wait_recv()
                par_copy().wait_recv()

            early_product(acc_kv, w_kv)
        with scope("kvy2"):
            kv_y(far_edge)
        with scope("earlyq"):
            q_edge().wait_recv()
            q_arrival(other, twin).wait_recv()
            early_product(acc_q, w_q)
        with scope("rest"):
            for step in (0, 2):
                for u in (2 * far_edge, 2 * far_edge + 1):
                    tok_late(step, u).wait_recv()
        with scope("kvrest"):

            @pl.when(away)
            def _():
                kv_arrival(far_edge, g).wait_recv()
                kv_arrival(far_edge, twin).wait_recv()

        def put_kv(at, value):
            k_all[at, :] = value[:, 0:LANES]
            v_all[at, :] = value[:, LANES:pair]

        def put_q(at, value):
            q_all[at, :] = value

        with scope("projkv"):
            late_product(acc_kv, w_kv, put_kv)
        with scope("qrest"):

            @pl.when(c == 0)
            def _():
                q_arrival(far_edge, twin).wait_recv()

            @pl.when(c == 1)
            def _():
                q_far_whole().wait_recv()

        with scope("projq"):
            late_product(acc_q, w_q, put_q)

        par_use[...] = jnp.where(at_home, par_own[...], par_in[...])
        lane = lax.broadcasted_iota(jnp.int32, (rows, LANES), 1)
        lt_rows = lt_send.shape[2]
        base = HD ** (-0.5)

        def one_head(b, h):
            head = 2 * c + h
            q = q_all[span(b, rows), h * LANES : (h + 1) * LANES]
            zero = jnp.zeros_like(q)
            both_q = jnp.concatenate(
                [jnp.where(lane < HD, q, zero), jnp.where(lane < HD, zero, q)], axis=0
            )
            raw = lax.dot_general(
                both_q, k_all[...], (((1,), (1,)), ((), ())), preferred_element_type=f32
            )
            highest = jnp.max(raw, axis=-1, keepdims=True)
            weights = jnp.exp2((raw - highest) * (base * math.log2(math.e)))
            totals = jnp.sum(weights, axis=-1, keepdims=True)
            reads = jnp.dot(weights.astype(bf16), v_all[...], preferred_element_type=f32) / totals
            logs = highest * base + jnp.log(totals)
            contrast = reads[:rows] - par_use[pl.ds(count + head, 1), :] * reads[rows:]
            scaled = (
                contrast
                * lax.rsqrt(jnp.mean(contrast * contrast, axis=-1, keepdims=True) + epsilon)
                * par_use[pl.ds(head, 1), :]
            ).astype(bf16)
            return scaled, logs[:rows], logs[rows:]

        def attend(b):
            done = [one_head(b, h) for h in range(2)]
            for h in range(2):
                head_own[span(b, rows), h * LANES : (h + 1) * LANES] = done[h][0]
            head_copy(0, b).start()

            @pl.when(away)
            def _():
                head_copy(1, b).start()

            @pl.when(at_home)
            def _():
                heads_all[c, span(b, rows), :] = head_own[span(b, rows), :]

            both = jnp.where(
                lane < 2,
                jnp.where(lane == 0, done[0][1], done[0][2]),
                jnp.where(lane == 2, done[1][1], done[1][2]),
            )
            padded = jnp.concatenate([both, jnp.zeros((lt_rows - rows, LANES), f32)], axis=0)
            lt_send[b] = jnp.transpose(padded)[0:8, :]

            @pl.when(jnp.logical_not(at_home & (b == s)))
            def _():
                lt_copy(b).start()

        def first_sum(b):
            for core in range(2):

                @pl.when(jnp.logical_not(at_home & (c == core)))
                def _():
                    head_arrival(b, core).wait_recv()

            for e in range(2):
                if e == 1:

                    @pl.when(b == 0)
                    def _():
                        with scope("wrest"):
                            w_arrival(1).wait_recv()
                            w_arrival(2).wait_recv()

                total = sum(
                    jnp.dot(
                        heads_all[core, span(b, rows), :],
                        wa_all[e, core * pair : (core + 1) * pair, :],
                        preferred_element_type=f32,
                    )
                    for core in range(2)
                )
                hand_parts(b, e, total + pool_product(b) if e == 0 else total)

        def nth(m):
            return jnp.where(m < 2, (count - 1) * m, m - 1)

        def attend_all(m, carry):
            with scope("att"):
                attend(nth(m))

            @pl.when(m == 0)
            def _():
                with scope("wao"):
                    w_arrival(0).wait_recv()
                    w_forward().start()

            return carry

        lax.fori_loop(0, count, attend_all, 0)
        local[6].wait()
        local[7].wait()

        def steps(m, carry):
            @pl.when(m < count)
            def _():
                with scope("S1"):
                    first_sum(nth(m))
                with scope("S2"):
                    for e in range(2):
                        second_sum(nth(m), e)

            @pl.when(m >= 2)
            def _():
                with scope("S3"):
                    for e in range(2):
                        third_sum(nth(m - 2), e, lambda: out_copy(nth(m - 2), e))

            return carry

        lax.fori_loop(0, count + 2, steps, 0)

    pl.when(inner)(inner_work)

    def put_logs(core, ref, at):
        for h in range(2):
            for m in range(2):
                i = 2 * core + h
                lt_out[m, i : i + 1, :] = ref[at, 2 * h + m : 2 * h + m + 1, 0:rows]

    for core in range(2):

        @pl.when(at_home & (c == core))
        def _():
            put_logs(core, lt_send, s)

        @pl.when(jnp.logical_not(at_home & (c == core)))
        def _():
            lt_arrival(core).wait_recv()
            put_logs(core, lt_in, core)

    for i in range(count):
        with scope(f"final{i}"):
            at = slice(i * cols, (i + 1) * cols)
            maker = min(max(i, 1), count - 2)
            e = 0 if i == maker else 1

            @pl.when(s == maker)
            def _():
                mixed_out[:, at] = block_out[s, e]

            @pl.when(s != maker)
            def _():
                out_arrival(i).wait_recv()
                mixed_out[:, at] = block_in[i]

            if e == 1:
                which = i // (count - 1)

                @pl.when(s == i)
                def _():
                    both = mixed_out[:, at].astype(f32) + block_out[s, 0].astype(f32)
                    mixed_out[:, at] = both.astype(bf16)

                @pl.when(s != i)
                def _():
                    pool_arrival(which).wait_recv()
                    both = mixed_out[:, at].astype(f32) + pool_in[which].astype(f32)
                    mixed_out[:, at] = both.astype(bf16)

    @pl.when(sends_near)
    def _():
        kv_first_whole().wait_send()
        all_sent(w_q.at[0 : 2 * shard, :], q_send.at[0])

    @pl.when(sends_relay)
    def _():
        relay_copy(0).wait_send()
        all_sent(w_q.at[0 : shard + part, :], q_send.at[0])

    @pl.when(away)
    def _():
        kv_first().wait_send()
        all_sent(w_q.at[0:shard, :], q_send.at[0])
        relay_forward(0).wait_send()
        all_sent(w_q.at[0 : shard + part, :], q_send.at[2])

    @pl.when(jnp.logical_not(inner))
    def _():
        all_sent(norm_all.at[0:rows, 0:quarter], z_send.at[0])
        w_copy(0).wait_send()
        w_copy(1).wait_send()
        all_sent(part_in.at[:, 0], p_send.at[0])
        all_sent(cross_in.at[:, 0], x_send.at[0])
        all_sent(block_out.at[0 : count - 1, 0], o_send.at[0])

    @pl.when(at_home)
    def _():
        kv_beside().wait_send()
        q_beside().wait_send()
        par_copy().wait_send()
        all_sent(w_kv, kv_fwd.at[0])

    @pl.when(away)
    def _():
        all_sent(head_own, h_send.at[1])

    @pl.when(inner)
    def _():
        all_sent(norm_all.at[0 : 2 * rows, 0:quarter], z_send.at[0])
        for sem in (z_send.at[1], f_send.at[0], f_send.at[1], f_send.at[2]):
            all_sent(norm_all.at[0 : 3 * rows, 0:quarter], sem)

        @pl.when(c == 0)
        def _():
            all_sent(w_q.at[0:shard, :], q_twin.at[0])

        @pl.when(c == 1)
        def _():
            all_sent(w_q.at[0:part, :], q_twin.at[0])

        w_forward().wait_send()
        all_sent(head_own, h_send.at[0])
        all_sent(part_in, p_send.at[0])
        all_sent(cross_in, x_send.at[0])
        all_sent(block_out.at[0 : count - 1], o_send.at[0])

    @pl.when(inner & jnp.logical_not(at_home))
    def _():
        all_sent(lt_send, l_send.at[0])

    @pl.when(at_home)
    def _():
        all_sent(lt_send.at[0 : count - 1], l_send.at[0])


def fused(
    count,
    tokens,
    norm_gain,
    query_weight,
    key_weight,
    value_weight,
    map_lambda,
    head_gain,
    attn_out_weight,
    pool_out_weight,
):
    rows, width = tokens.shape
    group, cols = pool_out_weight.shape
    shard = query_weight.shape[0]
    sub = rows // 4
    seq = rows * count
    pair = 2 * LANES
    lt_rows = -(-rows // LANES) * LANES
    bf16, f32 = jnp.bfloat16, jnp.float32
    vmem = pl.BlockSpec(memory_space=pltpu.VMEM)
    far = pl.BlockSpec(memory_space=pl.ANY)
    sems = pltpu.SemaphoreType.DMA
    return pl.pallas_call(
        functools.partial(fused_kernel, count),
        out_shape=(
            pltpu.VMEM((sub, width), bf16),
            pltpu.VMEM((2, count, rows), f32),
        ),
        in_specs=[far] * 9,
        out_specs=(vmem, vmem),
        scratch_shapes=[
            pltpu.VMEM((rows, width), bf16),
            pltpu.VMEM((1, width), f32),
            pltpu.SMEM((count,), f32),
            pltpu.VMEM((count, LANES), f32),
            pltpu.VMEM((seq, width), bf16),
            pltpu.VMEM((shard, pair), bf16),
            pltpu.VMEM((shard, count * LANES), bf16),
            pltpu.VMEM((shard // 2, pair), bf16),
            pltpu.VMEM((shard // 2, pair), bf16),
            pltpu.VMEM((shard, pair), bf16),
            pltpu.VMEM((width, pair), bf16),
            pltpu.VMEM((width, pair), bf16),
            pltpu.VMEM((2, group, cols), bf16),
            pltpu.VMEM((group, cols), bf16),
            pltpu.VMEM((2 * count, LANES), f32),
            pltpu.VMEM((2 * count, LANES), f32),
            pltpu.VMEM((2 * count, LANES), f32),
            pltpu.VMEM((3 * rows, pair), f32),
            pltpu.VMEM((3 * rows, pair), f32),
            pltpu.VMEM((seq, pair), bf16),
            pltpu.VMEM((seq, LANES), bf16),
            pltpu.VMEM((seq, LANES), bf16),
            pltpu.VMEM((seq, pair), bf16),
            pltpu.VMEM((2, seq, pair), bf16),
            pltpu.VMEM((seq, group), bf16),
            pltpu.VMEM((count, 2, 2, 2, sub, cols), bf16),
            pltpu.VMEM((count, 2, 2, sub, cols), bf16),
            pltpu.VMEM((count, 2, sub, cols), bf16),
            pltpu.VMEM((count, 2, sub, cols), bf16),
            pltpu.VMEM((count, 2, sub, cols), bf16),
            pltpu.VMEM((count, sub, cols), bf16),
            pltpu.VMEM((2, sub, cols), bf16),
            pltpu.VMEM((count, 8, lt_rows), f32),
            pltpu.VMEM((2, 8, lt_rows), f32),
            sems((12,)),
            sems((2,)),
            sems((2 * count,)),
            sems((3,)),
            sems((2 * count + 6,)),
            sems((3,)),
            sems((1,)),
            sems((count, 2)),
            sems((3,)),
            sems((1,)),
            sems((count, 2)),
            sems((3,)),
            sems((2,)),
            sems((1,)),
            sems((3,)),
            sems((2,)),
            sems((2,)),
            sems((count, 2)),
            sems((1,)),
            sems((count, 2)),
            sems((1,)),
            sems((count, 2)),
            sems((1,)),
            sems((count + 2,)),
            sems((1,)),
            sems((2,)),
        ],
        compiler_params=pltpu.CompilerParams(collective_id=0, has_side_effects=True),
    )(
        tokens,
        norm_gain.reshape(1, width),
        query_weight,
        key_weight,
        value_weight,
        map_lambda,
        head_gain,
        attn_out_weight,
        pool_out_weight,
    )


def fits(shape, tokens, query_weight, value_weight, map_lambda, pool_out_weight):
    count = shape["sp"]
    return (
        shape["grp"] == 2
        and shape["tp"] == 4
        and count == 4
        and map_lambda.shape[0] == count
        and value_weight.shape[1] == VD == LANES == 2 * HD
        and tokens.shape[0] % 32 == 0
        and tokens.shape[1] % (4 * LANES) == 0
        and query_weight.shape[0] % 32 == 0
        and query_weight.shape[1] == count * LANES
        and pool_out_weight.shape[0] * 4 == tokens.shape[1]
        and pool_out_weight.shape[1] % LANES == 0
        and pool_out_weight.shape[1] * count == tokens.shape[1]
        and pool_out_weight.shape[0] == pool_out_weight.shape[1]
        and pool_out_weight.shape[0] == query_weight.shape[0]
        and tokens.shape[0] * count * tokens.shape[1] <= 1 << 22
    )


def solution(mesh):
    placed = (
        P(("grp", "sp"), None),
        P(),
        P("sp", "tp"),
        P("sp", "tp"),
        P("sp", "tp"),
        P("tp"),
        P("tp", None),
        P("tp", "sp"),
        P("tp", "sp"),
    )
    shape = dict(mesh.shape)

    def chosen(*args):
        if fits(shape, args[0], args[2], args[4], args[5], args[8]):
            return fused(shape["sp"], *args)
        return on_device(*args)

    return jax.shard_map(
        chosen,
        mesh=mesh,
        in_specs=placed,
        out_specs=(P(("grp", "sp", "tp"), None), P(None, "tp", ("grp", "sp"))),
        check_vma=False,
    )
```

```python
import functools
import math

import jax
import jax.numpy as jnp
from jax import lax
from jax.experimental import pallas as pl
from jax.experimental.pallas import tpu as pltpu
from jax.sharding import PartitionSpec as P

HD = 64
VD = 128
POOL_SPAN = 16


epsilon = 1e-06
very_low = -1e30


def extended(cells, sides, width):
    for axis, dim in sides:
        count = lax.axis_size(axis)
        ends = count - 1
        head = lax.slice_in_dim(cells, 0, width, axis=dim)
        tail = lax.slice_in_dim(cells, cells.shape[dim] - width, cells.shape[dim], axis=dim)
        cells = jnp.concatenate(
            [
                lax.ppermute(tail, axis, [(i, (i + 1) % count) for i in range(ends)]),
                cells,
                lax.ppermute(head, axis, [((i + 1) % count, i) for i in range(ends)]),
            ],
            axis=dim,
        )
    return cells


def add_products(totals, pieces, source):
    results = []
    for running, piece in zip(totals, pieces):
        results.append(jnp.dot(source, piece, preferred_element_type=jnp.float32))
    return tuple(results)


def on_device(
    tokens,
    norm_gain,
    query_weight,
    key_weight,
    value_weight,
    map_lambda,
    head_gain,
    attn_out_weight,
    pool_out_weight,
):
    tokens_wide = tokens.astype(jnp.float32)
    normed = (
        tokens_wide
        * lax.rsqrt(jnp.mean(tokens_wide * tokens_wide, axis=-1, keepdims=True) + epsilon)
        * norm_gain
    ).astype(jnp.bfloat16)
    row_count = normed.shape[0]
    sp_index = lax.axis_index("sp")
    tp_index = lax.axis_index("tp")
    group_width = pool_out_weight.shape[0]
    local_heads = map_lambda.shape[0]
    key_heads = value_weight.shape[1] // VD
    group_heads = local_heads // key_heads
    q_empty = jnp.zeros((row_count, query_weight.shape[1]), jnp.float32)
    k_empty = jnp.zeros((row_count, key_weight.shape[1]), jnp.float32)
    v_empty = jnp.zeros((row_count, value_weight.shape[1]), jnp.float32)
    q_acc, k_acc, v_acc = add_products(
        (q_empty, k_empty, v_empty),
        (
            lax.all_gather(query_weight, "sp", axis=0, tiled=True),
            lax.all_gather(key_weight, "sp", axis=0, tiled=True),
            lax.all_gather(value_weight, "sp", axis=0, tiled=True),
        ),
        normed,
    )
    queries = q_acc.astype(jnp.bfloat16).reshape(row_count, key_heads, group_heads, 2, HD)
    keys_flat = k_acc.astype(jnp.bfloat16)
    values_flat = v_acc.astype(jnp.bfloat16)

    def key_block(state_now, key_pair):
        maxima, totals, accums = state_now
        key_blk, val_blk = key_pair
        scores = jnp.einsum(
            "qhgmd,khmd->hgmqk", queries, key_blk, preferred_element_type=jnp.float32
        ) * HD ** (-0.5)
        highest = jnp.maximum(maxima, jnp.max(scores, axis=-1))
        factor = jnp.exp(maxima - highest)
        weights = jnp.exp(scores - highest[..., None])
        totals = totals * factor + jnp.sum(weights, axis=-1)
        accums = accums * factor[..., None] + jnp.einsum(
            "hgmqk,khe->hgmqe",
            weights.astype(jnp.bfloat16),
            val_blk,
            preferred_element_type=jnp.float32,
        )
        return ((highest, totals, accums), None)

    start_state = (
        jnp.full((key_heads, group_heads, 2, row_count), very_low, jnp.float32),
        jnp.zeros((key_heads, group_heads, 2, row_count), jnp.float32),
        jnp.zeros((key_heads, group_heads, 2, row_count, VD), jnp.float32),
    )
    key_piece = lax.all_gather(keys_flat, "sp", axis=0, tiled=True)
    val_piece = lax.all_gather(values_flat, "sp", axis=0, tiled=True)
    piece_len = key_piece.shape[0]
    block_len = math.gcd(piece_len, 512)
    key_blocks = key_piece.reshape(piece_len // block_len, block_len, key_heads, 2, HD)
    val_blocks = val_piece.reshape(piece_len // block_len, block_len, key_heads, VD)
    state_next, unused = lax.scan(key_block, start_state, (key_blocks, val_blocks))
    maxima, totals, accums = state_next
    log_parts = maxima + jnp.log(totals)
    log_totals = jnp.transpose(log_parts, (2, 0, 1, 3)).reshape(2, local_heads, row_count)
    reads = accums / totals[..., None]
    contrast = reads[:, :, 0] - map_lambda.reshape(key_heads, group_heads, 1, 1) * reads[:, :, 1]
    scaled = (
        contrast
        * lax.rsqrt(jnp.mean(contrast * contrast, axis=-1, keepdims=True) + epsilon)
        * head_gain.reshape(key_heads, group_heads, 1, VD)
    )
    attention_head_rows = (
        jnp.transpose(scaled, (2, 0, 1, 3))
        .reshape(row_count, local_heads * VD)
        .astype(jnp.bfloat16)
    )
    head_rows, log_totals = (attention_head_rows, log_totals)
    own_chan = lax.dynamic_slice_in_dim(normed, tp_index * group_width, group_width, 1)
    reach = POOL_SPAN // 2
    padded = extended(own_chan, (("sp", 0),), reach)
    window = jnp.left_shift(jnp.int32(2), tp_index)
    half_span = window // 2
    running = jnp.zeros((row_count, group_width), jnp.float32)
    for offset in range(POOL_SPAN):
        piece = lax.dynamic_slice_in_dim(padded, reach - half_span + offset, row_count, 0).astype(
            jnp.float32
        )
        running = running + jnp.where(offset < window, piece, 0.0)
    seq_len = row_count * lax.axis_size("sp")
    position = sp_index * row_count + jnp.arange(row_count, dtype=jnp.int32)
    lower_edge = jnp.clip(position - half_span, 0, seq_len)
    upper_edge = jnp.clip(position + window - half_span, 0, seq_len)
    counts_f = (upper_edge - lower_edge).astype(jnp.float32)[:, None]
    pooled = (running / counts_f - own_chan.astype(jnp.float32)).astype(jnp.bfloat16)
    attn_whole, pool_whole = (
        lax.all_gather(attn_out_weight, "sp", axis=1, tiled=True),
        lax.all_gather(pool_out_weight, "sp", axis=1, tiled=True),
    )
    mixed = lax.psum_scatter(
        (
            jnp.dot(head_rows, attn_whole, preferred_element_type=jnp.float32)
            + jnp.dot(pooled, pool_whole, preferred_element_type=jnp.float32)
        ).astype(jnp.bfloat16),
        "tp",
        scatter_dimension=0,
        tiled=True,
    )
    return (mixed, log_totals)


MESH = pl.DeviceIdType.MESH
LANES = 128
scope = jax.named_scope


def fused_kernel(
    count,
    tok,
    gain,
    wq,
    wk,
    wv,
    lam,
    hgain,
    wao,
    wpo,
    mixed_out,
    lt_out,
    tok_own,
    gain_own,
    lam_own,
    hgain_own,
    norm_all,
    kv_own,
    q_own,
    kv_relay,
    q_relay,
    q_relay_whole,
    w_kv,
    w_q,
    wa_all,
    wp_own,
    par_own,
    par_in,
    par_use,
    acc_kv,
    acc_q,
    q_all,
    k_all,
    v_all,
    head_own,
    heads_all,
    pooled_all,
    part_out,
    part_in,
    cross_out,
    cross_in,
    block_out,
    block_in,
    pool_in,
    lt_send,
    lt_in,
    local_sem,
    z_send,
    z_recv,
    f_send,
    f_recv,
    kv_send,
    kv_fwd,
    kv_recv,
    q_send,
    q_twin,
    q_recv,
    r_recv,
    w_send,
    w_fwd,
    w_recv,
    par_sem,
    h_send,
    h_recv,
    p_send,
    p_recv,
    x_send,
    x_recv,
    o_send,
    o_recv,
    l_send,
    l_recv,
):
    g = lax.axis_index("grp")
    s = lax.axis_index("sp")
    t = lax.axis_index("tp")
    c = lax.rem(t, 2)
    x = t // 2
    rows, width = tok.shape
    quarter = width // 4
    shard = wq.shape[0]
    part = shard // 2
    pair = 2 * LANES
    group = wpo.shape[0]
    cols = wpo.shape[1]
    half = s // 2
    inner = (s > 0) & (s < count - 1)
    at_home = inner & (c == half)
    away = inner & (c != half)
    sib = t + 1 - 2 * c
    far = lax.rem(t + 2, 4)
    twin = 1 - g
    near = 1 + half
    other = count - 1 - s
    edge = jnp.where(half == 0, 0, count - 1)
    far_edge = count - 1 - edge
    target = 1 + c
    home = 2 * x + half
    f32, bf16 = jnp.float32, jnp.bfloat16

    def span(index, size):
        return pl.ds(pl.multiple_of(index * size, size), size)

    def half_rows(owner, which):
        return pl.ds(pl.multiple_of(owner * shard + which * part, part), part)

    barrier = pltpu.get_barrier_semaphore()

    def greet(where):
        pl.semaphore_signal(barrier, inc=1, device_id=where, device_id_type=MESH)

    for off in range(1, count):
        peer = lax.rem(s + off, count)
        peer_inner = (peer > 0) & (peer < count - 1)

        @pl.when(inner | peer_inner)
        def _():
            greet({"sp": peer})
            greet({"sp": peer, "tp": sib})

    greet({"tp": sib})
    greet({"tp": far})

    @pl.when(inner)
    def _():
        greet({"grp": twin})

    pieces = (
        (tok, tok_own),
        (gain, gain_own),
        (wk, kv_own.at[:, 0:LANES]),
        (wv, kv_own.at[:, LANES:pair]),
        (lam, lam_own),
        (hgain, hgain_own),
        (wao, wa_all.at[0]),
        (wpo, wp_own),
        (wk, w_kv.at[span(s, shard), 0:LANES]),
        (wv, w_kv.at[span(s, shard), LANES:pair]),
        (wq.at[:, span(c, pair)], w_q.at[span(s, shard), :]),
        (wq, q_own),
    )
    local = [
        pltpu.make_async_copy(src, dst, local_sem.at[i]) for i, (src, dst) in enumerate(pieces)
    ]
    for piece in local[:4]:
        piece.start()
    local[11].start()

    local[7].start()

    @pl.when(inner)
    def _():
        for piece in local[4:7]:
            piece.start()

    @pl.when(at_home)
    def _():
        for piece in local[8:11]:
            piece.start()

    def copy(src, dst, send, recv, where):
        return pltpu.make_async_remote_copy(
            src_ref=src,
            dst_ref=dst,
            send_sem=send,
            recv_sem=recv,
            device_id=where,
            device_id_type=MESH,
        )

    chunk = rows // 2

    def z_copy(u, dest):
        place = norm_all.at[span(u, chunk), span(t, quarter)]
        return copy(place, place, z_send.at[0], z_recv.at[u], {"sp": dest})

    def z_outward(u):
        place = norm_all.at[span(u, chunk), span(t, quarter)]
        return copy(place, place, z_send.at[1], z_recv.at[u], {"sp": edge})

    def tok_forward(step, u):
        col = span(far if step == 2 else t, quarter)
        place = norm_all.at[span(u, chunk), col]
        where = {"tp": far if step == 1 else sib}
        got = f_recv.at[u] if step == 1 else f_recv.at[2 * count + step // 2]
        return copy(place, place, f_send.at[step], got, where)

    def tok_late(step, u):
        col = span(far if step == 2 else t, quarter)
        place = norm_all.at[span(u, chunk), col]
        got = f_recv.at[2 * count + 2 + step + lax.rem(u, 2)]
        return copy(place, place, f_send.at[step], got, {"tp": sib})

    def all_sent(ref, sem):
        copy(ref, ref, sem, sem, {"tp": sib}).wait_send()

    def kv_first():
        src = kv_own.at[span(g, part), :]
        dst = w_kv.at[half_rows(s, g), :]
        return copy(src, dst, kv_send.at[0], kv_recv.at[s, g], {"sp": target})

    def kv_first_whole():
        dst = w_kv.at[span(s, shard), :]
        return copy(kv_own, dst, kv_send.at[0], kv_recv.at[s, 0], {"sp": near})

    def kv_beside():
        dst = w_kv.at[span(s, shard), :]
        return copy(kv_own, dst, kv_send.at[1], kv_recv.at[s, 0], {"tp": sib})

    def kv_edge():
        place = w_kv.at[span(edge, shard), :]
        return copy(place, place, kv_fwd.at[0], kv_recv.at[edge, 0], {"tp": sib})

    def kv_forward(kind, owner):
        which = twin if kind == 2 else g
        place = w_kv.at[half_rows(owner, which), :]
        where = {"grp": twin} if kind == 0 else {"tp": sib}
        return copy(place, place, kv_fwd.at[0], kv_recv.at[owner, which], where)

    def kv_arrival(owner, which):
        place = w_kv.at[half_rows(owner, which), :]
        return copy(place, place, kv_fwd.at[0], kv_recv.at[owner, which], {"tp": sib})

    def q_copy(core):
        src = q_own.at[span(g, part), core * pair : (core + 1) * pair]
        dst = w_q.at[half_rows(s, g), :]
        where = {"sp": target, "tp": 2 * x + core}
        return copy(src, dst, q_send.at[0], q_recv.at[s, g], where)

    def q_whole(core):
        src = q_own.at[:, core * pair : (core + 1) * pair]
        dst = w_q.at[span(s, shard), :]
        where = {"sp": near, "tp": 2 * x + core}
        return copy(src, dst, q_send.at[0], q_recv.at[s, 0], where)

    def q_edge():
        place = w_q.at[span(edge, shard), :]
        return copy(place, place, q_twin.at[0], q_recv.at[edge, 0], {"tp": sib})

    def relay_copy(i):
        if i == 0:
            src, dst = kv_own.at[span(g, part), :], kv_relay
        elif i == 1:
            src, dst = q_own.at[span(g, part), 0:pair], q_relay
        else:
            src, dst = q_own.at[:, pair : 2 * pair], q_relay_whole
        send = kv_send.at[0] if i == 0 else q_send.at[0]
        return copy(src, dst, send, r_recv.at[i], {"sp": near})

    def relay_forward(i):
        if i == 0:
            dst = w_kv.at[half_rows(edge, g), :]
            return copy(kv_relay, dst, kv_send.at[2], kv_recv.at[edge, g], {"sp": other})
        where = {"sp": other, "tp": 2 * x + i - 1}
        if i == 1:
            dst = w_q.at[half_rows(edge, g), :]
            return copy(q_relay, dst, q_send.at[2], q_recv.at[edge, g], where)
        dst = w_q.at[span(edge, shard), :]
        return copy(q_relay_whole, dst, q_send.at[2], q_recv.at[edge, 0], where)

    def q_far_whole():
        place = w_q.at[span(far_edge, shard), :]
        return copy(place, place, q_twin.at[0], q_recv.at[far_edge, 0], {"tp": sib})

    def q_beside():
        src = q_own.at[:, span(1 - c, pair)]
        return copy(src, w_q.at[span(s, shard), :], q_send.at[1], q_recv.at[s, 0], {"tp": sib})

    def q_forward(owner):
        place = w_q.at[half_rows(owner, g), :]
        return copy(place, place, q_twin.at[0], q_recv.at[owner, g], {"grp": twin})

    def q_arrival(owner, which):
        place = w_q.at[half_rows(owner, which), :]
        return copy(place, place, q_twin.at[0], q_recv.at[owner, which], {"grp": twin})

    w_rows = (span(g, part // 2), pl.ds(part, part), span(twin, part // 2))

    def w_copy(kind):
        src, dst = wao.at[w_rows[kind], :], wa_all.at[1, w_rows[kind], :]
        return copy(src, dst, w_send.at[kind], w_recv.at[kind], {"sp": near})

    def w_forward():
        place = wa_all.at[1, w_rows[0], :]
        return copy(place, place, w_fwd.at[0], w_recv.at[2], {"grp": twin})

    def w_arrival(kind):
        place = wa_all.at[1, w_rows[kind], :]
        return copy(place, place, w_fwd.at[0], w_recv.at[kind], {"grp": twin})

    def par_copy():
        return copy(par_own, par_in, par_sem.at[0], par_sem.at[1], {"tp": sib})

    head_where = ({"sp": other, "tp": home}, {"tp": sib})

    def head_copy(kind, b):
        dst = heads_all.at[c, span(b, rows), :]
        src = head_own.at[span(b, rows), :]
        return copy(src, dst, h_send.at[kind], h_recv.at[b, c], head_where[kind])

    def head_arrival(b, core):
        place = heads_all.at[core, span(b, rows), :]
        return copy(place, place, h_send.at[0], h_recv.at[b, core], {"tp": sib})

    def lt_copy(b):
        where = {"sp": b, "tp": home}
        return copy(lt_send.at[b], lt_in.at[c], l_send.at[0], l_recv.at[c], where)

    def lt_arrival(core):
        return copy(lt_send.at[0], lt_in.at[core], l_send.at[0], l_recv.at[core], {"tp": sib})

    def part_copy(b, e):
        src = part_out.at[b, e, 1 - c]
        return copy(src, part_in.at[b, e], p_send.at[0], p_recv.at[b, e], {"tp": sib})

    def cross_copy(b, e):
        src = cross_out.at[b, e]
        return copy(src, cross_in.at[b, e], x_send.at[0], x_recv.at[b, e], {"tp": far})

    def out_copy(b, e):
        to = s if e == 0 else edge
        return copy(block_out.at[b, e], block_in.at[to], o_send.at[0], o_recv.at[to], {"sp": b})

    def out_arrival(i):
        return copy(block_out.at[0, 0], block_in.at[i], o_send.at[0], o_recv.at[i], {"sp": near})

    def pool_copy(b):
        dst = pool_in.at[half]
        where = {"sp": b}
        return copy(block_out.at[b, 0], dst, o_send.at[0], o_recv.at[count + half], where)

    def pool_arrival(i):
        dst = pool_in.at[i]
        return copy(block_out.at[0, 0], dst, o_send.at[0], o_recv.at[count + i], {"sp": near})

    local[0].wait()
    local[1].wait()
    step = rows // 2

    def norm_rows(i, carry):
        at = pl.ds(pl.multiple_of(i * step, step), step)
        v = tok_own[at, :].astype(f32)
        scale = lax.rsqrt(jnp.mean(v * v, axis=-1, keepdims=True) + epsilon)
        to = pl.ds(pl.multiple_of(s * rows + i * step, step), step)
        norm_all[to, :] = (v * scale * gain_own[...]).astype(bf16)
        return carry

    with scope("norm"):
        lax.fori_loop(0, rows // step, norm_rows, 0)
    with scope("barrier"):
        pl.semaphore_wait(barrier, jnp.where(inner, 9, 6))
    sends_on = s != target

    @pl.when(inner)
    def _():
        z_copy(2 * s, other).start()
        z_copy(2 * s + 1, other).start()
        z_outward(2 * s).start()
        z_outward(2 * s + 1).start()

    @pl.when(jnp.logical_not(inner))
    def _():
        z_copy(2 * s, near).start()
        z_copy(2 * s + 1, near).start()

    local[2].wait()
    local[3].wait()
    local[11].wait()

    sends_near = jnp.logical_not(inner) & (c == half)

    sends_relay = jnp.logical_not(inner) & (c != half)

    @pl.when(sends_relay)
    def _():
        for i in range(3):
            relay_copy(i).start()

    @pl.when(away)
    def _():
        kv_first().start()
        for core in range(2):
            q_copy(core).start()

    seq = rows * count
    window = jnp.where(t == 0, 2, jnp.where(t == 1, 4, jnp.where(t == 2, 8, 16)))
    half_span = window // 2
    sub = rows // 4

    def pool(b, carry):
        at = b * rows + lax.broadcasted_iota(jnp.int32, (rows, seq), 0)
        col = lax.broadcasted_iota(jnp.int32, (rows, seq), 1)
        inside = (col >= at - half_span) & (col < at + window - half_span)
        band = jnp.where(inside, 1.0, 0.0).astype(bf16)
        total = jnp.dot(band, norm_all[:, span(t, group)], preferred_element_type=f32)
        pos = b * rows + lax.broadcasted_iota(jnp.int32, (rows, 1), 0)
        low = jnp.maximum(pos - half_span, 0)
        high = jnp.minimum(pos + window - half_span, seq)
        own = norm_all[span(b, rows), span(t, group)].astype(f32)
        pooled_all[span(b, rows), :] = (total / (high - low).astype(f32) - own).astype(bf16)
        return carry

    def hand_parts(b, e, total):
        for j in range(4):
            part_out[b, e, j % 2, j // 2] = total[j * sub : (j + 1) * sub, :].astype(bf16)
        part_copy(b, e).start()

    def pool_product(b):
        return jnp.dot(pooled_all[span(b, rows), :], wp_own[...], preferred_element_type=f32)

    def second_sum(b, e):
        part_copy(b, e).wait_recv()
        cross_out[b, e] = (
            part_out[b, e, c, 1 - x].astype(f32) + part_in[b, e, 1 - x].astype(f32)
        ).astype(bf16)
        cross_copy(b, e).start()

    def third_sum(b, e, send):
        cross_copy(b, e).wait_recv()
        block_out[b, e] = (
            part_out[b, e, c, x].astype(f32)
            + part_in[b, e, x].astype(f32)
            + cross_in[b, e].astype(f32)
        ).astype(bf16)

        @pl.when(b != s)
        def _():
            send().start()

    def outer_work():
        with scope("otok"):
            for u in (2 * near, 2 * near + 1, 2 * (count - 1 - near)):
                z_copy(u, near).wait_recv()

            @pl.when(sends_near)
            def _():
                kv_first_whole().start()
                for core in range(2):
                    q_whole(core).start()
                w_copy(0).start()
                w_copy(1).start()

            z_copy(2 * (count - 1 - near) + 1, near).wait_recv()
            z_copy(2 * far_edge, near).wait_recv()
            z_copy(2 * far_edge + 1, near).wait_recv()
        local[7].wait()

        def turn(m):
            return jnp.where(half == 0, count - 1 - m, m)

        def hand_on(m, carry):
            pool(turn(m), 0)
            hand_parts(turn(m), 0, pool_product(turn(m)))
            return carry

        with scope("opool"):
            lax.fori_loop(0, count, hand_on, 0)

        @pl.when(sends_relay)
        def _():
            w_copy(0).start()
            w_copy(1).start()

        def cross_over(m, carry):
            second_sum(turn(m), 0)
            return carry

        def hand_out(m, carry):
            third_sum(turn(m), 0, lambda: pool_copy(turn(m)))
            return carry

        with scope("osum"):
            lax.fori_loop(0, count, cross_over, 0)
            lax.fori_loop(0, count, hand_out, 0)

    pl.when(jnp.logical_not(inner))(outer_work)

    def inner_work():
        @pl.when(at_home)
        def _():
            kv_beside().start()
            q_beside().start()

        local[4].wait()
        local[5].wait()
        par_own[0:count, :] = hgain_own[...]
        for i in range(count):
            par_own[count + i : count + i + 1, :] = jnp.full((1, LANES), lam_own[i], f32)

        @pl.when(at_home)
        def _():
            par_copy().start()

        def tok_in(u, onward, beside=tok_forward):
            z_copy(u, other).wait_recv()
            if onward:
                z_copy(u, other).start()
            else:
                z_outward(u).start()
            tok_forward(1, u).start()
            beside(0, u).start()

        def tok_x(u, beside=tok_forward):
            tok_forward(1, u).wait_recv()
            beside(2, u).start()

        def kv_in(owner):
            @pl.when(at_home)
            def _():
                kv_arrival(owner, g).wait_recv()
                kv_forward(0, owner).start()
                kv_forward(1, owner).start()

        def r_arrive(i):
            relay_copy(i).wait_recv()
            relay_forward(i).start()

        def kv_y(owner):
            @pl.when(at_home)
            def _():
                kv_arrival(owner, twin).wait_recv()
                kv_forward(2, owner).start()

        def q_in(owner):
            q_arrival(owner, g).wait_recv()
            q_forward(owner).start()

        owners = (edge, other, far_edge)
        split = (other, far_edge)
        with scope("tok0"):
            tok_in(2 * edge, True)
            tok_in(2 * other, False)
        with scope("tok1"):
            tok_in(2 * edge + 1, True)
            tok_in(2 * other + 1, False)
        with scope("relay0"):

            @pl.when(away)
            def _():
                r_arrive(0)

        with scope("kv1"):
            kv_in(other)
        with scope("x0"):
            tok_x(2 * edge)
            tok_x(2 * other)
        with scope("q1"):
            q_in(other)
        with scope("relay1"):

            @pl.when(away)
            def _():
                r_arrive(1)

        with scope("tok2"):
            tok_in(2 * far_edge, False, tok_late)
        with scope("kvy1"):
            kv_y(other)
        with scope("x1"):
            tok_x(2 * edge + 1)
            tok_x(2 * other + 1)
        with scope("tok3"):
            tok_in(2 * far_edge + 1, False, tok_late)
        with scope("relay2"):

            @pl.when(away)
            def _():
                r_arrive(2)

        with scope("kv0"):

            @pl.when(at_home)
            def _():
                kv_edge().wait_recv()
                kv_edge().start()

        with scope("kv2"):
            kv_in(far_edge)
        with scope("pool"):
            lax.fori_loop(0, count, pool, 0)
        with scope("q2"):

            @pl.when(c == 0)
            def _():
                q_in(far_edge)

        with scope("x2"):
            tok_x(2 * far_edge, tok_late)
            tok_x(2 * far_edge + 1, tok_late)

        early = pl.ds(pl.multiple_of(half * rows, rows), 3 * rows)
        late = span(far_edge, rows)
        k_early = pl.ds(pl.multiple_of(half * shard, shard), 3 * shard)
        k_late = span(far_edge, shard)

        def early_product(store, w):
            store[...] = jnp.dot(
                norm_all[early, k_early], w[k_early, :], preferred_element_type=f32
            )

        def late_product(store, w, put):
            acc = store[...] + jnp.dot(
                norm_all[early, k_late], w[k_late, :], preferred_element_type=f32
            )
            put(early, acc.astype(bf16))
            acc = jnp.dot(norm_all[late, :], w[...], preferred_element_type=f32)
            put(late, acc.astype(bf16))

        def early_tokens(step):
            place = norm_all.at[0 : 2 * rows, 0:quarter]
            got = f_recv.at[2 * count + step // 2]
            return copy(place, place, f_send.at[step], got, {"tp": sib})

        with scope("earlykv"):
            for step in (0, 2):
                early_tokens(step).wait_recv()

            @pl.when(at_home)
            def _():
                local[8].wait()
                local[9].wait()
                local[10].wait()

            @pl.when(away)
            def _():
                kv_edge().wait_recv()
                kv_arrival(other, g).wait_recv()
                kv_arrival(other, twin).wait_recv()
                kv_beside().wait_recv()
                q_beside().wait_recv()
                par_copy().wait_recv()

            early_product(acc_kv, w_kv)
        with scope("kvy2"):
            kv_y(far_edge)
        with scope("earlyq"):
            q_edge().wait_recv()
            q_arrival(other, twin).wait_recv()
            early_product(acc_q, w_q)
        with scope("rest"):
            for step in (0, 2):
                for u in (2 * far_edge, 2 * far_edge + 1):
                    tok_late(step, u).wait_recv()
        with scope("kvrest"):

            @pl.when(away)
            def _():
                kv_arrival(far_edge, g).wait_recv()
                kv_arrival(far_edge, twin).wait_recv()

        def put_kv(at, value):
            k_all[at, :] = value[:, 0:LANES]
            v_all[at, :] = value[:, LANES:pair]

        def put_q(at, value):
            q_all[at, :] = value

        with scope("projkv"):
            late_product(acc_kv, w_kv, put_kv)
        with scope("qrest"):

            @pl.when(c == 0)
            def _():
                q_arrival(far_edge, twin).wait_recv()

            @pl.when(c == 1)
            def _():
                q_far_whole().wait_recv()

        with scope("projq"):
            late_product(acc_q, w_q, put_q)

        par_use[...] = jnp.where(at_home, par_own[...], par_in[...])
        lane = lax.broadcasted_iota(jnp.int32, (rows, LANES), 1)
        lt_rows = lt_send.shape[2]
        base = HD ** (-0.5)

        def two_heads(b):
            zero = jnp.zeros((rows, LANES), bf16)
            parts = []
            for h in range(2):
                q = q_all[span(b, rows), h * LANES : (h + 1) * LANES]
                parts += [jnp.where(lane < HD, q, zero), jnp.where(lane < HD, zero, q)]
            raw = lax.dot_general(
                jnp.concatenate(parts, axis=0),
                k_all[...],
                (((1,), (1,)), ((), ())),
                preferred_element_type=f32,
            )
            highest = jnp.max(raw, axis=-1, keepdims=True)
            weights = jnp.exp2((raw - highest) * (base * math.log2(math.e)))
            totals = jnp.sum(weights, axis=-1, keepdims=True)
            reads = jnp.dot(weights.astype(bf16), v_all[...], preferred_element_type=f32) / totals
            logs = highest * base + jnp.log(totals)
            done = []
            for h in range(2):
                head = 2 * c + h
                first = slice(2 * h * rows, (2 * h + 1) * rows)
                second = slice((2 * h + 1) * rows, (2 * h + 2) * rows)
                contrast = reads[first] - par_use[pl.ds(count + head, 1), :] * reads[second]
                scaled = (
                    contrast
                    * lax.rsqrt(jnp.mean(contrast * contrast, axis=-1, keepdims=True) + epsilon)
                    * par_use[pl.ds(head, 1), :]
                ).astype(bf16)
                done.append((scaled, logs[first], logs[second]))
            return done

        def attend(b):
            done = two_heads(b)
            for h in range(2):
                head_own[span(b, rows), h * LANES : (h + 1) * LANES] = done[h][0]
            head_copy(0, b).start()

            @pl.when(away)
            def _():
                head_copy(1, b).start()

            @pl.when(at_home)
            def _():
                heads_all[c, span(b, rows), :] = head_own[span(b, rows), :]

            both = jnp.where(
                lane < 2,
                jnp.where(lane == 0, done[0][1], done[0][2]),
                jnp.where(lane == 2, done[1][1], done[1][2]),
            )
            padded = jnp.concatenate([both, jnp.zeros((lt_rows - rows, LANES), f32)], axis=0)
            lt_send[b] = jnp.transpose(padded)[0:8, :]

        def send_logs(b, carry):
            @pl.when(jnp.logical_not(at_home & (b == s)))
            def _():
                lt_copy(b).start()

            return carry

        def first_sum(b, e):
            if e == 0:
                for core in range(2):

                    @pl.when(jnp.logical_not(at_home & (c == core)))
                    def _():
                        head_arrival(b, core).wait_recv()

            total = sum(
                jnp.dot(
                    heads_all[core, span(b, rows), :],
                    wa_all[e, core * pair : (core + 1) * pair, :],
                    preferred_element_type=f32,
                )
                for core in range(2)
            )
            hand_parts(b, e, total + pool_product(b) if e == 0 else total)

        def nth(m):
            return jnp.where(m < 2, (count - 1) * m, m - 1)

        def attend_all(m, carry):
            with scope("att"):
                attend(nth(m))

            @pl.when(m == jnp.where(at_home, 0, 1))
            def _():
                with scope("wao"):
                    w_arrival(0).wait_recv()
                    w_forward().start()

            return carry

        lax.fori_loop(0, count, attend_all, 0)
        local[6].wait()
        local[7].wait()

        with scope("S1"):
            first_sum(0, 0)
        lax.fori_loop(0, count, send_logs, 0)
        with scope("S2"):
            second_sum(0, 0)
        with scope("wrest"):
            w_arrival(1).wait_recv()
            w_arrival(2).wait_recv()
        first_sum(0, 1)
        second_sum(0, 1)

        def steps(m, carry):
            @pl.when(m < count)
            def _():
                with scope("S1"):
                    for e in range(2):
                        first_sum(nth(m), e)
                with scope("S2"):
                    for e in range(2):
                        second_sum(nth(m), e)

            @pl.when(m >= 2)
            def _():
                with scope("S3"):
                    for e in range(2):
                        third_sum(nth(m - 2), e, lambda: out_copy(nth(m - 2), e))

            return carry

        lax.fori_loop(1, count + 2, steps, 0)

    pl.when(inner)(inner_work)

    def put_logs(core, ref, at):
        for h in range(2):
            for m in range(2):
                i = 2 * core + h
                lt_out[m, i : i + 1, :] = ref[at, 2 * h + m : 2 * h + m + 1, 0:rows]

    for core in range(2):

        @pl.when(at_home & (c == core))
        def _():
            put_logs(core, lt_send, s)

        @pl.when(jnp.logical_not(at_home & (c == core)))
        def _():
            lt_arrival(core).wait_recv()
            put_logs(core, lt_in, core)

    for i in range(count):
        with scope(f"final{i}"):
            at = slice(i * cols, (i + 1) * cols)
            maker = min(max(i, 1), count - 2)
            e = 0 if i == maker else 1

            @pl.when(s == maker)
            def _():
                mixed_out[:, at] = block_out[s, e]

            @pl.when(s != maker)
            def _():
                out_arrival(i).wait_recv()
                mixed_out[:, at] = block_in[i]

            if e == 1:
                which = i // (count - 1)

                @pl.when(s == i)
                def _():
                    both = mixed_out[:, at].astype(f32) + block_out[s, 0].astype(f32)
                    mixed_out[:, at] = both.astype(bf16)

                @pl.when(s != i)
                def _():
                    pool_arrival(which).wait_recv()
                    both = mixed_out[:, at].astype(f32) + pool_in[which].astype(f32)
                    mixed_out[:, at] = both.astype(bf16)

    @pl.when(sends_near)
    def _():
        kv_first_whole().wait_send()
        all_sent(w_q.at[0 : 2 * shard, :], q_send.at[0])

    @pl.when(sends_relay)
    def _():
        relay_copy(0).wait_send()
        all_sent(w_q.at[0 : shard + part, :], q_send.at[0])

    @pl.when(away)
    def _():
        kv_first().wait_send()
        all_sent(w_q.at[0:shard, :], q_send.at[0])
        relay_forward(0).wait_send()
        all_sent(w_q.at[0 : shard + part, :], q_send.at[2])

    @pl.when(jnp.logical_not(inner))
    def _():
        all_sent(norm_all.at[0:rows, 0:quarter], z_send.at[0])
        w_copy(0).wait_send()
        w_copy(1).wait_send()
        all_sent(part_in.at[:, 0], p_send.at[0])
        all_sent(cross_in.at[:, 0], x_send.at[0])
        all_sent(block_out.at[0 : count - 1, 0], o_send.at[0])

    @pl.when(at_home)
    def _():
        kv_beside().wait_send()
        q_beside().wait_send()
        par_copy().wait_send()
        all_sent(w_kv, kv_fwd.at[0])

    @pl.when(away)
    def _():
        all_sent(head_own, h_send.at[1])

    @pl.when(inner)
    def _():
        all_sent(norm_all.at[0 : 2 * rows, 0:quarter], z_send.at[0])
        for sem in (z_send.at[1], f_send.at[0], f_send.at[1], f_send.at[2]):
            all_sent(norm_all.at[0 : 3 * rows, 0:quarter], sem)

        @pl.when(c == 0)
        def _():
            all_sent(w_q.at[0:shard, :], q_twin.at[0])

        @pl.when(c == 1)
        def _():
            all_sent(w_q.at[0:part, :], q_twin.at[0])

        w_forward().wait_send()
        all_sent(head_own, h_send.at[0])
        all_sent(part_in, p_send.at[0])
        all_sent(cross_in, x_send.at[0])
        all_sent(block_out.at[0 : count - 1], o_send.at[0])

    @pl.when(inner & jnp.logical_not(at_home))
    def _():
        all_sent(lt_send, l_send.at[0])

    @pl.when(at_home)
    def _():
        all_sent(lt_send.at[0 : count - 1], l_send.at[0])


def fused(
    count,
    tokens,
    norm_gain,
    query_weight,
    key_weight,
    value_weight,
    map_lambda,
    head_gain,
    attn_out_weight,
    pool_out_weight,
):
    rows, width = tokens.shape
    group, cols = pool_out_weight.shape
    shard = query_weight.shape[0]
    sub = rows // 4
    seq = rows * count
    pair = 2 * LANES
    lt_rows = -(-rows // LANES) * LANES
    bf16, f32 = jnp.bfloat16, jnp.float32
    vmem = pl.BlockSpec(memory_space=pltpu.VMEM)
    far = pl.BlockSpec(memory_space=pl.ANY)
    sems = pltpu.SemaphoreType.DMA
    return pl.pallas_call(
        functools.partial(fused_kernel, count),
        out_shape=(
            pltpu.VMEM((sub, width), bf16),
            pltpu.VMEM((2, count, rows), f32),
        ),
        in_specs=[far] * 9,
        out_specs=(vmem, vmem),
        scratch_shapes=[
            pltpu.VMEM((rows, width), bf16),
            pltpu.VMEM((1, width), f32),
            pltpu.SMEM((count,), f32),
            pltpu.VMEM((count, LANES), f32),
            pltpu.VMEM((seq, width), bf16),
            pltpu.VMEM((shard, pair), bf16),
            pltpu.VMEM((shard, count * LANES), bf16),
            pltpu.VMEM((shard // 2, pair), bf16),
            pltpu.VMEM((shard // 2, pair), bf16),
            pltpu.VMEM((shard, pair), bf16),
            pltpu.VMEM((width, pair), bf16),
            pltpu.VMEM((width, pair), bf16),
            pltpu.VMEM((2, group, cols), bf16),
            pltpu.VMEM((group, cols), bf16),
            pltpu.VMEM((2 * count, LANES), f32),
            pltpu.VMEM((2 * count, LANES), f32),
            pltpu.VMEM((2 * count, LANES), f32),
            pltpu.VMEM((3 * rows, pair), f32),
            pltpu.VMEM((3 * rows, pair), f32),
            pltpu.VMEM((seq, pair), bf16),
            pltpu.VMEM((seq, LANES), bf16),
            pltpu.VMEM((seq, LANES), bf16),
            pltpu.VMEM((seq, pair), bf16),
            pltpu.VMEM((2, seq, pair), bf16),
            pltpu.VMEM((seq, group), bf16),
            pltpu.VMEM((count, 2, 2, 2, sub, cols), bf16),
            pltpu.VMEM((count, 2, 2, sub, cols), bf16),
            pltpu.VMEM((count, 2, sub, cols), bf16),
            pltpu.VMEM((count, 2, sub, cols), bf16),
            pltpu.VMEM((count, 2, sub, cols), bf16),
            pltpu.VMEM((count, sub, cols), bf16),
            pltpu.VMEM((2, sub, cols), bf16),
            pltpu.VMEM((count, 8, lt_rows), f32),
            pltpu.VMEM((2, 8, lt_rows), f32),
            sems((12,)),
            sems((2,)),
            sems((2 * count,)),
            sems((3,)),
            sems((2 * count + 6,)),
            sems((3,)),
            sems((1,)),
            sems((count, 2)),
            sems((3,)),
            sems((1,)),
            sems((count, 2)),
            sems((3,)),
            sems((2,)),
            sems((1,)),
            sems((3,)),
            sems((2,)),
            sems((2,)),
            sems((count, 2)),
            sems((1,)),
            sems((count, 2)),
            sems((1,)),
            sems((count, 2)),
            sems((1,)),
            sems((count + 2,)),
            sems((1,)),
            sems((2,)),
        ],
        compiler_params=pltpu.CompilerParams(collective_id=0, has_side_effects=True),
    )(
        tokens,
        norm_gain.reshape(1, width),
        query_weight,
        key_weight,
        value_weight,
        map_lambda,
        head_gain,
        attn_out_weight,
        pool_out_weight,
    )


def fits(shape, tokens, query_weight, value_weight, map_lambda, pool_out_weight):
    count = shape["sp"]
    return (
        shape["grp"] == 2
        and shape["tp"] == 4
        and count == 4
        and map_lambda.shape[0] == count
        and value_weight.shape[1] == VD == LANES == 2 * HD
        and tokens.shape[0] % 32 == 0
        and tokens.shape[1] % (4 * LANES) == 0
        and query_weight.shape[0] % 32 == 0
        and query_weight.shape[1] == count * LANES
        and pool_out_weight.shape[0] * 4 == tokens.shape[1]
        and pool_out_weight.shape[1] % LANES == 0
        and pool_out_weight.shape[1] * count == tokens.shape[1]
        and pool_out_weight.shape[0] == pool_out_weight.shape[1]
        and pool_out_weight.shape[0] == query_weight.shape[0]
        and tokens.shape[0] * count * tokens.shape[1] <= 1 << 22
    )


def solution(mesh):
    placed = (
        P(("grp", "sp"), None),
        P(),
        P("sp", "tp"),
        P("sp", "tp"),
        P("sp", "tp"),
        P("tp"),
        P("tp", None),
        P("tp", "sp"),
        P("tp", "sp"),
    )
    shape = dict(mesh.shape)

    def chosen(*args):
        if fits(shape, args[0], args[2], args[4], args[5], args[8]):
            return fused(shape["sp"], *args)
        return on_device(*args)

    return jax.shard_map(
        chosen,
        mesh=mesh,
        in_specs=placed,
        out_specs=(P(("grp", "sp", "tp"), None), P(None, "tp", ("grp", "sp"))),
        check_vma=False,
    )
```

```python
import functools
import math

import jax
import jax.numpy as jnp
from jax import lax
from jax.experimental import pallas as pl
from jax.experimental.pallas import tpu as pltpu
from jax.sharding import PartitionSpec as P

HD = 64
VD = 128
POOL_SPAN = 16


epsilon = 1e-06
very_low = -1e30


def extended(cells, sides, width):
    for axis, dim in sides:
        count = lax.axis_size(axis)
        ends = count - 1
        head = lax.slice_in_dim(cells, 0, width, axis=dim)
        tail = lax.slice_in_dim(cells, cells.shape[dim] - width, cells.shape[dim], axis=dim)
        cells = jnp.concatenate(
            [
                lax.ppermute(tail, axis, [(i, (i + 1) % count) for i in range(ends)]),
                cells,
                lax.ppermute(head, axis, [((i + 1) % count, i) for i in range(ends)]),
            ],
            axis=dim,
        )
    return cells


def add_products(totals, pieces, source):
    results = []
    for running, piece in zip(totals, pieces):
        results.append(jnp.dot(source, piece, preferred_element_type=jnp.float32))
    return tuple(results)


def on_device(
    tokens,
    norm_gain,
    query_weight,
    key_weight,
    value_weight,
    map_lambda,
    head_gain,
    attn_out_weight,
    pool_out_weight,
):
    tokens_wide = tokens.astype(jnp.float32)
    normed = (
        tokens_wide
        * lax.rsqrt(jnp.mean(tokens_wide * tokens_wide, axis=-1, keepdims=True) + epsilon)
        * norm_gain
    ).astype(jnp.bfloat16)
    row_count = normed.shape[0]
    sp_index = lax.axis_index("sp")
    tp_index = lax.axis_index("tp")
    group_width = pool_out_weight.shape[0]
    local_heads = map_lambda.shape[0]
    key_heads = value_weight.shape[1] // VD
    group_heads = local_heads // key_heads
    q_empty = jnp.zeros((row_count, query_weight.shape[1]), jnp.float32)
    k_empty = jnp.zeros((row_count, key_weight.shape[1]), jnp.float32)
    v_empty = jnp.zeros((row_count, value_weight.shape[1]), jnp.float32)
    q_acc, k_acc, v_acc = add_products(
        (q_empty, k_empty, v_empty),
        (
            lax.all_gather(query_weight, "sp", axis=0, tiled=True),
            lax.all_gather(key_weight, "sp", axis=0, tiled=True),
            lax.all_gather(value_weight, "sp", axis=0, tiled=True),
        ),
        normed,
    )
    queries = q_acc.astype(jnp.bfloat16).reshape(row_count, key_heads, group_heads, 2, HD)
    keys_flat = k_acc.astype(jnp.bfloat16)
    values_flat = v_acc.astype(jnp.bfloat16)

    def key_block(state_now, key_pair):
        maxima, totals, accums = state_now
        key_blk, val_blk = key_pair
        scores = jnp.einsum(
            "qhgmd,khmd->hgmqk", queries, key_blk, preferred_element_type=jnp.float32
        ) * HD ** (-0.5)
        highest = jnp.maximum(maxima, jnp.max(scores, axis=-1))
        factor = jnp.exp(maxima - highest)
        weights = jnp.exp(scores - highest[..., None])
        totals = totals * factor + jnp.sum(weights, axis=-1)
        accums = accums * factor[..., None] + jnp.einsum(
            "hgmqk,khe->hgmqe",
            weights.astype(jnp.bfloat16),
            val_blk,
            preferred_element_type=jnp.float32,
        )
        return ((highest, totals, accums), None)

    start_state = (
        jnp.full((key_heads, group_heads, 2, row_count), very_low, jnp.float32),
        jnp.zeros((key_heads, group_heads, 2, row_count), jnp.float32),
        jnp.zeros((key_heads, group_heads, 2, row_count, VD), jnp.float32),
    )
    key_piece = lax.all_gather(keys_flat, "sp", axis=0, tiled=True)
    val_piece = lax.all_gather(values_flat, "sp", axis=0, tiled=True)
    piece_len = key_piece.shape[0]
    block_len = math.gcd(piece_len, 512)
    key_blocks = key_piece.reshape(piece_len // block_len, block_len, key_heads, 2, HD)
    val_blocks = val_piece.reshape(piece_len // block_len, block_len, key_heads, VD)
    state_next, unused = lax.scan(key_block, start_state, (key_blocks, val_blocks))
    maxima, totals, accums = state_next
    log_parts = maxima + jnp.log(totals)
    log_totals = jnp.transpose(log_parts, (2, 0, 1, 3)).reshape(2, local_heads, row_count)
    reads = accums / totals[..., None]
    contrast = reads[:, :, 0] - map_lambda.reshape(key_heads, group_heads, 1, 1) * reads[:, :, 1]
    scaled = (
        contrast
        * lax.rsqrt(jnp.mean(contrast * contrast, axis=-1, keepdims=True) + epsilon)
        * head_gain.reshape(key_heads, group_heads, 1, VD)
    )
    attention_head_rows = (
        jnp.transpose(scaled, (2, 0, 1, 3))
        .reshape(row_count, local_heads * VD)
        .astype(jnp.bfloat16)
    )
    head_rows, log_totals = (attention_head_rows, log_totals)
    own_chan = lax.dynamic_slice_in_dim(normed, tp_index * group_width, group_width, 1)
    reach = POOL_SPAN // 2
    padded = extended(own_chan, (("sp", 0),), reach)
    window = jnp.left_shift(jnp.int32(2), tp_index)
    half_span = window // 2
    running = jnp.zeros((row_count, group_width), jnp.float32)
    for offset in range(POOL_SPAN):
        piece = lax.dynamic_slice_in_dim(padded, reach - half_span + offset, row_count, 0).astype(
            jnp.float32
        )
        running = running + jnp.where(offset < window, piece, 0.0)
    seq_len = row_count * lax.axis_size("sp")
    position = sp_index * row_count + jnp.arange(row_count, dtype=jnp.int32)
    lower_edge = jnp.clip(position - half_span, 0, seq_len)
    upper_edge = jnp.clip(position + window - half_span, 0, seq_len)
    counts_f = (upper_edge - lower_edge).astype(jnp.float32)[:, None]
    pooled = (running / counts_f - own_chan.astype(jnp.float32)).astype(jnp.bfloat16)
    attn_whole, pool_whole = (
        lax.all_gather(attn_out_weight, "sp", axis=1, tiled=True),
        lax.all_gather(pool_out_weight, "sp", axis=1, tiled=True),
    )
    mixed = lax.psum_scatter(
        (
            jnp.dot(head_rows, attn_whole, preferred_element_type=jnp.float32)
            + jnp.dot(pooled, pool_whole, preferred_element_type=jnp.float32)
        ).astype(jnp.bfloat16),
        "tp",
        scatter_dimension=0,
        tiled=True,
    )
    return (mixed, log_totals)


MESH = pl.DeviceIdType.MESH
LANES = 128
scope = jax.named_scope


def fused_kernel(
    count,
    tok,
    gain,
    wq,
    wk,
    wv,
    lam,
    hgain,
    wao,
    wpo,
    mixed_out,
    lt_out,
    tok_own,
    gain_own,
    lam_own,
    hgain_own,
    norm_all,
    kv_own,
    q_own,
    kv_relay,
    q_relay,
    q_relay_whole,
    w_kv,
    w_q,
    wa_all,
    wp_own,
    par_own,
    par_in,
    par_use,
    acc_kv,
    acc_q,
    q_all,
    k_all,
    v_all,
    head_own,
    heads_all,
    pooled_all,
    part_out,
    part_in,
    cross_out,
    cross_in,
    block_out,
    block_in,
    pool_in,
    lt_send,
    lt_in,
    local_sem,
    z_send,
    z_recv,
    f_recv,
    kv_send,
    kv_recv,
    q_recv,
    r_recv,
    w_recv,
    par_sem,
    h_recv,
    p_send,
    p_recv,
    x_send,
    x_recv,
    o_send,
    o_recv,
    l_send,
    l_recv,
):
    g = lax.axis_index("grp")
    s = lax.axis_index("sp")
    t = lax.axis_index("tp")
    c = lax.rem(t, 2)
    x = t // 2
    rows, width = tok.shape
    quarter = width // 4
    shard = wq.shape[0]
    part = shard // 2
    pair = 2 * LANES
    group = wpo.shape[0]
    cols = wpo.shape[1]
    half = s // 2
    inner = (s > 0) & (s < count - 1)
    at_home = inner & (c == half)
    away = inner & (c != half)
    sib = t + 1 - 2 * c
    far = lax.rem(t + 2, 4)
    twin = 1 - g
    near = 1 + half
    other = count - 1 - s
    edge = jnp.where(half == 0, 0, count - 1)
    far_edge = count - 1 - edge
    target = 1 + c
    home = 2 * x + half
    f32, bf16 = jnp.float32, jnp.bfloat16

    def span(index, size):
        return pl.ds(pl.multiple_of(index * size, size), size)

    def half_rows(owner, which):
        return pl.ds(pl.multiple_of(owner * shard + which * part, part), part)

    barrier = pltpu.get_barrier_semaphore()

    def greet(where):
        pl.semaphore_signal(barrier, inc=1, device_id=where, device_id_type=MESH)

    def greet_beside(up):
        peer = lax.rem(s + (1 if up else count - 1), count)
        greet({"sp": peer})
        greet({"sp": peer, "tp": sib})

    @pl.when(s < count - 1)
    def _():
        greet_beside(True)

    @pl.when(s > 0)
    def _():
        greet_beside(False)

    greet({"tp": sib})
    greet({"tp": far})

    @pl.when(inner)
    def _():
        greet({"grp": twin})

    pieces = (
        (tok, tok_own),
        (gain, gain_own),
        (wk, kv_own.at[:, 0:LANES]),
        (wv, kv_own.at[:, LANES:pair]),
        (lam, lam_own),
        (hgain, hgain_own),
        (wao, wa_all.at[0]),
        (wpo, wp_own),
        (wk, w_kv.at[span(s, shard), 0:LANES]),
        (wv, w_kv.at[span(s, shard), LANES:pair]),
        (wq.at[:, span(c, pair)], w_q.at[span(s, shard), :]),
        (wq, q_own),
    )
    local = [
        pltpu.make_async_copy(src, dst, local_sem.at[i]) for i, (src, dst) in enumerate(pieces)
    ]
    for piece in local[:4]:
        piece.start()
    local[11].start()

    local[7].start()

    @pl.when(inner)
    def _():
        for piece in local[4:7]:
            piece.start()

    @pl.when(at_home)
    def _():
        for piece in local[8:11]:
            piece.start()

    def copy(src, dst, send, recv, where):
        return pltpu.make_async_remote_copy(
            src_ref=src,
            dst_ref=dst,
            send_sem=send,
            recv_sem=recv,
            device_id=where,
            device_id_type=MESH,
        )

    chunk = rows // 2

    def z_copy(u, dest):
        place = norm_all.at[span(u, chunk), span(t, quarter)]
        return copy(place, place, z_send.at[0], z_recv.at[u], {"sp": dest})

    def z_outward(u):
        place = norm_all.at[span(u, chunk), span(t, quarter)]
        return copy(place, place, z_send.at[0], z_recv.at[u], {"sp": edge})

    def tok_forward(step, u):
        col = span(far if step == 2 else t, quarter)
        place = norm_all.at[span(u, chunk), col]
        where = {"tp": far if step == 1 else sib}
        got = f_recv.at[u] if step == 1 else f_recv.at[2 * count + step // 2]
        return copy(place, place, z_send.at[0], got, where)

    def tok_late(step, u):
        col = span(far if step == 2 else t, quarter)
        place = norm_all.at[span(u, chunk), col]
        got = f_recv.at[2 * count + 2 + step + lax.rem(u, 2)]
        return copy(place, place, z_send.at[0], got, {"tp": sib})

    def all_sent(ref, sem):
        copy(ref, ref, sem, sem, {"tp": sib}).wait_send()

    def kv_first():
        src = kv_own.at[span(g, part), :]
        dst = w_kv.at[half_rows(s, g), :]
        return copy(src, dst, kv_send.at[0], kv_recv.at[s, g], {"sp": target})

    def kv_first_whole():
        dst = w_kv.at[span(s, shard), :]
        return copy(kv_own, dst, kv_send.at[0], kv_recv.at[s, 0], {"sp": near})

    def kv_beside():
        dst = w_kv.at[span(s, shard), :]
        return copy(kv_own, dst, kv_send.at[0], kv_recv.at[s, 0], {"tp": sib})

    def kv_edge():
        place = w_kv.at[span(edge, shard), :]
        return copy(place, place, kv_send.at[0], kv_recv.at[edge, 0], {"tp": sib})

    def kv_forward(kind, owner):
        which = twin if kind == 2 else g
        place = w_kv.at[half_rows(owner, which), :]
        where = {"grp": twin} if kind == 0 else {"tp": sib}
        return copy(place, place, kv_send.at[0], kv_recv.at[owner, which], where)

    def kv_arrival(owner, which):
        place = w_kv.at[half_rows(owner, which), :]
        return copy(place, place, kv_send.at[0], kv_recv.at[owner, which], {"tp": sib})

    def q_copy(core):
        src = q_own.at[span(g, part), core * pair : (core + 1) * pair]
        dst = w_q.at[half_rows(s, g), :]
        where = {"sp": target, "tp": 2 * x + core}
        return copy(src, dst, kv_send.at[0], q_recv.at[s, g], where)

    def q_whole(core):
        src = q_own.at[:, core * pair : (core + 1) * pair]
        dst = w_q.at[span(s, shard), :]
        where = {"sp": near, "tp": 2 * x + core}
        return copy(src, dst, kv_send.at[0], q_recv.at[s, 0], where)

    def q_edge():
        place = w_q.at[span(edge, shard), :]
        return copy(place, place, kv_send.at[0], q_recv.at[edge, 0], {"tp": sib})

    def relay_copy(i):
        if i == 0:
            src, dst = kv_own.at[span(g, part), :], kv_relay
        elif i == 1:
            src, dst = q_own.at[span(g, part), 0:pair], q_relay
        else:
            src, dst = q_own.at[:, pair : 2 * pair], q_relay_whole
        send = kv_send.at[0]
        return copy(src, dst, send, r_recv.at[i], {"sp": near})

    def relay_forward(i):
        if i == 0:
            dst = w_kv.at[half_rows(edge, g), :]
            return copy(kv_relay, dst, kv_send.at[0], kv_recv.at[edge, g], {"sp": other})
        where = {"sp": other, "tp": 2 * x + i - 1}
        if i == 1:
            dst = w_q.at[half_rows(edge, g), :]
            return copy(q_relay, dst, kv_send.at[0], q_recv.at[edge, g], where)
        dst = w_q.at[span(edge, shard), :]
        return copy(q_relay_whole, dst, kv_send.at[0], q_recv.at[edge, 0], where)

    def q_far_whole():
        place = w_q.at[span(far_edge, shard), :]
        return copy(place, place, kv_send.at[0], q_recv.at[far_edge, 0], {"tp": sib})

    def q_beside():
        src = q_own.at[:, span(1 - c, pair)]
        return copy(src, w_q.at[span(s, shard), :], kv_send.at[0], q_recv.at[s, 0], {"tp": sib})

    def q_forward(owner):
        place = w_q.at[half_rows(owner, g), :]
        return copy(place, place, kv_send.at[0], q_recv.at[owner, g], {"grp": twin})

    def q_arrival(owner, which):
        place = w_q.at[half_rows(owner, which), :]
        return copy(place, place, kv_send.at[0], q_recv.at[owner, which], {"grp": twin})

    w_rows = (span(g, part // 2), pl.ds(part, part), span(twin, part // 2))

    def w_copy(kind):
        src, dst = wao.at[w_rows[kind], :], wa_all.at[1, w_rows[kind], :]
        return copy(src, dst, kv_send.at[0], w_recv.at[kind], {"sp": near})

    def w_forward():
        place = wa_all.at[1, w_rows[0], :]
        return copy(place, place, kv_send.at[0], w_recv.at[2], {"grp": twin})

    def w_arrival(kind):
        place = wa_all.at[1, w_rows[kind], :]
        return copy(place, place, kv_send.at[0], w_recv.at[kind], {"grp": twin})

    def par_copy():
        return copy(par_own, par_in, par_sem.at[0], par_sem.at[1], {"tp": sib})

    head_where = ({"sp": other, "tp": home}, {"tp": sib})

    def head_copy(kind, b):
        dst = heads_all.at[c, span(b, rows), :]
        src = head_own.at[span(b, rows), :]
        return copy(src, dst, kv_send.at[0], h_recv.at[b, c], head_where[kind])

    def head_arrival(b, core):
        place = heads_all.at[core, span(b, rows), :]
        return copy(place, place, kv_send.at[0], h_recv.at[b, core], {"tp": sib})

    def lt_copy(b):
        where = {"sp": b, "tp": home}
        return copy(lt_send.at[b], lt_in.at[c], l_send.at[0], l_recv.at[c], where)

    def lt_arrival(core):
        return copy(lt_send.at[0], lt_in.at[core], l_send.at[0], l_recv.at[core], {"tp": sib})

    def part_copy(b, e):
        src = part_out.at[b, e, 1 - c]
        return copy(src, part_in.at[b, e], p_send.at[0], p_recv.at[b, e], {"tp": sib})

    def cross_copy(b, e):
        src = cross_out.at[b, e]
        return copy(src, cross_in.at[b, e], x_send.at[0], x_recv.at[b, e], {"tp": far})

    def out_copy(b, e):
        to = s if e == 0 else edge
        return copy(block_out.at[b, e], block_in.at[to], o_send.at[0], o_recv.at[to], {"sp": b})

    def out_arrival(i):
        return copy(block_out.at[0, 0], block_in.at[i], o_send.at[0], o_recv.at[i], {"sp": near})

    def pool_copy(b):
        dst = pool_in.at[half]
        where = {"sp": b}
        return copy(block_out.at[b, 0], dst, o_send.at[0], o_recv.at[count + half], where)

    def pool_arrival(i):
        dst = pool_in.at[i]
        return copy(block_out.at[0, 0], dst, o_send.at[0], o_recv.at[count + i], {"sp": near})

    local[0].wait()
    local[1].wait()
    step = rows // 2

    def norm_rows(i, carry):
        at = pl.ds(pl.multiple_of(i * step, step), step)
        v = tok_own[at, :].astype(f32)
        scale = lax.rsqrt(jnp.mean(v * v, axis=-1, keepdims=True) + epsilon)
        to = pl.ds(pl.multiple_of(s * rows + i * step, step), step)
        norm_all[to, :] = (v * scale * gain_own[...]).astype(bf16)
        return carry

    with scope("norm"):
        lax.fori_loop(0, rows // step, norm_rows, 0)
    with scope("barrier"):
        pl.semaphore_wait(barrier, jnp.where(inner, 7, 4))
    sends_on = s != target

    @pl.when(inner)
    def _():
        z_copy(2 * s, other).start()
        z_copy(2 * s + 1, other).start()
        z_outward(2 * s).start()
        z_outward(2 * s + 1).start()

    @pl.when(jnp.logical_not(inner))
    def _():
        z_copy(2 * s, near).start()
        z_copy(2 * s + 1, near).start()

    local[2].wait()
    local[3].wait()
    local[11].wait()

    sends_near = jnp.logical_not(inner) & (c == half)

    sends_relay = jnp.logical_not(inner) & (c != half)

    @pl.when(sends_relay)
    def _():
        for i in range(3):
            relay_copy(i).start()

    @pl.when(away)
    def _():
        kv_first().start()
        for core in range(2):
            q_copy(core).start()

    seq = rows * count
    window = jnp.where(t == 0, 2, jnp.where(t == 1, 4, jnp.where(t == 2, 8, 16)))
    half_span = window // 2
    sub = rows // 4

    def pool(b, carry):
        at = b * rows + lax.broadcasted_iota(jnp.int32, (rows, seq), 0)
        col = lax.broadcasted_iota(jnp.int32, (rows, seq), 1)
        inside = (col >= at - half_span) & (col < at + window - half_span)
        band = jnp.where(inside, 1.0, 0.0).astype(bf16)
        total = jnp.dot(band, norm_all[:, span(t, group)], preferred_element_type=f32)
        pos = b * rows + lax.broadcasted_iota(jnp.int32, (rows, 1), 0)
        low = jnp.maximum(pos - half_span, 0)
        high = jnp.minimum(pos + window - half_span, seq)
        own = norm_all[span(b, rows), span(t, group)].astype(f32)
        pooled_all[span(b, rows), :] = (total / (high - low).astype(f32) - own).astype(bf16)
        return carry

    def hand_parts(b, e, total):
        for j in range(4):
            part_out[b, e, j % 2, j // 2] = total[j * sub : (j + 1) * sub, :].astype(bf16)
        part_copy(b, e).start()

    def pool_product(b):
        return jnp.dot(pooled_all[span(b, rows), :], wp_own[...], preferred_element_type=f32)

    def second_sum(b, e):
        part_copy(b, e).wait_recv()
        cross_out[b, e] = (
            part_out[b, e, c, 1 - x].astype(f32) + part_in[b, e, 1 - x].astype(f32)
        ).astype(bf16)
        cross_copy(b, e).start()

    def third_sum(b, e, send):
        cross_copy(b, e).wait_recv()
        block_out[b, e] = (
            part_out[b, e, c, x].astype(f32)
            + part_in[b, e, x].astype(f32)
            + cross_in[b, e].astype(f32)
        ).astype(bf16)

        @pl.when(b != s)
        def _():
            send().start()

    def outer_work():
        with scope("otok"):
            for u in (2 * near, 2 * near + 1, 2 * (count - 1 - near)):
                z_copy(u, near).wait_recv()

            @pl.when(sends_near)
            def _():
                kv_first_whole().start()
                for core in range(2):
                    q_whole(core).start()
                w_copy(0).start()
                w_copy(1).start()

            z_copy(2 * (count - 1 - near) + 1, near).wait_recv()
            z_copy(2 * far_edge, near).wait_recv()
            z_copy(2 * far_edge + 1, near).wait_recv()
        local[7].wait()

        def turn(m):
            return jnp.where(half == 0, count - 1 - m, m)

        def hand_on(m, carry):
            pool(turn(m), 0)
            hand_parts(turn(m), 0, pool_product(turn(m)))
            return carry

        with scope("opool"):
            lax.fori_loop(0, count, hand_on, 0)

        @pl.when(sends_relay)
        def _():
            w_copy(0).start()
            w_copy(1).start()

        def cross_over(m, carry):
            second_sum(turn(m), 0)
            return carry

        def hand_out(m, carry):
            third_sum(turn(m), 0, lambda: pool_copy(turn(m)))
            return carry

        with scope("osum"):
            lax.fori_loop(0, count, cross_over, 0)
            lax.fori_loop(0, count, hand_out, 0)

    pl.when(jnp.logical_not(inner))(outer_work)

    def inner_work():
        @pl.when(at_home)
        def _():
            kv_beside().start()
            q_beside().start()

        local[4].wait()
        local[5].wait()
        par_own[0:count, :] = hgain_own[...]
        for i in range(count):
            par_own[count + i : count + i + 1, :] = jnp.full((1, LANES), lam_own[i], f32)

        @pl.when(at_home)
        def _():
            par_copy().start()

        def tok_in(u, onward, beside=tok_forward):
            z_copy(u, other).wait_recv()
            if onward:
                z_copy(u, other).start()
            else:
                z_outward(u).start()
            tok_forward(1, u).start()
            beside(0, u).start()

        def tok_x(u, beside=tok_forward):
            tok_forward(1, u).wait_recv()
            beside(2, u).start()

        def kv_in(owner):
            @pl.when(at_home)
            def _():
                kv_arrival(owner, g).wait_recv()
                kv_forward(0, owner).start()
                kv_forward(1, owner).start()

        def r_arrive(i):
            relay_copy(i).wait_recv()
            relay_forward(i).start()

        def kv_y(owner):
            @pl.when(at_home)
            def _():
                kv_arrival(owner, twin).wait_recv()
                kv_forward(2, owner).start()

        def q_in(owner):
            q_arrival(owner, g).wait_recv()
            q_forward(owner).start()

        owners = (edge, other, far_edge)
        split = (other, far_edge)
        with scope("tok0"):
            tok_in(2 * edge, True)
            tok_in(2 * other, False)
        with scope("tok1"):
            tok_in(2 * edge + 1, True)
            tok_in(2 * other + 1, False)
        with scope("relay0"):

            @pl.when(away)
            def _():
                r_arrive(0)

        with scope("kv1"):
            kv_in(other)
        with scope("x0"):
            tok_x(2 * edge)
            tok_x(2 * other)
        with scope("q1"):
            q_in(other)
        with scope("relay1"):

            @pl.when(away)
            def _():
                r_arrive(1)

        with scope("tok2"):
            tok_in(2 * far_edge, False, tok_late)
        with scope("kvy1"):
            kv_y(other)
        with scope("x1"):
            tok_x(2 * edge + 1)
            tok_x(2 * other + 1)
        with scope("tok3"):
            tok_in(2 * far_edge + 1, False, tok_late)
        with scope("relay2"):

            @pl.when(away)
            def _():
                r_arrive(2)

        with scope("kv0"):

            @pl.when(at_home)
            def _():
                kv_edge().wait_recv()
                kv_edge().start()

        with scope("kv2"):
            kv_in(far_edge)
        with scope("pool"):
            lax.fori_loop(0, count, pool, 0)
        with scope("q2"):

            @pl.when(c == 0)
            def _():
                q_in(far_edge)

        with scope("x2"):
            tok_x(2 * far_edge, tok_late)
            tok_x(2 * far_edge + 1, tok_late)

        early = pl.ds(pl.multiple_of(half * rows, rows), 3 * rows)
        late = span(far_edge, rows)
        k_early = pl.ds(pl.multiple_of(half * shard, shard), 3 * shard)
        k_late = span(far_edge, shard)

        def early_product(store, w):
            store[...] = jnp.dot(
                norm_all[early, k_early], w[k_early, :], preferred_element_type=f32
            )

        def late_product(store, w, put):
            acc = store[...] + jnp.dot(
                norm_all[early, k_late], w[k_late, :], preferred_element_type=f32
            )
            put(early, acc.astype(bf16))
            acc = jnp.dot(norm_all[late, :], w[...], preferred_element_type=f32)
            put(late, acc.astype(bf16))

        def early_tokens(step):
            place = norm_all.at[0 : 2 * rows, 0:quarter]
            got = f_recv.at[2 * count + step // 2]
            return copy(place, place, z_send.at[0], got, {"tp": sib})

        with scope("earlykv"):
            for step in (0, 2):
                early_tokens(step).wait_recv()

            @pl.when(at_home)
            def _():
                local[8].wait()
                local[9].wait()
                local[10].wait()

            @pl.when(away)
            def _():
                kv_edge().wait_recv()
                kv_arrival(other, g).wait_recv()
                kv_arrival(other, twin).wait_recv()
                kv_beside().wait_recv()
                q_beside().wait_recv()
                par_copy().wait_recv()

            early_product(acc_kv, w_kv)
        with scope("kvy2"):
            kv_y(far_edge)
        with scope("earlyq"):
            q_edge().wait_recv()
            q_arrival(other, twin).wait_recv()
            early_product(acc_q, w_q)
        with scope("rest"):
            for step in (0, 2):
                for u in (2 * far_edge, 2 * far_edge + 1):
                    tok_late(step, u).wait_recv()
        with scope("kvrest"):

            @pl.when(away)
            def _():
                kv_arrival(far_edge, g).wait_recv()
                kv_arrival(far_edge, twin).wait_recv()

        def put_kv(at, value):
            k_all[at, :] = value[:, 0:LANES]
            v_all[at, :] = value[:, LANES:pair]

        def put_q(at, value):
            q_all[at, :] = value

        with scope("projkv"):
            late_product(acc_kv, w_kv, put_kv)
        with scope("qrest"):

            @pl.when(c == 0)
            def _():
                q_arrival(far_edge, twin).wait_recv()

            @pl.when(c == 1)
            def _():
                q_far_whole().wait_recv()

        with scope("projq"):
            late_product(acc_q, w_q, put_q)

        par_use[...] = jnp.where(at_home, par_own[...], par_in[...])
        lane = lax.broadcasted_iota(jnp.int32, (rows, LANES), 1)
        lt_rows = lt_send.shape[2]
        base = HD ** (-0.5)

        def two_heads(b):
            zero = jnp.zeros((rows, LANES), bf16)
            parts = []
            for h in range(2):
                q = q_all[span(b, rows), h * LANES : (h + 1) * LANES]
                parts += [jnp.where(lane < HD, q, zero), jnp.where(lane < HD, zero, q)]
            raw = lax.dot_general(
                jnp.concatenate(parts, axis=0),
                k_all[...],
                (((1,), (1,)), ((), ())),
                preferred_element_type=f32,
            )
            highest = jnp.max(raw, axis=-1, keepdims=True)
            weights = jnp.exp2((raw - highest) * (base * math.log2(math.e)))
            totals = jnp.sum(weights, axis=-1, keepdims=True)
            reads = jnp.dot(weights.astype(bf16), v_all[...], preferred_element_type=f32) / totals
            logs = highest * base + jnp.log(totals)
            done = []
            for h in range(2):
                head = 2 * c + h
                first = slice(2 * h * rows, (2 * h + 1) * rows)
                second = slice((2 * h + 1) * rows, (2 * h + 2) * rows)
                contrast = reads[first] - par_use[pl.ds(count + head, 1), :] * reads[second]
                scaled = (
                    contrast
                    * lax.rsqrt(jnp.mean(contrast * contrast, axis=-1, keepdims=True) + epsilon)
                    * par_use[pl.ds(head, 1), :]
                ).astype(bf16)
                done.append((scaled, logs[first], logs[second]))
            return done

        def attend(b):
            done = two_heads(b)
            for h in range(2):
                head_own[span(b, rows), h * LANES : (h + 1) * LANES] = done[h][0]
            head_copy(0, b).start()

            @pl.when(away)
            def _():
                head_copy(1, b).start()

            @pl.when(at_home)
            def _():
                heads_all[c, span(b, rows), :] = head_own[span(b, rows), :]

            both = jnp.where(
                lane < 2,
                jnp.where(lane == 0, done[0][1], done[0][2]),
                jnp.where(lane == 2, done[1][1], done[1][2]),
            )
            padded = jnp.concatenate([both, jnp.zeros((lt_rows - rows, LANES), f32)], axis=0)
            lt_send[b] = jnp.transpose(padded)[0:8, :]

        def send_logs(b, carry):
            @pl.when(jnp.logical_not(at_home & (b == s)))
            def _():
                lt_copy(b).start()

            return carry

        def first_sum(b, e):
            if e == 0:
                for core in range(2):

                    @pl.when(jnp.logical_not(at_home & (c == core)))
                    def _():
                        head_arrival(b, core).wait_recv()

            total = sum(
                jnp.dot(
                    heads_all[core, span(b, rows), :],
                    wa_all[e, core * pair : (core + 1) * pair, :],
                    preferred_element_type=f32,
                )
                for core in range(2)
            )
            hand_parts(b, e, total + pool_product(b) if e == 0 else total)

        def nth(m):
            return jnp.where(m < 2, (count - 1) * m, m - 1)

        def attend_all(m, carry):
            with scope("att"):
                attend(nth(m))

            @pl.when(m == jnp.where(at_home, 0, 1))
            def _():
                with scope("wao"):
                    w_arrival(0).wait_recv()
                    w_forward().start()

            return carry

        lax.fori_loop(0, count, attend_all, 0)
        local[6].wait()
        local[7].wait()

        with scope("S1"):
            first_sum(0, 0)
        lax.fori_loop(0, count, send_logs, 0)
        with scope("S2"):
            second_sum(0, 0)
        with scope("wrest"):
            w_arrival(1).wait_recv()
            w_arrival(2).wait_recv()
        first_sum(0, 1)
        second_sum(0, 1)

        def steps(m, carry):
            @pl.when(m < count)
            def _():
                with scope("S1"):
                    for e in range(2):
                        first_sum(nth(m), e)
                with scope("S2"):
                    for e in range(2):
                        second_sum(nth(m), e)

            @pl.when(m >= 2)
            def _():
                with scope("S3"):
                    for e in range(2):
                        third_sum(nth(m - 2), e, lambda: out_copy(nth(m - 2), e))

            return carry

        lax.fori_loop(1, count + 2, steps, 0)

    pl.when(inner)(inner_work)

    def put_logs(core, ref, at):
        for h in range(2):
            for m in range(2):
                i = 2 * core + h
                lt_out[m, i : i + 1, :] = ref[at, 2 * h + m : 2 * h + m + 1, 0:rows]

    for core in range(2):

        @pl.when(at_home & (c == core))
        def _():
            put_logs(core, lt_send, s)

        @pl.when(jnp.logical_not(at_home & (c == core)))
        def _():
            lt_arrival(core).wait_recv()
            put_logs(core, lt_in, core)

    for i in range(count):
        with scope(f"final{i}"):
            at = slice(i * cols, (i + 1) * cols)
            maker = min(max(i, 1), count - 2)
            e = 0 if i == maker else 1

            @pl.when(s == maker)
            def _():
                mixed_out[:, at] = block_out[s, e]

            @pl.when(s != maker)
            def _():
                out_arrival(i).wait_recv()
                mixed_out[:, at] = block_in[i]

            if e == 1:
                which = i // (count - 1)

                @pl.when(s == i)
                def _():
                    both = mixed_out[:, at].astype(f32) + block_out[s, 0].astype(f32)
                    mixed_out[:, at] = both.astype(bf16)

                @pl.when(s != i)
                def _():
                    pool_arrival(which).wait_recv()
                    both = mixed_out[:, at].astype(f32) + pool_in[which].astype(f32)
                    mixed_out[:, at] = both.astype(bf16)

    def weights_sent(amount):
        all_sent(norm_all.at[0 : amount * pair // width, :], kv_send.at[0])

    @pl.when(sends_near)
    def _():
        weights_sent(3 * shard + 3 * part)

    @pl.when(sends_relay)
    def _():
        weights_sent(shard + 5 * part)

    for core in range(2):

        @pl.when(at_home & (c == core))
        def _():
            weights_sent(3 * shard + (9 - core) * part + seq)

        @pl.when(away & (c == core))
        def _():
            weights_sent(shard + (8 - core) * part + 2 * seq)

    @pl.when(jnp.logical_not(inner))
    def _():
        all_sent(norm_all.at[0:rows, 0:quarter], z_send.at[0])
        all_sent(part_in.at[:, 0], p_send.at[0])
        all_sent(cross_in.at[:, 0], x_send.at[0])
        all_sent(block_out.at[0 : count - 1, 0], o_send.at[0])

    @pl.when(at_home)
    def _():
        par_copy().wait_send()

    @pl.when(inner)
    def _():
        all_sent(norm_all.at[0 : 7 * rows // 2, :], z_send.at[0])
        all_sent(part_in, p_send.at[0])
        all_sent(cross_in, x_send.at[0])
        all_sent(block_out.at[0 : count - 1], o_send.at[0])

    @pl.when(inner & jnp.logical_not(at_home))
    def _():
        all_sent(lt_send, l_send.at[0])

    @pl.when(at_home)
    def _():
        all_sent(lt_send.at[0 : count - 1], l_send.at[0])


def fused(
    count,
    tokens,
    norm_gain,
    query_weight,
    key_weight,
    value_weight,
    map_lambda,
    head_gain,
    attn_out_weight,
    pool_out_weight,
):
    rows, width = tokens.shape
    group, cols = pool_out_weight.shape
    shard = query_weight.shape[0]
    sub = rows // 4
    seq = rows * count
    pair = 2 * LANES
    lt_rows = -(-rows // LANES) * LANES
    bf16, f32 = jnp.bfloat16, jnp.float32
    vmem = pl.BlockSpec(memory_space=pltpu.VMEM)
    far = pl.BlockSpec(memory_space=pl.ANY)
    sems = pltpu.SemaphoreType.DMA
    return pl.pallas_call(
        functools.partial(fused_kernel, count),
        out_shape=(
            pltpu.VMEM((sub, width), bf16),
            pltpu.VMEM((2, count, rows), f32),
        ),
        in_specs=[far] * 9,
        out_specs=(vmem, vmem),
        scratch_shapes=[
            pltpu.VMEM((rows, width), bf16),
            pltpu.VMEM((1, width), f32),
            pltpu.SMEM((count,), f32),
            pltpu.VMEM((count, LANES), f32),
            pltpu.VMEM((seq, width), bf16),
            pltpu.VMEM((shard, pair), bf16),
            pltpu.VMEM((shard, count * LANES), bf16),
            pltpu.VMEM((shard // 2, pair), bf16),
            pltpu.VMEM((shard // 2, pair), bf16),
            pltpu.VMEM((shard, pair), bf16),
            pltpu.VMEM((width, pair), bf16),
            pltpu.VMEM((width, pair), bf16),
            pltpu.VMEM((2, group, cols), bf16),
            pltpu.VMEM((group, cols), bf16),
            pltpu.VMEM((2 * count, LANES), f32),
            pltpu.VMEM((2 * count, LANES), f32),
            pltpu.VMEM((2 * count, LANES), f32),
            pltpu.VMEM((3 * rows, pair), f32),
            pltpu.VMEM((3 * rows, pair), f32),
            pltpu.VMEM((seq, pair), bf16),
            pltpu.VMEM((seq, LANES), bf16),
            pltpu.VMEM((seq, LANES), bf16),
            pltpu.VMEM((seq, pair), bf16),
            pltpu.VMEM((2, seq, pair), bf16),
            pltpu.VMEM((seq, group), bf16),
            pltpu.VMEM((count, 2, 2, 2, sub, cols), bf16),
            pltpu.VMEM((count, 2, 2, sub, cols), bf16),
            pltpu.VMEM((count, 2, sub, cols), bf16),
            pltpu.VMEM((count, 2, sub, cols), bf16),
            pltpu.VMEM((count, 2, sub, cols), bf16),
            pltpu.VMEM((count, sub, cols), bf16),
            pltpu.VMEM((2, sub, cols), bf16),
            pltpu.VMEM((count, 8, lt_rows), f32),
            pltpu.VMEM((2, 8, lt_rows), f32),
            sems((12,)),
            sems((1,)),
            sems((2 * count,)),
            sems((2 * count + 6,)),
            sems((1,)),
            sems((count, 2)),
            sems((count, 2)),
            sems((3,)),
            sems((3,)),
            sems((2,)),
            sems((count, 2)),
            sems((1,)),
            sems((count, 2)),
            sems((1,)),
            sems((count, 2)),
            sems((1,)),
            sems((count + 2,)),
            sems((1,)),
            sems((2,)),
        ],
        compiler_params=pltpu.CompilerParams(collective_id=0, has_side_effects=True),
    )(
        tokens,
        norm_gain.reshape(1, width),
        query_weight,
        key_weight,
        value_weight,
        map_lambda,
        head_gain,
        attn_out_weight,
        pool_out_weight,
    )


def fits(shape, tokens, query_weight, value_weight, map_lambda, pool_out_weight):
    count = shape["sp"]
    return (
        shape["grp"] == 2
        and shape["tp"] == 4
        and count == 4
        and map_lambda.shape[0] == count
        and value_weight.shape[1] == VD == LANES == 2 * HD
        and tokens.shape[0] % 32 == 0
        and tokens.shape[1] % (4 * LANES) == 0
        and query_weight.shape[0] % 32 == 0
        and query_weight.shape[1] == count * LANES
        and pool_out_weight.shape[0] * 4 == tokens.shape[1]
        and pool_out_weight.shape[1] % LANES == 0
        and pool_out_weight.shape[1] * count == tokens.shape[1]
        and pool_out_weight.shape[0] == pool_out_weight.shape[1]
        and pool_out_weight.shape[0] == query_weight.shape[0]
        and tokens.shape[0] * count * tokens.shape[1] <= 1 << 22
    )


def solution(mesh):
    placed = (
        P(("grp", "sp"), None),
        P(),
        P("sp", "tp"),
        P("sp", "tp"),
        P("sp", "tp"),
        P("tp"),
        P("tp", None),
        P("tp", "sp"),
        P("tp", "sp"),
    )
    shape = dict(mesh.shape)

    def chosen(*args):
        if fits(shape, args[0], args[2], args[4], args[5], args[8]):
            return fused(shape["sp"], *args)
        return on_device(*args)

    return jax.shard_map(
        chosen,
        mesh=mesh,
        in_specs=placed,
        out_specs=(P(("grp", "sp", "tp"), None), P(None, "tp", ("grp", "sp"))),
        check_vma=False,
    )
```

```python
import functools
import math

import jax
import jax.numpy as jnp
from jax import lax
from jax.experimental import pallas as pl
from jax.experimental.pallas import tpu as pltpu
from jax.sharding import PartitionSpec as P

HD = 64
VD = 128
POOL_SPAN = 16


epsilon = 1e-06
very_low = -1e30


def extended(cells, sides, width):
    for axis, dim in sides:
        count = lax.axis_size(axis)
        ends = count - 1
        head = lax.slice_in_dim(cells, 0, width, axis=dim)
        tail = lax.slice_in_dim(cells, cells.shape[dim] - width, cells.shape[dim], axis=dim)
        cells = jnp.concatenate(
            [
                lax.ppermute(tail, axis, [(i, (i + 1) % count) for i in range(ends)]),
                cells,
                lax.ppermute(head, axis, [((i + 1) % count, i) for i in range(ends)]),
            ],
            axis=dim,
        )
    return cells


def add_products(totals, pieces, source):
    results = []
    for running, piece in zip(totals, pieces):
        results.append(jnp.dot(source, piece, preferred_element_type=jnp.float32))
    return tuple(results)


def on_device(
    tokens,
    norm_gain,
    query_weight,
    key_weight,
    value_weight,
    map_lambda,
    head_gain,
    attn_out_weight,
    pool_out_weight,
):
    tokens_wide = tokens.astype(jnp.float32)
    normed = (
        tokens_wide
        * lax.rsqrt(jnp.mean(tokens_wide * tokens_wide, axis=-1, keepdims=True) + epsilon)
        * norm_gain
    ).astype(jnp.bfloat16)
    row_count = normed.shape[0]
    sp_index = lax.axis_index("sp")
    tp_index = lax.axis_index("tp")
    group_width = pool_out_weight.shape[0]
    local_heads = map_lambda.shape[0]
    key_heads = value_weight.shape[1] // VD
    group_heads = local_heads // key_heads
    q_empty = jnp.zeros((row_count, query_weight.shape[1]), jnp.float32)
    k_empty = jnp.zeros((row_count, key_weight.shape[1]), jnp.float32)
    v_empty = jnp.zeros((row_count, value_weight.shape[1]), jnp.float32)
    q_acc, k_acc, v_acc = add_products(
        (q_empty, k_empty, v_empty),
        (
            lax.all_gather(query_weight, "sp", axis=0, tiled=True),
            lax.all_gather(key_weight, "sp", axis=0, tiled=True),
            lax.all_gather(value_weight, "sp", axis=0, tiled=True),
        ),
        normed,
    )
    queries = q_acc.astype(jnp.bfloat16).reshape(row_count, key_heads, group_heads, 2, HD)
    keys_flat = k_acc.astype(jnp.bfloat16)
    values_flat = v_acc.astype(jnp.bfloat16)

    def key_block(state_now, key_pair):
        maxima, totals, accums = state_now
        key_blk, val_blk = key_pair
        scores = jnp.einsum(
            "qhgmd,khmd->hgmqk", queries, key_blk, preferred_element_type=jnp.float32
        ) * HD ** (-0.5)
        highest = jnp.maximum(maxima, jnp.max(scores, axis=-1))
        factor = jnp.exp(maxima - highest)
        weights = jnp.exp(scores - highest[..., None])
        totals = totals * factor + jnp.sum(weights, axis=-1)
        accums = accums * factor[..., None] + jnp.einsum(
            "hgmqk,khe->hgmqe",
            weights.astype(jnp.bfloat16),
            val_blk,
            preferred_element_type=jnp.float32,
        )
        return ((highest, totals, accums), None)

    start_state = (
        jnp.full((key_heads, group_heads, 2, row_count), very_low, jnp.float32),
        jnp.zeros((key_heads, group_heads, 2, row_count), jnp.float32),
        jnp.zeros((key_heads, group_heads, 2, row_count, VD), jnp.float32),
    )
    key_piece = lax.all_gather(keys_flat, "sp", axis=0, tiled=True)
    val_piece = lax.all_gather(values_flat, "sp", axis=0, tiled=True)
    piece_len = key_piece.shape[0]
    block_len = math.gcd(piece_len, 512)
    key_blocks = key_piece.reshape(piece_len // block_len, block_len, key_heads, 2, HD)
    val_blocks = val_piece.reshape(piece_len // block_len, block_len, key_heads, VD)
    state_next, unused = lax.scan(key_block, start_state, (key_blocks, val_blocks))
    maxima, totals, accums = state_next
    log_parts = maxima + jnp.log(totals)
    log_totals = jnp.transpose(log_parts, (2, 0, 1, 3)).reshape(2, local_heads, row_count)
    reads = accums / totals[..., None]
    contrast = reads[:, :, 0] - map_lambda.reshape(key_heads, group_heads, 1, 1) * reads[:, :, 1]
    scaled = (
        contrast
        * lax.rsqrt(jnp.mean(contrast * contrast, axis=-1, keepdims=True) + epsilon)
        * head_gain.reshape(key_heads, group_heads, 1, VD)
    )
    attention_head_rows = (
        jnp.transpose(scaled, (2, 0, 1, 3))
        .reshape(row_count, local_heads * VD)
        .astype(jnp.bfloat16)
    )
    head_rows, log_totals = (attention_head_rows, log_totals)
    own_chan = lax.dynamic_slice_in_dim(normed, tp_index * group_width, group_width, 1)
    reach = POOL_SPAN // 2
    padded = extended(own_chan, (("sp", 0),), reach)
    window = jnp.left_shift(jnp.int32(2), tp_index)
    half_span = window // 2
    running = jnp.zeros((row_count, group_width), jnp.float32)
    for offset in range(POOL_SPAN):
        piece = lax.dynamic_slice_in_dim(padded, reach - half_span + offset, row_count, 0).astype(
            jnp.float32
        )
        running = running + jnp.where(offset < window, piece, 0.0)
    seq_len = row_count * lax.axis_size("sp")
    position = sp_index * row_count + jnp.arange(row_count, dtype=jnp.int32)
    lower_edge = jnp.clip(position - half_span, 0, seq_len)
    upper_edge = jnp.clip(position + window - half_span, 0, seq_len)
    counts_f = (upper_edge - lower_edge).astype(jnp.float32)[:, None]
    pooled = (running / counts_f - own_chan.astype(jnp.float32)).astype(jnp.bfloat16)
    attn_whole, pool_whole = (
        lax.all_gather(attn_out_weight, "sp", axis=1, tiled=True),
        lax.all_gather(pool_out_weight, "sp", axis=1, tiled=True),
    )
    mixed = lax.psum_scatter(
        (
            jnp.dot(head_rows, attn_whole, preferred_element_type=jnp.float32)
            + jnp.dot(pooled, pool_whole, preferred_element_type=jnp.float32)
        ).astype(jnp.bfloat16),
        "tp",
        scatter_dimension=0,
        tiled=True,
    )
    return (mixed, log_totals)


MESH = pl.DeviceIdType.MESH
LANES = 128
scope = jax.named_scope


def fused_kernel(
    count,
    tok,
    gain,
    wq,
    wk,
    wv,
    lam,
    hgain,
    wao,
    wpo,
    mixed_out,
    lt_out,
    tok_own,
    gain_own,
    lam_own,
    hgain_own,
    norm_all,
    kv_own,
    q_own,
    kv_relay,
    q_relay,
    q_relay_whole,
    w_kv,
    w_q,
    wa_all,
    wp_own,
    par_own,
    par_in,
    par_use,
    acc_kv,
    acc_q,
    q_all,
    k_all,
    v_all,
    head_own,
    heads_all,
    pooled_all,
    part_out,
    part_in,
    cross_out,
    cross_in,
    block_out,
    block_in,
    pool_in,
    lt_send,
    lt_in,
    local_sem,
    z_send,
    z_recv,
    f_recv,
    kv_send,
    kv_recv,
    q_recv,
    r_recv,
    w_recv,
    par_sem,
    h_recv,
    p_send,
    p_recv,
    x_send,
    x_recv,
    o_send,
    o_recv,
    l_send,
    l_recv,
):
    g = lax.axis_index("grp")
    s = lax.axis_index("sp")
    t = lax.axis_index("tp")
    c = lax.rem(t, 2)
    x = t // 2
    rows, width = tok.shape
    quarter = width // 4
    shard = wq.shape[0]
    part = shard // 2
    pair = 2 * LANES
    group = wpo.shape[0]
    cols = wpo.shape[1]
    half = s // 2
    inner = (s > 0) & (s < count - 1)
    at_home = inner & (c == half)
    away = inner & (c != half)
    sib = t + 1 - 2 * c
    far = lax.rem(t + 2, 4)
    twin = 1 - g
    near = 1 + half
    other = count - 1 - s
    edge = jnp.where(half == 0, 0, count - 1)
    far_edge = count - 1 - edge
    target = 1 + c
    home = 2 * x + half
    f32, bf16 = jnp.float32, jnp.bfloat16

    def span(index, size):
        return pl.ds(pl.multiple_of(index * size, size), size)

    def half_rows(owner, which):
        return pl.ds(pl.multiple_of(owner * shard + which * part, part), part)

    barrier = pltpu.get_barrier_semaphore()

    def greet(where):
        pl.semaphore_signal(barrier, inc=1, device_id=where, device_id_type=MESH)

    def greet_beside(up):
        peer = lax.rem(s + (1 if up else count - 1), count)
        greet({"sp": peer})
        greet({"sp": peer, "tp": sib})

    @pl.when(s < count - 1)
    def _():
        greet_beside(True)

    @pl.when(s > 0)
    def _():
        greet_beside(False)

    greet({"tp": sib})
    greet({"tp": far})

    @pl.when(inner)
    def _():
        greet({"grp": twin})

    pieces = (
        (tok, tok_own),
        (gain, gain_own),
        (wk, kv_own.at[:, 0:LANES]),
        (wv, kv_own.at[:, LANES:pair]),
        (lam, lam_own),
        (hgain, hgain_own),
        (wao, wa_all.at[0]),
        (wpo, wp_own),
        (wk, w_kv.at[span(s, shard), 0:LANES]),
        (wv, w_kv.at[span(s, shard), LANES:pair]),
        (wq.at[:, span(c, pair)], w_q.at[span(s, shard), :]),
        (wq, q_own),
    )
    local = [
        pltpu.make_async_copy(src, dst, local_sem.at[i]) for i, (src, dst) in enumerate(pieces)
    ]
    for piece in local[:4]:
        piece.start()
    local[11].start()

    local[7].start()

    @pl.when(inner)
    def _():
        for piece in local[4:7]:
            piece.start()

    @pl.when(at_home)
    def _():
        for piece in local[8:11]:
            piece.start()

    def copy(src, dst, send, recv, where):
        return pltpu.make_async_remote_copy(
            src_ref=src,
            dst_ref=dst,
            send_sem=send,
            recv_sem=recv,
            device_id=where,
            device_id_type=MESH,
        )

    chunk = rows // 2

    def z_copy(u, dest):
        place = norm_all.at[span(u, chunk), span(t, quarter)]
        return copy(place, place, z_send.at[0], z_recv.at[u], {"sp": dest})

    def z_outward(u):
        place = norm_all.at[span(u, chunk), span(t, quarter)]
        return copy(place, place, z_send.at[0], z_recv.at[u], {"sp": edge})

    def tok_forward(step, u):
        col = span(far if step == 2 else t, quarter)
        place = norm_all.at[span(u, chunk), col]
        where = {"tp": far if step == 1 else sib}
        got = f_recv.at[u] if step == 1 else f_recv.at[2 * count + step // 2]
        return copy(place, place, z_send.at[0], got, where)

    def tok_late(step, u):
        col = span(far if step == 2 else t, quarter)
        place = norm_all.at[span(u, chunk), col]
        got = f_recv.at[2 * count + 2 + step + lax.rem(u, 2)]
        return copy(place, place, z_send.at[0], got, {"tp": sib})

    def all_sent(ref, sem):
        copy(ref, ref, sem, sem, {"tp": sib}).wait_send()

    def kv_first():
        src = kv_own.at[span(g, part), :]
        dst = w_kv.at[half_rows(s, g), :]
        return copy(src, dst, kv_send.at[0], kv_recv.at[s, g], {"sp": target})

    def kv_first_whole():
        dst = w_kv.at[span(s, shard), :]
        return copy(kv_own, dst, kv_send.at[0], kv_recv.at[s, 0], {"sp": near})

    def kv_beside():
        dst = w_kv.at[span(s, shard), :]
        return copy(kv_own, dst, kv_send.at[0], kv_recv.at[s, 0], {"tp": sib})

    def kv_edge():
        place = w_kv.at[span(edge, shard), :]
        return copy(place, place, kv_send.at[0], kv_recv.at[edge, 0], {"tp": sib})

    def kv_forward(kind, owner):
        which = twin if kind == 2 else g
        place = w_kv.at[half_rows(owner, which), :]
        where = {"grp": twin} if kind == 0 else {"tp": sib}
        return copy(place, place, kv_send.at[0], kv_recv.at[owner, which], where)

    def kv_arrival(owner, which):
        place = w_kv.at[half_rows(owner, which), :]
        return copy(place, place, kv_send.at[0], kv_recv.at[owner, which], {"tp": sib})

    def q_copy(core):
        src = q_own.at[span(g, part), core * pair : (core + 1) * pair]
        dst = w_q.at[half_rows(s, g), :]
        where = {"sp": target, "tp": 2 * x + core}
        return copy(src, dst, kv_send.at[0], q_recv.at[s, g], where)

    def q_whole(core):
        src = q_own.at[:, core * pair : (core + 1) * pair]
        dst = w_q.at[span(s, shard), :]
        where = {"sp": near, "tp": 2 * x + core}
        return copy(src, dst, kv_send.at[0], q_recv.at[s, 0], where)

    def q_edge():
        place = w_q.at[span(edge, shard), :]
        return copy(place, place, kv_send.at[0], q_recv.at[edge, 0], {"tp": sib})

    def relay_copy(i):
        if i == 0:
            src, dst = kv_own.at[span(g, part), :], kv_relay
        elif i == 1:
            src, dst = q_own.at[span(g, part), 0:pair], q_relay
        else:
            src, dst = q_own.at[:, pair : 2 * pair], q_relay_whole
        send = kv_send.at[0]
        return copy(src, dst, send, r_recv.at[i], {"sp": near})

    def relay_forward(i):
        if i == 0:
            dst = w_kv.at[half_rows(edge, g), :]
            return copy(kv_relay, dst, kv_send.at[0], kv_recv.at[edge, g], {"sp": other})
        where = {"sp": other, "tp": 2 * x + i - 1}
        if i == 1:
            dst = w_q.at[half_rows(edge, g), :]
            return copy(q_relay, dst, kv_send.at[0], q_recv.at[edge, g], where)
        dst = w_q.at[span(edge, shard), :]
        return copy(q_relay_whole, dst, kv_send.at[0], q_recv.at[edge, 0], where)

    def q_far_whole():
        place = w_q.at[span(far_edge, shard), :]
        return copy(place, place, kv_send.at[0], q_recv.at[far_edge, 0], {"tp": sib})

    def q_beside():
        src = q_own.at[:, span(1 - c, pair)]
        return copy(src, w_q.at[span(s, shard), :], kv_send.at[0], q_recv.at[s, 0], {"tp": sib})

    def q_forward(owner):
        place = w_q.at[half_rows(owner, g), :]
        return copy(place, place, kv_send.at[0], q_recv.at[owner, g], {"grp": twin})

    def q_arrival(owner, which):
        place = w_q.at[half_rows(owner, which), :]
        return copy(place, place, kv_send.at[0], q_recv.at[owner, which], {"grp": twin})

    w_rows = (span(g, part // 2), pl.ds(part, part), span(twin, part // 2))

    def w_copy(kind):
        src, dst = wao.at[w_rows[kind], :], wa_all.at[1, w_rows[kind], :]
        return copy(src, dst, kv_send.at[0], w_recv.at[kind], {"sp": near})

    def w_forward():
        place = wa_all.at[1, w_rows[0], :]
        return copy(place, place, kv_send.at[0], w_recv.at[2], {"grp": twin})

    def w_arrival(kind):
        place = wa_all.at[1, w_rows[kind], :]
        return copy(place, place, kv_send.at[0], w_recv.at[kind], {"grp": twin})

    def par_copy():
        return copy(par_own, par_in, par_sem.at[0], par_sem.at[1], {"tp": sib})

    head_where = ({"sp": other, "tp": home}, {"tp": sib})

    def head_copy(kind, b):
        dst = heads_all.at[c, span(b, rows), :]
        src = head_own.at[span(b, rows), :]
        return copy(src, dst, kv_send.at[0], h_recv.at[b, c], head_where[kind])

    def head_arrival(b, core):
        place = heads_all.at[core, span(b, rows), :]
        return copy(place, place, kv_send.at[0], h_recv.at[b, core], {"tp": sib})

    def lt_copy(b):
        where = {"sp": b, "tp": home}
        return copy(lt_send.at[b], lt_in.at[c], l_send.at[0], l_recv.at[c], where)

    def lt_arrival(core):
        return copy(lt_send.at[0], lt_in.at[core], l_send.at[0], l_recv.at[core], {"tp": sib})

    def part_copy(b, e):
        src = part_out.at[b, e, 1 - c]
        return copy(src, part_in.at[b, e], p_send.at[0], p_recv.at[b, e], {"tp": sib})

    def cross_copy(b, e):
        src = cross_out.at[b, e]
        return copy(src, cross_in.at[b, e], x_send.at[0], x_recv.at[b, e], {"tp": far})

    def out_copy(b, e):
        to = s if e == 0 else edge
        return copy(block_out.at[b, e], block_in.at[to], o_send.at[0], o_recv.at[to], {"sp": b})

    def out_arrival(i):
        return copy(block_out.at[0, 0], block_in.at[i], o_send.at[0], o_recv.at[i], {"sp": near})

    def pool_copy(b):
        dst = pool_in.at[half]
        where = {"sp": b}
        return copy(block_out.at[b, 0], dst, o_send.at[0], o_recv.at[count + half], where)

    def pool_arrival(i):
        dst = pool_in.at[i]
        return copy(block_out.at[0, 0], dst, o_send.at[0], o_recv.at[count + i], {"sp": near})

    local[0].wait()
    local[1].wait()
    step = rows // 2

    def norm_rows(i, carry):
        at = pl.ds(pl.multiple_of(i * step, step), step)
        v = tok_own[at, :].astype(f32)
        scale = lax.rsqrt(jnp.mean(v * v, axis=-1, keepdims=True) + epsilon)
        to = pl.ds(pl.multiple_of(s * rows + i * step, step), step)
        norm_all[to, :] = (v * scale * gain_own[...]).astype(bf16)
        return carry

    with scope("norm"):
        lax.fori_loop(0, rows // step, norm_rows, 0)
    with scope("barrier"):
        pl.semaphore_wait(barrier, jnp.where(inner, 7, 4))
    sends_on = s != target

    @pl.when(inner)
    def _():
        z_copy(2 * s, other).start()
        z_copy(2 * s + 1, other).start()
        z_outward(2 * s).start()
        z_outward(2 * s + 1).start()

    @pl.when(jnp.logical_not(inner))
    def _():
        z_copy(2 * s, near).start()
        z_copy(2 * s + 1, near).start()

    local[2].wait()
    local[3].wait()
    local[11].wait()

    sends_near = jnp.logical_not(inner) & (c == half)

    sends_relay = jnp.logical_not(inner) & (c != half)

    @pl.when(sends_relay)
    def _():
        for i in range(3):
            relay_copy(i).start()

    @pl.when(away)
    def _():
        kv_first().start()
        for core in range(2):
            q_copy(core).start()

    seq = rows * count
    window = jnp.where(t == 0, 2, jnp.where(t == 1, 4, jnp.where(t == 2, 8, 16)))
    half_span = window // 2
    sub = rows // 4

    def pool(b, carry):
        at = b * rows + lax.broadcasted_iota(jnp.int32, (rows, seq), 0)
        col = lax.broadcasted_iota(jnp.int32, (rows, seq), 1)
        inside = (col >= at - half_span) & (col < at + window - half_span)
        band = jnp.where(inside, 1.0, 0.0).astype(bf16)
        total = jnp.dot(band, norm_all[:, span(t, group)], preferred_element_type=f32)
        pos = b * rows + lax.broadcasted_iota(jnp.int32, (rows, 1), 0)
        low = jnp.maximum(pos - half_span, 0)
        high = jnp.minimum(pos + window - half_span, seq)
        own = norm_all[span(b, rows), span(t, group)].astype(f32)
        pooled_all[span(b, rows), :] = (total / (high - low).astype(f32) - own).astype(bf16)
        return carry

    def hand_parts(b, e, total):
        for j in range(4):
            part_out[b, e, j % 2, j // 2] = total[j * sub : (j + 1) * sub, :].astype(bf16)
        part_copy(b, e).start()

    def pool_product(b):
        return jnp.dot(pooled_all[span(b, rows), :], wp_own[...], preferred_element_type=f32)

    def second_sum(b, e):
        part_copy(b, e).wait_recv()
        cross_out[b, e] = (
            part_out[b, e, c, 1 - x].astype(f32) + part_in[b, e, 1 - x].astype(f32)
        ).astype(bf16)
        cross_copy(b, e).start()

    def third_sum(b, e, send):
        cross_copy(b, e).wait_recv()
        block_out[b, e] = (
            part_out[b, e, c, x].astype(f32)
            + part_in[b, e, x].astype(f32)
            + cross_in[b, e].astype(f32)
        ).astype(bf16)

        @pl.when(b != s)
        def _():
            send().start()

    def outer_work():
        with scope("otok"):
            for u in (2 * near, 2 * near + 1, 2 * (count - 1 - near)):
                z_copy(u, near).wait_recv()

            @pl.when(sends_near)
            def _():
                kv_first_whole().start()
                for core in range(2):
                    q_whole(core).start()
                w_copy(0).start()
                w_copy(1).start()

            z_copy(2 * (count - 1 - near) + 1, near).wait_recv()
            z_copy(2 * far_edge, near).wait_recv()
            z_copy(2 * far_edge + 1, near).wait_recv()
        local[7].wait()

        def turn(m):
            return jnp.where(half == 0, count - 1 - m, m)

        def hand_on(m, carry):
            pool(turn(m), 0)
            hand_parts(turn(m), 0, pool_product(turn(m)))
            return carry

        with scope("opool"):
            lax.fori_loop(0, count, hand_on, 0)

        @pl.when(sends_relay)
        def _():
            w_copy(0).start()
            w_copy(1).start()

        def cross_over(m, carry):
            second_sum(turn(m), 0)
            return carry

        def hand_out(m, carry):
            third_sum(turn(m), 0, lambda: pool_copy(turn(m)))
            return carry

        with scope("osum"):
            lax.fori_loop(0, count, cross_over, 0)
            lax.fori_loop(0, count, hand_out, 0)

    pl.when(jnp.logical_not(inner))(outer_work)

    def inner_work():
        @pl.when(at_home)
        def _():
            kv_beside().start()
            q_beside().start()

        local[4].wait()
        local[5].wait()
        par_own[0:count, :] = hgain_own[...]
        for i in range(count):
            par_own[count + i : count + i + 1, :] = jnp.full((1, LANES), lam_own[i], f32)

        @pl.when(at_home)
        def _():
            par_copy().start()

        def tok_in(u, onward, beside=tok_forward):
            z_copy(u, other).wait_recv()
            if onward:
                z_copy(u, other).start()
            else:
                z_outward(u).start()
            tok_forward(1, u).start()
            beside(0, u).start()

        def tok_x(u, beside=tok_forward):
            tok_forward(1, u).wait_recv()
            beside(2, u).start()

        def kv_in(owner):
            @pl.when(at_home)
            def _():
                kv_arrival(owner, g).wait_recv()
                kv_forward(0, owner).start()
                kv_forward(1, owner).start()

        def r_arrive(i):
            relay_copy(i).wait_recv()
            relay_forward(i).start()

        def kv_y(owner):
            @pl.when(at_home)
            def _():
                kv_arrival(owner, twin).wait_recv()
                kv_forward(2, owner).start()

        def q_in(owner):
            q_arrival(owner, g).wait_recv()
            q_forward(owner).start()

        owners = (edge, other, far_edge)
        split = (other, far_edge)
        with scope("tok0"):
            tok_in(2 * edge, True)
            tok_in(2 * other, False)
        with scope("tok1"):
            tok_in(2 * edge + 1, True)
            tok_in(2 * other + 1, False)
        with scope("relay0"):

            @pl.when(away)
            def _():
                r_arrive(0)

        with scope("kv1"):
            kv_in(other)
        with scope("x0"):
            tok_x(2 * edge)
            tok_x(2 * other)
        with scope("q1"):
            q_in(other)
        with scope("relay1"):

            @pl.when(away)
            def _():
                r_arrive(1)

        with scope("tok2"):
            tok_in(2 * far_edge, False, tok_late)
        with scope("kvy1"):
            kv_y(other)
        with scope("x1"):
            tok_x(2 * edge + 1)
            tok_x(2 * other + 1)
        with scope("tok3"):
            tok_in(2 * far_edge + 1, False, tok_late)
        with scope("relay2"):

            @pl.when(away)
            def _():
                r_arrive(2)

        with scope("kv0"):

            @pl.when(at_home)
            def _():
                kv_edge().wait_recv()
                kv_edge().start()

        with scope("kv2"):
            kv_in(far_edge)
        with scope("pool"):
            lax.fori_loop(0, count, pool, 0)
        with scope("q2"):

            @pl.when(c == 0)
            def _():
                q_in(far_edge)

        with scope("x2"):
            tok_x(2 * far_edge, tok_late)
            tok_x(2 * far_edge + 1, tok_late)

        early = pl.ds(pl.multiple_of(half * rows, rows), 3 * rows)
        late = span(far_edge, rows)
        k_early = pl.ds(pl.multiple_of(half * shard, shard), 3 * shard)
        k_late = span(far_edge, shard)

        def early_product(store, w):
            store[...] = jnp.dot(
                norm_all[early, k_early], w[k_early, :], preferred_element_type=f32
            )

        def late_product(store, w, put):
            acc = store[...] + jnp.dot(
                norm_all[early, k_late], w[k_late, :], preferred_element_type=f32
            )
            put(early, acc.astype(bf16))
            acc = jnp.dot(norm_all[late, :], w[...], preferred_element_type=f32)
            put(late, acc.astype(bf16))

        def early_tokens(step):
            place = norm_all.at[0 : 2 * rows, 0:quarter]
            got = f_recv.at[2 * count + step // 2]
            return copy(place, place, z_send.at[0], got, {"tp": sib})

        with scope("earlykv"):
            for step in (0, 2):
                early_tokens(step).wait_recv()

            @pl.when(at_home)
            def _():
                local[8].wait()
                local[9].wait()
                local[10].wait()

            @pl.when(away)
            def _():
                kv_edge().wait_recv()
                kv_arrival(other, g).wait_recv()
                kv_arrival(other, twin).wait_recv()
                kv_beside().wait_recv()
                q_beside().wait_recv()
                par_copy().wait_recv()

            early_product(acc_kv, w_kv)
        with scope("kvy2"):
            kv_y(far_edge)
        k_edge = span(edge, shard)

        def add_edge():
            q_edge().wait_recv()
            acc_q[...] += jnp.dot(
                norm_all[early, k_edge], w_q[k_edge, :], preferred_element_type=f32
            )

        with scope("earlyq"):
            q_arrival(other, twin).wait_recv()
            acc_q[...] = jnp.dot(
                norm_all[early, shard : 3 * shard],
                w_q[shard : 3 * shard, :],
                preferred_element_type=f32,
            )

        @pl.when(away)
        def _():
            with scope("edgeq"):
                add_edge()

        with scope("rest"):
            for step in (0, 2):
                for u in (2 * far_edge, 2 * far_edge + 1):
                    tok_late(step, u).wait_recv()
        with scope("kvrest"):

            @pl.when(away)
            def _():
                kv_arrival(far_edge, g).wait_recv()
                kv_arrival(far_edge, twin).wait_recv()

        def put_kv(at, value):
            k_all[at, :] = value[:, 0:LANES]
            v_all[at, :] = value[:, LANES:pair]

        def put_q(at, value):
            q_all[at, :] = value

        with scope("projkv"):
            late_product(acc_kv, w_kv, put_kv)
        @pl.when(at_home)
        def _():
            with scope("edgeq"):
                add_edge()

        with scope("qrest"):

            @pl.when(c == 0)
            def _():
                q_arrival(far_edge, twin).wait_recv()

            @pl.when(c == 1)
            def _():
                q_far_whole().wait_recv()

        with scope("projq"):
            late_product(acc_q, w_q, put_q)

        par_use[...] = jnp.where(at_home, par_own[...], par_in[...])
        lane = lax.broadcasted_iota(jnp.int32, (rows, LANES), 1)
        lt_rows = lt_send.shape[2]
        base = HD ** (-0.5)

        def two_heads(b):
            zero = jnp.zeros((rows, LANES), bf16)
            parts = []
            for h in range(2):
                q = q_all[span(b, rows), h * LANES : (h + 1) * LANES]
                parts += [jnp.where(lane < HD, q, zero), jnp.where(lane < HD, zero, q)]
            raw = lax.dot_general(
                jnp.concatenate(parts, axis=0),
                k_all[...],
                (((1,), (1,)), ((), ())),
                preferred_element_type=f32,
            )
            highest = jnp.max(raw, axis=-1, keepdims=True)
            weights = jnp.exp2((raw - highest) * (base * math.log2(math.e)))
            totals = jnp.sum(weights, axis=-1, keepdims=True)
            reads = jnp.dot(weights.astype(bf16), v_all[...], preferred_element_type=f32) / totals
            logs = highest * base + jnp.log(totals)
            done = []
            for h in range(2):
                head = 2 * c + h
                first = slice(2 * h * rows, (2 * h + 1) * rows)
                second = slice((2 * h + 1) * rows, (2 * h + 2) * rows)
                contrast = reads[first] - par_use[pl.ds(count + head, 1), :] * reads[second]
                scaled = (
                    contrast
                    * lax.rsqrt(jnp.mean(contrast * contrast, axis=-1, keepdims=True) + epsilon)
                    * par_use[pl.ds(head, 1), :]
                ).astype(bf16)
                done.append((scaled, logs[first], logs[second]))
            return done

        def attend(b):
            done = two_heads(b)
            for h in range(2):
                head_own[span(b, rows), h * LANES : (h + 1) * LANES] = done[h][0]
            head_copy(0, b).start()

            @pl.when(away)
            def _():
                head_copy(1, b).start()

            @pl.when(at_home)
            def _():
                heads_all[c, span(b, rows), :] = head_own[span(b, rows), :]

            both = jnp.where(
                lane < 2,
                jnp.where(lane == 0, done[0][1], done[0][2]),
                jnp.where(lane == 2, done[1][1], done[1][2]),
            )
            padded = jnp.concatenate([both, jnp.zeros((lt_rows - rows, LANES), f32)], axis=0)
            lt_send[b] = jnp.transpose(padded)[0:8, :]

        def send_logs(b, carry):
            @pl.when(jnp.logical_not(at_home & (b == s)))
            def _():
                lt_copy(b).start()

            return carry

        def first_sum(b, e):
            if e == 0:
                for core in range(2):

                    @pl.when(jnp.logical_not(at_home & (c == core)))
                    def _():
                        head_arrival(b, core).wait_recv()

            total = sum(
                jnp.dot(
                    heads_all[core, span(b, rows), :],
                    wa_all[e, core * pair : (core + 1) * pair, :],
                    preferred_element_type=f32,
                )
                for core in range(2)
            )
            hand_parts(b, e, total + pool_product(b) if e == 0 else total)

        def nth(m):
            return jnp.where(m < 2, (count - 1) * m, m - 1)

        def attend_all(m, carry):
            with scope("att"):
                attend(nth(m))

            @pl.when(m == jnp.where(at_home, 0, 1))
            def _():
                with scope("wao"):
                    w_arrival(0).wait_recv()
                    w_forward().start()

            return carry

        lax.fori_loop(0, count, attend_all, 0)
        local[6].wait()
        local[7].wait()

        with scope("S1"):
            first_sum(0, 0)
        lax.fori_loop(0, count, send_logs, 0)
        with scope("S2"):
            second_sum(0, 0)
        with scope("wrest"):
            w_arrival(1).wait_recv()
            w_arrival(2).wait_recv()
        first_sum(0, 1)
        second_sum(0, 1)

        def steps(m, carry):
            @pl.when(m < count)
            def _():
                with scope("S1"):
                    for e in range(2):
                        first_sum(nth(m), e)
                with scope("S2"):
                    for e in range(2):
                        second_sum(nth(m), e)

            @pl.when(m >= 2)
            def _():
                with scope("S3"):
                    for e in range(2):
                        third_sum(nth(m - 2), e, lambda: out_copy(nth(m - 2), e))

            return carry

        lax.fori_loop(1, count + 2, steps, 0)

    pl.when(inner)(inner_work)

    def put_logs(core, ref, at):
        for h in range(2):
            for m in range(2):
                i = 2 * core + h
                lt_out[m, i : i + 1, :] = ref[at, 2 * h + m : 2 * h + m + 1, 0:rows]

    for core in range(2):

        @pl.when(at_home & (c == core))
        def _():
            put_logs(core, lt_send, s)

        @pl.when(jnp.logical_not(at_home & (c == core)))
        def _():
            lt_arrival(core).wait_recv()
            put_logs(core, lt_in, core)

    for i in range(count):
        with scope(f"final{i}"):
            at = slice(i * cols, (i + 1) * cols)
            maker = min(max(i, 1), count - 2)
            e = 0 if i == maker else 1

            @pl.when(s == maker)
            def _():
                mixed_out[:, at] = block_out[s, e]

            @pl.when(s != maker)
            def _():
                out_arrival(i).wait_recv()
                mixed_out[:, at] = block_in[i]

            if e == 1:
                which = i // (count - 1)

                @pl.when(s == i)
                def _():
                    both = mixed_out[:, at].astype(f32) + block_out[s, 0].astype(f32)
                    mixed_out[:, at] = both.astype(bf16)

                @pl.when(s != i)
                def _():
                    pool_arrival(which).wait_recv()
                    both = mixed_out[:, at].astype(f32) + pool_in[which].astype(f32)
                    mixed_out[:, at] = both.astype(bf16)

    def weights_sent(amount):
        all_sent(norm_all.at[0 : amount * pair // width, :], kv_send.at[0])

    @pl.when(sends_near)
    def _():
        weights_sent(3 * shard + 3 * part)

    @pl.when(sends_relay)
    def _():
        weights_sent(shard + 5 * part)

    for core in range(2):

        @pl.when(at_home & (c == core))
        def _():
            weights_sent(3 * shard + (9 - core) * part + seq)

        @pl.when(away & (c == core))
        def _():
            weights_sent(shard + (8 - core) * part + 2 * seq)

    @pl.when(jnp.logical_not(inner))
    def _():
        all_sent(norm_all.at[0:rows, 0:quarter], z_send.at[0])
        all_sent(part_in.at[:, 0], p_send.at[0])
        all_sent(cross_in.at[:, 0], x_send.at[0])
        all_sent(block_out.at[0 : count - 1, 0], o_send.at[0])

    @pl.when(at_home)
    def _():
        par_copy().wait_send()

    @pl.when(inner)
    def _():
        all_sent(norm_all.at[0 : 7 * rows // 2, :], z_send.at[0])
        all_sent(part_in, p_send.at[0])
        all_sent(cross_in, x_send.at[0])
        all_sent(block_out.at[0 : count - 1], o_send.at[0])

    @pl.when(inner & jnp.logical_not(at_home))
    def _():
        all_sent(lt_send, l_send.at[0])

    @pl.when(at_home)
    def _():
        all_sent(lt_send.at[0 : count - 1], l_send.at[0])


def fused(
    count,
    tokens,
    norm_gain,
    query_weight,
    key_weight,
    value_weight,
    map_lambda,
    head_gain,
    attn_out_weight,
    pool_out_weight,
):
    rows, width = tokens.shape
    group, cols = pool_out_weight.shape
    shard = query_weight.shape[0]
    sub = rows // 4
    seq = rows * count
    pair = 2 * LANES
    lt_rows = -(-rows // LANES) * LANES
    bf16, f32 = jnp.bfloat16, jnp.float32
    vmem = pl.BlockSpec(memory_space=pltpu.VMEM)
    far = pl.BlockSpec(memory_space=pl.ANY)
    sems = pltpu.SemaphoreType.DMA
    return pl.pallas_call(
        functools.partial(fused_kernel, count),
        out_shape=(
            pltpu.VMEM((sub, width), bf16),
            pltpu.VMEM((2, count, rows), f32),
        ),
        in_specs=[far] * 9,
        out_specs=(vmem, vmem),
        scratch_shapes=[
            pltpu.VMEM((rows, width), bf16),
            pltpu.VMEM((1, width), f32),
            pltpu.SMEM((count,), f32),
            pltpu.VMEM((count, LANES), f32),
            pltpu.VMEM((seq, width), bf16),
            pltpu.VMEM((shard, pair), bf16),
            pltpu.VMEM((shard, count * LANES), bf16),
            pltpu.VMEM((shard // 2, pair), bf16),
            pltpu.VMEM((shard // 2, pair), bf16),
            pltpu.VMEM((shard, pair), bf16),
            pltpu.VMEM((width, pair), bf16),
            pltpu.VMEM((width, pair), bf16),
            pltpu.VMEM((2, group, cols), bf16),
            pltpu.VMEM((group, cols), bf16),
            pltpu.VMEM((2 * count, LANES), f32),
            pltpu.VMEM((2 * count, LANES), f32),
            pltpu.VMEM((2 * count, LANES), f32),
            pltpu.VMEM((3 * rows, pair), f32),
            pltpu.VMEM((3 * rows, pair), f32),
            pltpu.VMEM((seq, pair), bf16),
            pltpu.VMEM((seq, LANES), bf16),
            pltpu.VMEM((seq, LANES), bf16),
            pltpu.VMEM((seq, pair), bf16),
            pltpu.VMEM((2, seq, pair), bf16),
            pltpu.VMEM((seq, group), bf16),
            pltpu.VMEM((count, 2, 2, 2, sub, cols), bf16),
            pltpu.VMEM((count, 2, 2, sub, cols), bf16),
            pltpu.VMEM((count, 2, sub, cols), bf16),
            pltpu.VMEM((count, 2, sub, cols), bf16),
            pltpu.VMEM((count, 2, sub, cols), bf16),
            pltpu.VMEM((count, sub, cols), bf16),
            pltpu.VMEM((2, sub, cols), bf16),
            pltpu.VMEM((count, 8, lt_rows), f32),
            pltpu.VMEM((2, 8, lt_rows), f32),
            sems((12,)),
            sems((1,)),
            sems((2 * count,)),
            sems((2 * count + 6,)),
            sems((1,)),
            sems((count, 2)),
            sems((count, 2)),
            sems((3,)),
            sems((3,)),
            sems((2,)),
            sems((count, 2)),
            sems((1,)),
            sems((count, 2)),
            sems((1,)),
            sems((count, 2)),
            sems((1,)),
            sems((count + 2,)),
            sems((1,)),
            sems((2,)),
        ],
        compiler_params=pltpu.CompilerParams(collective_id=0, has_side_effects=True),
    )(
        tokens,
        norm_gain.reshape(1, width),
        query_weight,
        key_weight,
        value_weight,
        map_lambda,
        head_gain,
        attn_out_weight,
        pool_out_weight,
    )


def fits(shape, tokens, query_weight, value_weight, map_lambda, pool_out_weight):
    count = shape["sp"]
    return (
        shape["grp"] == 2
        and shape["tp"] == 4
        and count == 4
        and map_lambda.shape[0] == count
        and value_weight.shape[1] == VD == LANES == 2 * HD
        and tokens.shape[0] % 32 == 0
        and tokens.shape[1] % (4 * LANES) == 0
        and query_weight.shape[0] % 32 == 0
        and query_weight.shape[1] == count * LANES
        and pool_out_weight.shape[0] * 4 == tokens.shape[1]
        and pool_out_weight.shape[1] % LANES == 0
        and pool_out_weight.shape[1] * count == tokens.shape[1]
        and pool_out_weight.shape[0] == pool_out_weight.shape[1]
        and pool_out_weight.shape[0] == query_weight.shape[0]
        and tokens.shape[0] * count * tokens.shape[1] <= 1 << 22
    )


def solution(mesh):
    placed = (
        P(("grp", "sp"), None),
        P(),
        P("sp", "tp"),
        P("sp", "tp"),
        P("sp", "tp"),
        P("tp"),
        P("tp", None),
        P("tp", "sp"),
        P("tp", "sp"),
    )
    shape = dict(mesh.shape)

    def chosen(*args):
        if fits(shape, args[0], args[2], args[4], args[5], args[8]):
            return fused(shape["sp"], *args)
        return on_device(*args)

    return jax.shard_map(
        chosen,
        mesh=mesh,
        in_specs=placed,
        out_specs=(P(("grp", "sp", "tp"), None), P(None, "tp", ("grp", "sp"))),
        check_vma=False,
    )
```
